32 devices in a mesh: sp: 4 (over y, x), tp: 8 (over z, core).
Axes of the slice: x: 2, y: 2, z: 4, core: 2. Of those that a mesh axis runs over, the one named last changes fastest.
Arguments:
- queries: bfloat16 [2048, 1536], P('sp', 'tp'), may hold values from -34 to 34
- latent: bfloat16 [2048, 512], P('sp'), may hold values from -6 to 6
- rot_key: bfloat16 [2048, 32], P('sp'), may hold values from -34 to 34
- latent_gain: float32 [512], replicated, may hold values from 0.1 to 1.9
- key_up: bfloat16 [512, 1024], P(None, 'tp'), may hold values from -0.25 to 0.25
- value_up: bfloat16 [512, 1024], P(None, 'tp'), may hold values from -0.70710678 to 0.70710678
- query_gain: float32 [96], replicated, may hold values from 0.5 to 6
- key_gain: float32 [96], replicated, may hold values from 0.5 to 6
- out_gain: float32 [1024], replicated, may hold values from 0.1 to 1.9
- out_weight: bfloat16 [1024, 2048], replicated, may hold values from -0.1875 to 0.1875
- residual: bfloat16 [2048, 2048], P(('sp', 'tp')), may hold values from -6 to 6
- ffn_gain: float32 [2048], replicated, may hold values from 0.1 to 1.9
- routes: int32 [2048, 2], P(('sp', 'tp')), may hold values from 0 to 3, all different within a row; in each aligned block of 64 rows (0 to 63, 64 to 127, ...) at most 36 rows name the same one
- route_weights: float32 [2048, 2], P(('sp', 'tp')), may hold values from 0.2 to 1
- expert_gate: bfloat16 [4, 2048, 2048], P('sp', None, 'tp'), may hold values from -0.125 to 0.125
- expert_up: bfloat16 [4, 2048, 2048], P('sp', None, 'tp'), may hold values from -0.125 to 0.125
- expert_down: bfloat16 [4, 2048, 2048], P('sp', 'tp'), may hold values from -0.125 to 0.125
Outputs:
- layer_out: bfloat16 [2048, 2048], P(('sp', 'tp'))
The draws below stay inside these ranges and needn't reach their ends.
Inputs may be any that keep to these rules, and one draw needn't show every extreme that they name: `routes`: the 2 experts of a token differ. Among the 64 rows of one device each expert is named by at most 36 rows, a bound that some block reaches.
All inputs are finite; a program needn't handle non-finite values.
Results may differ from the reference program's by a relative error of at most 0.02.
The reference program's roundings to bfloat16 on the way count: a program that leaves them out, or rounds other values in their place, can miss the bound.
Values may be sent and summed in bfloat16 or wider, within the bound.
A program may use at most 128 MiB of HBM per device.

```python
import math
import jax
import jax.numpy as jnp
import numpy as np
from jax import lax

D = 2048
HEADS = 16
NOPE = 64
ROPE = 32
VH = 64
LAT = 512
FF_E = 2048
TOPK = 2
TOK_DEV = 64
QK = 96
ATT_WIDTH = 1024
POS_SP = 512
LENGTH = 2048
EXPERTS = 4
CAP = 36
N_SP = 4
N_TP = 8


def drawn_pair(key):
    base_query = jnp.clip(jax.random.normal(jax.random.fold_in(key, 11), (LENGTH, HEADS, QK), jnp.float32), -6.0, 6.0)
    base_key = jnp.clip(jax.random.normal(jax.random.fold_in(key, 12), (LENGTH, ROPE), jnp.float32), -6.0, 6.0)
    return (base_query.reshape(LENGTH, HEADS * QK), base_key)


def draw_queries(key, part):
    return drawn_pair(key)[0].astype(jnp.bfloat16)


def draw_rot_key(key, part):
    return drawn_pair(key)[1].astype(jnp.bfloat16)


def head_gains(key):
    spread = 1.0 + 0.18 * jax.random.uniform(jax.random.fold_in(key, 1), (QK,), jnp.float32, -2.5, 2.5)
    return spread


def draw_query_gain(key, part):
    return head_gains(jax.random.fold_in(key, 21))


def draw_key_gain(key, part):
    return head_gains(jax.random.fold_in(key, 22))


def draw_value_up(key, part):
    head_ids = jnp.arange(HEADS * VH, dtype=jnp.int32) // VH
    rising = head_ids.astype(jnp.float32) / max(HEADS - 1, 1)
    entries = jnp.clip(jax.random.normal(jax.random.fold_in(key, 32), (LAT, HEADS * VH), jnp.float32), -4.0, 4.0)
    column_scale = 3.0 ** rising
    return (entries * column_scale[None, :] / jnp.sqrt(jnp.float32(LAT))).astype(jnp.bfloat16)


def shard_levels(rng, extent, shards, smallest, top_value):
    loudness = 1.0
    for position, parts in shards:
        steps = jax.random.uniform(jax.random.fold_in(jax.random.fold_in(rng, 6), position), (parts,), jnp.float32, smallest / len(shards), top_value / len(shards))
        loudness = loudness * jnp.repeat(jnp.exp(steps), extent[position] // parts).reshape((-1,) + (1,) * (len(extent) - 1 - position))
    return loudness


def shared_out(own_key, own, number, rows, number_of, top, reach, lean):
    ranking = jax.random.permutation(own_key, number_of)
    packed, ordinary = load_shares(number_of, rows * top, reach, lean, True), load_shares(number_of, rows * top, reach, lean, False)
    places = jnp.arange(number_of)

    def named(lengths, offset_by):
        used = int((lengths > 0).sum())
        fixed = max(1, used // 4)
        moved = fixed + (places - fixed + offset_by * (used - fixed)) % max(1, number_of - fixed)
        return jnp.zeros((number_of,), jnp.int32).at[ranking[jnp.where(places < fixed, places, moved)]].set(jnp.asarray(lengths, jnp.int32))

    lengths = jnp.where(number % 4 == 0, named(packed, number // 4), named(ordinary, number - number // 4 - 1))
    mixed = jax.random.permutation(jax.random.fold_in(own, 3), number_of)
    giver, sink = mixed[0:number_of // 2 * 2:2], mixed[1:number_of // 2 * 2:2]
    slack = jnp.minimum(lengths[giver] - 1, reach - lengths[sink]) // 2
    slack = jnp.where((giver == ranking[0]) | (sink == ranking[0]) | (lengths[sink] == 0), 0, jnp.maximum(slack, 0))
    moved = jax.random.randint(jax.random.fold_in(own, 4), (number_of // 2,), 0, 1 << 20) % (slack + 1)
    lengths = lengths.at[giver].add(-moved).at[sink].add(moved)
    members = jnp.searchsorted(jnp.cumsum(lengths), jnp.arange(rows * top), side="right").astype(jnp.int32)
    listing = members.reshape(top, rows).T
    listing = listing[jax.random.permutation(jax.random.fold_in(own, 1), rows)]
    offset_by = jax.random.randint(jax.random.fold_in(own, 2), (rows, 1), 0, top)
    return jnp.take_along_axis(listing, (jnp.arange(top)[None, :] + offset_by) % top, axis=1)


def load_shares(number_of, total, bound, slope, full):
    portions = [(1 << 20) // math.isqrt(rank ** slope) + 1 for rank in range(1, number_of + 1)]
    largest = bound if full else min(bound, max(-(-total // number_of), total * portions[0] // sum(portions)))
    least = 1 if total - largest >= number_of - 1 else 0
    given, rest = [largest] + [least] * (number_of - 1), total - largest - least * (number_of - 1)
    while rest > 0:
        candidates = [i for i in range(1, number_of) if given[i] < largest] or [i for i in range(1, number_of) if given[i] < bound]
        pool, budget = sum([portions[i] for i in candidates]), rest
        for i in candidates:
            more = min(bound - given[i], max(1, budget * portions[i] // pool), rest)
            given[i] = given[i] + more
            rest = rest - more
    return np.array(given)


def bell_draw(rng, dims, deviation, bound, split=(), kind=jnp.bfloat16):
    values = deviation * jax.random.normal(rng, dims, jnp.float32)
    if split:
        values = values * shard_levels(rng, dims, split, -0.22, 0.18)
    return jnp.clip(values, -bound, bound).astype(kind)


def setup_inputs(seed: int = 0) -> dict:
    streams_of = jax.random.split(jax.random.key(seed), 18)
    queries = draw_queries(jax.random.fold_in(streams_of[17], 71), 0)
    latent = bell_draw(streams_of[1], (LENGTH, LAT), 1.0, 6.0, ((0, 4),))
    rot_key = draw_rot_key(jax.random.fold_in(streams_of[17], 71), 0)
    latent_gain = jnp.clip(1.0 + 0.18 * jax.random.normal(streams_of[3], (LAT,), jnp.float32), 0.1, 1.9)
    key_up = bell_draw(streams_of[4], (LAT, HEADS * NOPE), LAT ** -0.5, 0.25, ((1, 8),))
    value_up = draw_value_up(jax.random.fold_in(streams_of[17], 71), 0)
    query_gain = draw_query_gain(jax.random.fold_in(streams_of[17], 71), 0)
    key_gain = draw_key_gain(jax.random.fold_in(streams_of[17], 71), 0)
    out_gain = jnp.clip(1.0 + 0.18 * jax.random.normal(streams_of[8], (ATT_WIDTH,), jnp.float32), 0.1, 1.9)
    out_weight = bell_draw(streams_of[9], (ATT_WIDTH, D), ATT_WIDTH ** -0.5, 0.1875)
    residual = bell_draw(streams_of[10], (LENGTH, D), 1.0, 6.0, ((0, 32),))
    ffn_gain = jnp.clip(1.0 + 0.18 * jax.random.normal(streams_of[11], (D,), jnp.float32), 0.1, 1.9)
    routes_keys = jax.random.split(jax.random.fold_in(streams_of[12], 1), LENGTH // TOK_DEV)
    routes_turns = jax.random.permutation(jax.random.fold_in(streams_of[12], 3), LENGTH // TOK_DEV)
    routes = jax.vmap(lambda own, number: shared_out(jax.random.fold_in(streams_of[12], 2), own, number, TOK_DEV, EXPERTS, TOPK, CAP, 1))(routes_keys, routes_turns).reshape((LENGTH, TOPK))
    route_weights = jnp.clip(0.2 + 0.8 * jax.random.uniform(streams_of[13], (LENGTH, TOPK), jnp.float32) ** shard_levels(streams_of[13], (LENGTH, TOPK), ((0, 32),), -0.2, 0.2), 0.2, 1.0)
    expert_gate = bell_draw(streams_of[14], (EXPERTS, D, FF_E), D ** -0.5, 0.125, ((0, 4), (2, 8)))
    expert_up = bell_draw(streams_of[15], (EXPERTS, D, FF_E), D ** -0.5, 0.125, ((0, 4), (2, 8)))
    expert_down = bell_draw(streams_of[16], (EXPERTS, FF_E, D), FF_E ** -0.5, 0.125, ((0, 4), (1, 8)))
    return dict(queries=queries, latent=latent, rot_key=rot_key, latent_gain=latent_gain, key_up=key_up, value_up=value_up, query_gain=query_gain, key_gain=key_gain, out_gain=out_gain, out_weight=out_weight, residual=residual, ffn_gain=ffn_gain, routes=routes, route_weights=route_weights, expert_gate=expert_gate, expert_up=expert_up, expert_down=expert_down)


epsilon = 1e-06
rope_base = 10000.0

def rms_scale(values):
    return lax.rsqrt(lax.optimization_barrier(jnp.mean(values * values, axis=-1, keepdims=True)) + epsilon)

def rotate_half(values, angles):
    half_dims = values.shape[-1] // 2
    first_half = values[..., :half_dims]
    second_half = values[..., half_dims:]
    cosine = jnp.cos(angles)
    sine_val = jnp.sin(angles)
    return jnp.concatenate([first_half * cosine - second_half * sine_val, second_half * cosine + first_half * sine_val], axis=-1)

def head_prepare(raw_rows, gain_vec, angles):
    normed_rows = raw_rows * rms_scale(raw_rows) * gain_vec
    turned_rows = rotate_half(normed_rows[..., NOPE:], angles[:, None, :])
    return jnp.concatenate([normed_rows[..., :NOPE], turned_rows], axis=-1).astype(jnp.bfloat16)

def attend_head(head_inputs):
    query_head, key_head, value_head = head_inputs
    query_f32 = query_head.astype(jnp.float32)
    key_f32 = key_head.astype(jnp.float32)
    value_f32 = value_head.astype(jnp.float32)
    block_count = LENGTH // POS_SP
    query_blocks = query_f32.reshape(block_count, POS_SP, QK)
    key_pos = jnp.arange(LENGTH, dtype=jnp.int32)

    def one_block(block_inputs):
        block_index, query_block = block_inputs
        scores = jnp.dot(query_block, key_f32.T, precision=lax.Precision.HIGHEST) * QK ** (-0.5)
        query_pos = block_index * POS_SP + jnp.arange(POS_SP, dtype=jnp.int32)
        allowed = key_pos[None, :] <= query_pos[:, None]
        scores = jnp.where(allowed, scores, -1e+30)
        row_peak = lax.optimization_barrier(jnp.max(scores, axis=1, keepdims=True))
        exponent = jnp.where(allowed, jnp.exp(scores - row_peak), 0.0)
        row_total = lax.optimization_barrier(jnp.sum(exponent, axis=1))
        rounded_exp = lax.optimization_barrier(exponent.astype(jnp.bfloat16)).astype(jnp.float32)
        result = jnp.dot(rounded_exp, value_f32, precision=lax.Precision.HIGHEST) / row_total[:, None]
        return result.astype(jnp.bfloat16)
    outputs = lax.map(one_block, (jnp.arange(block_count, dtype=jnp.int32), query_blocks))
    return outputs.reshape(LENGTH, VH)

def reference(queries, latent, rot_key, latent_gain, key_up, value_up, query_gain, key_gain, out_gain, out_weight, residual, ffn_gain, routes, route_weights, expert_gate, expert_up, expert_down):
    lat_f32 = latent.astype(jnp.float32)
    normed_latent = (lat_f32 * rms_scale(lat_f32) * latent_gain).astype(jnp.bfloat16)
    key_nope = jnp.dot(normed_latent, key_up, preferred_element_type=jnp.float32).astype(jnp.bfloat16)
    values = jnp.dot(normed_latent, value_up, preferred_element_type=jnp.float32).astype(jnp.bfloat16)
    positions = jnp.arange(LENGTH, dtype=jnp.int32)
    inverse = rope_base ** (-jnp.arange(0, ROPE, 2, dtype=jnp.float32) / ROPE)
    angles = positions.astype(jnp.float32)[:, None] * inverse[None, :]
    shared = jnp.broadcast_to(rot_key.astype(jnp.float32)[:, None, :], (LENGTH, HEADS, ROPE))
    raw_keys = jnp.concatenate([key_nope.astype(jnp.float32).reshape(LENGTH, HEADS, NOPE), shared], axis=-1)
    key_rows = head_prepare(raw_keys, key_gain, angles)
    query_rows = head_prepare(queries.astype(jnp.float32).reshape(LENGTH, HEADS, QK), query_gain, angles)
    value_heads = values.reshape(LENGTH, HEADS, VH)
    attended = lax.map(attend_head, (jnp.transpose(query_rows, (1, 0, 2)), jnp.transpose(key_rows, (1, 0, 2)), jnp.transpose(value_heads, (1, 0, 2))))
    att_rows = jnp.transpose(attended, (1, 0, 2)).reshape(LENGTH, ATT_WIDTH).astype(jnp.float32)
    normed_att = (att_rows * rms_scale(att_rows) * out_gain).astype(jnp.bfloat16)
    group_width = ATT_WIDTH // N_TP
    mixed = jnp.zeros((LENGTH, D), jnp.float32)
    for group_index in range(N_TP):
        low = group_index * group_width
        partial_value = jnp.dot(normed_att[:, low:low + group_width], out_weight[low:low + group_width], preferred_element_type=jnp.float32).astype(jnp.bfloat16)
        mixed = mixed + lax.optimization_barrier(partial_value).astype(jnp.float32)
    middle = residual.astype(jnp.float32) + mixed
    ffn_input = (middle * rms_scale(middle) * ffn_gain).astype(jnp.bfloat16)
    flat_routes = routes.reshape(-1).astype(jnp.int32)
    row_order = jnp.argsort(flat_routes, stable=True).astype(jnp.int32)
    expert_counts = lax.optimization_barrier(jnp.sum((flat_routes[:, None] == jnp.arange(EXPERTS, dtype=jnp.int32)[None, :]).astype(jnp.int32), axis=0))
    offsets = (jnp.cumsum(expert_counts) - expert_counts).astype(jnp.int32)
    row_limit = N_SP * N_TP * CAP
    weights_flat = route_weights.reshape(-1).astype(jnp.float32)
    hidden_width = FF_E // N_TP

    def per_expert(expert_id, combined):
        slot_ids = jnp.arange(row_limit, dtype=jnp.int32)
        is_live = slot_ids < expert_counts[expert_id]
        picked = row_order[jnp.minimum(offsets[expert_id] + slot_ids, LENGTH * TOPK - 1)]
        token_ids = (picked // TOPK).astype(jnp.int32)
        expert_in = ffn_input[token_ids]
        gate_pre = jnp.dot(expert_in, expert_gate[expert_id], preferred_element_type=jnp.float32)
        up_pre = jnp.dot(expert_in, expert_up[expert_id], preferred_element_type=jnp.float32)
        hidden = (jax.nn.silu(gate_pre) * up_pre).astype(jnp.bfloat16)
        down_weight = expert_down[expert_id]
        down_sum = jnp.zeros((row_limit, D), jnp.float32)
        for group_index in range(N_TP):
            low = group_index * hidden_width
            partial_value = jnp.dot(hidden[:, low:low + hidden_width], down_weight[low:low + hidden_width], preferred_element_type=jnp.float32).astype(jnp.bfloat16)
            down_sum = down_sum + lax.optimization_barrier(partial_value).astype(jnp.float32)
        expert_out = lax.optimization_barrier(down_sum.astype(jnp.bfloat16)).astype(jnp.float32)
        contrib_rows = expert_out * (weights_flat[picked] * is_live.astype(jnp.float32))[:, None]
        return combined.at[token_ids].add(contrib_rows)
    combined = lax.fori_loop(0, EXPERTS, per_expert, jnp.zeros((LENGTH, D), jnp.float32))
    return (middle + combined).astype(jnp.bfloat16)
```

```python
import jax
import jax.numpy as jnp
from jax import lax
from jax.experimental import pallas as pl
from jax.experimental.pallas import tpu as pltpu
from jax.sharding import PartitionSpec as P

D = 2048
NOPE = 64
ROPE = 32
VH = 64
TOPK = 2
QK = 96

epsilon = 1e-06
rope_base = 10000.0
MESH_ID = pl.DeviceIdType.MESH


class Place:
    def __init__(self, n_sp, n_z):
        self.n_sp, self.n_z = n_sp, n_z
        self.sp = lax.axis_index("sp")
        self.tp = lax.axis_index("tp")
        self.core = lax.rem(self.tp, 2)
        self.z = lax.div(self.tp, 2)

    def partner(self):
        return (self.sp, self.tp + 1 - 2 * self.core)

    def sp_peer(self, step):
        return lax.rem(self.sp + step, self.n_sp)

    def z_peer(self, step):
        return lax.rem(self.z + step, self.n_z)

    def sp_id(self, index):
        return (index, self.tp)

    def z_id(self, index):
        return (self.sp, 2 * index + self.core)

    def barrier(self, use_sp, use_z):
        sem = pltpu.get_barrier_semaphore()
        count = 1
        pl.semaphore_signal(sem, inc=1, device_id=self.partner(), device_id_type=MESH_ID)
        if use_sp:
            for step in range(1, self.n_sp):
                pl.semaphore_signal(
                    sem, inc=1, device_id=self.sp_id(self.sp_peer(step)), device_id_type=MESH_ID
                )
            count += self.n_sp - 1
        if use_z:
            for step in range(1, self.n_z):
                pl.semaphore_signal(
                    sem, inc=1, device_id=self.z_id(self.z_peer(step)), device_id_type=MESH_ID
                )
            count += self.n_z - 1
        pl.semaphore_wait(sem, count)


def remote(src, dst, send, recv, device):
    return pltpu.make_async_remote_copy(
        src_ref=src,
        dst_ref=dst,
        send_sem=send,
        recv_sem=recv,
        device_id=device,
        device_id_type=MESH_ID,
    )


def vmem():
    return pl.BlockSpec(memory_space=pltpu.VMEM)


def send_rows(x, n_sp, n_z):
    rows, shared = x.shape[1], D // 4
    half = (D - shared) // 2

    def kernel(x_ref, o_ref, local_sem, *sems):
        place = Place(n_sp, n_z)
        core, me = place.core, place.sp
        place.barrier(True, True)
        side = lax.rem(place.z, 2)
        twin = place.z_id(place.z + 1 - 2 * side)
        mine = pl.ds(pl.multiple_of(shared + side * half, 128), half)
        other = pl.ds(pl.multiple_of(shared + (1 - side) * half, 128), half)
        both = pl.ds(0, shared)
        copies = []

        def push(kind, step, src, dst, device):
            copy = remote(src, dst, sems[2 * kind].at[step], sems[2 * kind + 1].at[step], device)
            copy.start()
            copies.append(copy)
            return copy

        split, direct, swapped = {}, {}, {}
        for step in range(1, n_sp):
            dst = place.sp_peer(step)
            split[step] = push(
                0, step, x_ref.at[dst, :, mine], o_ref.at[core, me, :, mine], place.sp_id(dst)
            )
        for step in range(1, n_sp):
            dst = place.sp_peer(step)
            direct[step] = push(
                1, step, x_ref.at[dst, :, both], o_ref.at[core, me, :, both], place.sp_id(dst)
            )
        local = pltpu.make_async_copy(x_ref.at[me], o_ref.at[core, me], local_sem.at[0])
        local.start()
        last = [push(3, 0, x_ref.at[me], o_ref.at[core, me], place.partner())]
        for step in range(1, n_sp):
            src = lax.rem(me - step + n_sp, n_sp)
            piece = o_ref.at[core, src, :, mine]
            split[step].wait_recv()
            swapped[step] = push(2, step, piece, piece, twin)
            last.append(push(3, step, piece, piece, place.partner()))
        for step in range(1, n_sp):
            src = lax.rem(me - step + n_sp, n_sp)
            piece = o_ref.at[core, src, :, both]
            direct[step].wait_recv()
            last.append(push(4, step, piece, piece, place.partner()))
        for step in range(1, n_sp):
            src = lax.rem(me - step + n_sp, n_sp)
            piece = o_ref.at[core, src, :, other]
            swapped[step].wait_recv()
            last.append(push(5, step, piece, piece, place.partner()))
        for copy in last:
            copy.wait_recv()
        for copy in copies:
            copy.wait_send()
        local.wait()

    return pl.pallas_call(
        kernel,
        out_shape=jax.ShapeDtypeStruct((2, n_sp, rows, D), x.dtype),
        in_specs=[vmem()],
        out_specs=vmem(),
        scratch_shapes=[pltpu.SemaphoreType.DMA((1,))] + [pltpu.SemaphoreType.DMA((n_sp,))] * 12,
        compiler_params=pltpu.CompilerParams(
            collective_id=2, has_side_effects=True, vmem_limit_bytes=60 << 20
        ),
        name="send_rows",
    )(x)


CHUNKS = 4


def return_rows(hidden, down, mixer, middle, n_sp, n_z):
    rows = hidden.shape[2]
    tok = middle.shape[0]
    width = D // CHUNKS

    def kernel(h_ref, w_ref, mix_ref, mid_ref, o_ref, ybuf, pbuf, sbuf, rbuf, cbuf, fbuf, *sems):
        pair_s, pair_r, sp_s, sp_r, z_s, z_r = sems
        place = Place(n_sp, n_z)
        core = place.core
        place.barrier(True, True)
        pairs, sends, zsends = {}, {}, {}
        order = list(range(1, n_sp)) + [0]
        for q in range(CHUNKS):
            cols = pl.ds(q * width, width)
            for step in order:
                dst = place.sp_peer(step)
                ybuf[dst, :, cols] = jnp.dot(
                    h_ref[1 - core, dst], w_ref[:, cols], preferred_element_type=jnp.float32
                ).astype(jnp.bfloat16)
                copy = remote(
                    ybuf.at[dst, :, cols],
                    pbuf.at[dst, :, cols],
                    pair_s.at[q, step],
                    pair_r.at[q, step],
                    place.partner(),
                )
                copy.start()
                pairs[q, step] = copy
        for q in range(CHUNKS):
            cols = pl.ds(q * width, width)
            for step in order:
                dst = place.sp_peer(step)
                own = jnp.dot(
                    h_ref[core, dst], w_ref[:, cols], preferred_element_type=jnp.float32
                )
                pairs[q, step].wait_recv()
                total = (own + pbuf[dst, :, cols].astype(jnp.float32)).astype(jnp.bfloat16)
                if step == 0:
                    rbuf[dst, :, cols] = total
                else:
                    sbuf[dst, :, cols] = total
                    copy = remote(
                        sbuf.at[dst, :, cols],
                        rbuf.at[place.sp, :, cols],
                        sp_s.at[q, step],
                        sp_r.at[q, step],
                        place.sp_id(dst),
                    )
                    copy.start()
                    sends[q, step] = copy
        for q in range(CHUNKS):
            cols = pl.ds(q * width, width)
            for step in range(1, n_sp):
                sends[q, step].wait_recv()
            combined = jnp.zeros((n_z * tok, width), jnp.float32)
            for src in range(n_sp):
                combined += jnp.dot(
                    mix_ref[src], rbuf[src, :, cols], preferred_element_type=jnp.float32
                )
            cbuf[:, :, cols] = combined.astype(jnp.bfloat16).reshape(n_z, tok, width)
            for step in range(1, n_z):
                dst = place.z_peer(step)
                copy = remote(
                    cbuf.at[dst, :, cols],
                    fbuf.at[place.z, :, cols],
                    z_s.at[q, step],
                    z_r.at[q, step],
                    place.z_id(dst),
                )
                copy.start()
                zsends[q, step] = copy
        for q in range(CHUNKS):
            cols = pl.ds(q * width, width)
            total = mid_ref[:, cols] + cbuf[place.z, :, cols].astype(jnp.float32)
            for step in range(1, n_z):
                src = lax.rem(place.z - step + n_z, n_z)
                zsends[q, step].wait_recv()
                total += fbuf[src, :, cols].astype(jnp.float32)
            o_ref[:, cols] = total.astype(jnp.bfloat16)
        for group in (pairs, sends, zsends):
            for copy in group.values():
                copy.wait_send()

    dma = pltpu.SemaphoreType.DMA
    block = pltpu.VMEM((n_sp, rows, D), jnp.bfloat16)
    zblock = pltpu.VMEM((n_z, tok, D), jnp.bfloat16)
    return pl.pallas_call(
        kernel,
        out_shape=jax.ShapeDtypeStruct((tok, D), jnp.bfloat16),
        in_specs=[vmem()] * 4,
        out_specs=vmem(),
        scratch_shapes=[block, block, block, block, zblock, zblock]
        + [dma((CHUNKS, n_sp))] * 4
        + [dma((CHUNKS, n_z))] * 2,
        compiler_params=pltpu.CompilerParams(
            collective_id=3, has_side_effects=True, vmem_limit_bytes=60 << 20
        ),
        name="return_rows",
    )(hidden, down, mixer, middle)


def split_dot(a, b, dims):
    return lax.dot_general(a, b, (dims, ((), ())), preferred_element_type=jnp.float32)


NT = ((1,), (1,))
NN = ((1,), (0,))
TN = ((0,), (0,))


def front(
    queries, latent, rot_key, lat_gain, key_up, value_up, q_gain, k_gain, out_gain,
    out_weight, residual, ffn_gain, routes, weights, cosine, sine, n_sp, n_z, width,
):
    length = queries.shape[0]
    heads = queries.shape[1] // QK
    n_tp = 2 * n_z
    tok = residual.shape[0]
    part = n_z * tok
    cap = max(2, 9 * tok * TOPK // (8 * n_sp))
    rows = n_z * cap
    bundle = 2 * length + length // 2
    half = length // 2
    lanes = 128
    att_width = width
    qt = 256
    pt = 128

    def kernel(
        q_in, lat_in, rot_in, latg, kup, vup, qg, kg, outg, w_hbm, res_in, ffng, routes_in,
        weights_in, cos_in, sin_in, out_rows, mixer, mid_out,
        qbuf, kv, peak, total, acc, att, gath, normed, wbuf, resbuf, metabuf, mid, ffn,
        w_sem, local_sem, kv_s, kv_r, res_s, res_r, meta_s, meta_r, att_s, att_r,
    ):
        place = Place(n_sp, n_z)
        sp, core, z, tp = place.sp, place.core, place.z, place.tp
        load_w = pltpu.make_async_copy(w_hbm, wbuf, w_sem.at[0])
        load_w.start()
        sem = pltpu.get_barrier_semaphore()
        for step in range(1, n_tp):
            pl.semaphore_signal(
                sem, inc=1, device_id=(sp, lax.rem(tp + step, n_tp)), device_id_type=MESH_ID
            )
        for step in range(1, n_sp):
            pl.semaphore_signal(
                sem, inc=1, device_id=place.sp_id(place.sp_peer(step)), device_id_type=MESH_ID
            )

        lane_id = lax.broadcasted_iota(jnp.int32, (tok, lanes), 1)
        r0, r1 = routes_in[:, 0:1], routes_in[:, 1:2]
        named0, named1 = lane_id == r0, lane_id == r1
        named = jnp.where(named0 | named1, 1.0, 0.0)
        earlier = jnp.where(
            lax.broadcasted_iota(jnp.int32, (tok, tok), 1)
            < lax.broadcasted_iota(jnp.int32, (tok, tok), 0),
            1.0,
            0.0,
        ).astype(jnp.bfloat16)
        rank = split_dot(earlier, named.astype(jnp.bfloat16), NN)
        slot = jnp.where(named0 | named1, rank + (z * cap).astype(jnp.float32), -1.0)
        share = jnp.where(named0, weights_in[:, 0:1], 0.0) + jnp.where(
            named1, weights_in[:, 1:2], 0.0
        )
        metabuf[z] = jnp.where(lane_id < 64, slot, pltpu.roll(share, 64, 1))

        pl.semaphore_wait(sem, n_tp - 1 + n_sp - 1)
        sends = []

        def push(src, dst, send, recv, device):
            copy = remote(src, dst, send, recv, device)
            copy.start()
            return copy

        res_copies, meta_copies = [], []
        for step in range(1, n_z):
            to = place.z_id(place.z_peer(step))
            meta_copies.append(
                push(metabuf.at[z], metabuf.at[z], meta_s.at[step], meta_r.at[step], to)
            )
        for step in range(1, n_z):
            to = place.z_id(place.z_peer(step))
            res_copies.append(push(res_in, resbuf.at[z], res_s.at[step], res_r.at[step], to))
        local = pltpu.make_async_copy(res_in, resbuf.at[z], local_sem.at[0])
        local.start()

        lane = lax.broadcasted_iota(jnp.int32, (1, lanes), 1)
        low = lane % ROPE < ROPE // 2
        mine = kv.at[sp]

        def turn(values, cos, sin):
            return (
                values * cos
                + pltpu.roll(values, lanes - ROPE // 2, 1) * jnp.where(low, -sin, 0.0)
                + pltpu.roll(values, ROPE // 2, 1) * jnp.where(low, 0.0, sin)
            )

        sel = lax.broadcasted_iota(jnp.int32, (ROPE, lanes), 0)
        rot_sel = jnp.where(
            (lax.broadcasted_iota(jnp.int32, (ROPE, lanes), 1) % ROPE == sel)
            & (lax.broadcasted_iota(jnp.int32, (ROPE, lanes), 1) < heads * ROPE),
            1.0,
            0.0,
        ).astype(jnp.bfloat16)
        rot_parts = length // pt

        def make_keys(i, carry):
            at = pl.ds(pl.multiple_of(i * pt, pt), pt)
            lat = lat_in[at, :].astype(jnp.float32)
            scale = lax.rsqrt(jnp.mean(lat * lat, axis=-1, keepdims=True) + epsilon)
            normed_lat = (lat * scale * latg[...]).astype(jnp.bfloat16)
            nope = split_dot(normed_lat, kup[...], NN).astype(jnp.bfloat16).astype(jnp.float32)
            vals = split_dot(normed_lat, vup[...], NN).astype(jnp.bfloat16)
            kv[sp, pl.ds(pl.multiple_of(length + i * pt, pt), pt), :] = vals
            rot = split_dot(rot_in[at, :], rot_sel, NN)
            square, rot_square = nope * nope, rot * rot
            nope_scale, rot_scale = None, None
            for h in range(heads):
                in_nope = (lane >= h * NOPE) & (lane < (h + 1) * NOPE)
                in_rot = (lane >= h * ROPE) & (lane < (h + 1) * ROPE)
                one = lax.rsqrt(
                    jnp.sum(
                        jnp.where(in_nope, square, 0.0) + jnp.where(in_rot, rot_square, 0.0),
                        axis=-1,
                        keepdims=True,
                    )
                    / QK
                    + epsilon
                )
                nope_scale = one if h == 0 else jnp.where(in_nope, one, nope_scale)
                rot_scale = one if h == 0 else jnp.where(in_rot, one, rot_scale)
            kv[sp, at, :] = (nope * nope_scale * kg[0:1, :lanes]).astype(jnp.bfloat16)
            turned = turn(rot * rot_scale * kg[0:1, lanes:], cos_in[at, :], sin_in[at, :])
            return turned

        def make_pair(i, carry):
            first = make_keys(i, carry)
            second = make_keys(i + rot_parts // 2, carry)
            packed = first + pltpu.roll(second, 64, 1)
            kv[sp, pl.ds(pl.multiple_of(2 * length + i * pt, pt), pt), :] = packed.astype(
                jnp.bfloat16
            )
            return carry

        lax.fori_loop(0, rot_parts // 2, make_pair, 0)
        for step in range(1, n_sp):
            dst = sp + n_sp - step

            @pl.when(dst < n_sp)
            def _(dst=dst):
                push(mine, mine, kv_s.at[dst], kv_r.at[sp], place.sp_id(dst))

        wide = 2 * lanes
        src_id = lax.broadcasted_iota(jnp.int32, (heads * QK, wide), 0)
        dst_id = lax.broadcasted_iota(jnp.int32, (heads * QK, wide), 1)
        pickers = []
        for h in range(heads):
            entry = src_id - h * QK
            nope_hit = (entry >= 0) & (entry < NOPE) & (dst_id == h * NOPE + entry)
            rot_hit = (
                (entry >= NOPE) & (entry < QK) & (dst_id == lanes + h * ROPE + entry - NOPE)
            )
            pickers.append(jnp.where(nope_hit | rot_hit, 1.0, 0.0).astype(jnp.bfloat16))

        def make_queries(i, carry):
            at = pl.ds(pl.multiple_of(i * pt, pt), pt)
            raw = q_in[at, :]
            for h in range(heads):
                spread = split_dot(raw, pickers[h], NN)
                scale = lax.rsqrt(
                    jnp.sum(spread * spread, axis=-1, keepdims=True) / QK + epsilon
                )
                spread = spread * scale * qg[0:1, :]
                nope = spread[:, :lanes].astype(jnp.bfloat16)
                rot = turn(spread[:, lanes:], cos_in[at, :], sin_in[at, :])
                qbuf[h, 0, at, :lanes] = nope
                qbuf[h, 1, at, :lanes] = nope
                qbuf[h, 0, at, lanes:] = rot.astype(jnp.bfloat16)
                qbuf[h, 1, at, lanes:] = pltpu.roll(rot, 64, 1).astype(jnp.bfloat16)
            return carry

        lax.fori_loop(0, length // pt, make_queries, 0)

        factor = QK ** (-0.5) * 1.4426950408889634

        def attend(src, first, diagonal):
            knope = [kv[src, s * half : (s + 1) * half, :] for s in range(2)]
            krot = kv[src, 2 * length : bundle, :]
            keys = [jnp.concatenate([knope[s], krot], axis=1) for s in range(2)]
            vals = kv[src, length : 2 * length, :]

            def tile(i, carry):
                at = pl.ds(pl.multiple_of(i * qt, qt), qt)
                outs = []
                for h in range(heads):
                    scores = jnp.concatenate(
                        [split_dot(qbuf[h, s, at, :], keys[s], NT) for s in range(2)], axis=1
                    )
                    scores = scores * factor
                    if diagonal:
                        row = lax.broadcasted_iota(jnp.int32, scores.shape, 0) + i * qt
                        col = lax.broadcasted_iota(jnp.int32, scores.shape, 1)
                        scores = jnp.where(col <= row, scores, -1e30)
                    top = jnp.max(scores, axis=-1, keepdims=True)
                    if not first:
                        old = peak[h, at, :]
                        top = jnp.maximum(old[:, :1], top)
                    weight = jnp.exp2(scores - top)
                    sums = jnp.sum(weight, axis=-1, keepdims=True)
                    part_out = split_dot(weight.astype(jnp.bfloat16), vals, NN)
                    if first:
                        total[h, at, :] = jnp.broadcast_to(sums, (qt, lanes))
                        outs.append((part_out, None))
                    else:
                        fade = jnp.exp2(old[:, :1] - top)
                        total[h, at, :] = total[h, at, :] * fade + sums
                        outs.append((part_out, fade))
                    peak[h, at, :] = jnp.broadcast_to(top, (qt, lanes))
                new, fade = outs[0]
                for h in range(1, heads):
                    new = jnp.where(lane >= h * VH, outs[h][0], new)
                    if not first:
                        fade = jnp.where(lane >= h * VH, outs[h][1], fade)
                acc[at, :] = new if first else acc[at, :] * fade + new
                return carry

            lax.fori_loop(0, length // qt, tile, 0)

        attend(sp, True, True)

        def visit(step, carry):
            src = sp - step

            @pl.when(src >= 0)
            def _():
                remote(
                    kv.at[src], kv.at[src], kv_s.at[src], kv_r.at[src], place.sp_id(src)
                ).wait_recv()
                attend(src, False, False)

            return carry

        lax.fori_loop(1, n_sp, visit, 0)

        for block in range(n_tp):
            at = pl.ds(block * tok, tok)
            bottom = total[0, at, :]
            for h in range(1, heads):
                bottom = jnp.where(lane >= h * VH, total[h, at, :], bottom)
            att[block % 2, (block // 2) * tok : (block // 2 + 1) * tok, :] = (
                acc[at, :] / bottom
            ).astype(jnp.bfloat16)
        att_copies = []
        for step in range(1, n_tp):
            dst = lax.rem(tp + step, n_tp)
            att_copies.append(
                push(
                    att.at[lax.rem(dst, 2)],
                    gath.at[tp],
                    att_s.at[step],
                    att_r.at[step],
                    (sp, dst),
                )
            )
        own = pltpu.make_async_copy(att.at[core], gath.at[tp], local_sem.at[1])
        own.start()

        for copy in meta_copies:
            copy.wait_recv()
        meta = metabuf[...].reshape(part, lanes)
        slot_id = lax.broadcasted_iota(jnp.int32, (part, rows), 1).astype(jnp.float32)
        for e in range(n_sp):
            hit = meta[:, e : e + 1] == slot_id
            mixer[e] = jnp.where(hit, meta[:, 64 + e : 65 + e], 0.0).astype(jnp.bfloat16)
        for copy in res_copies:
            copy.wait_recv()
        local.wait()
        load_w.wait()
        own.wait()
        for copy in att_copies:
            copy.wait_recv()

        square = None
        for t in range(n_tp):
            block = gath[t].astype(jnp.float32)
            square = block * block if square is None else square + block * block
        scale = lax.rsqrt(jnp.sum(square, axis=-1, keepdims=True) / att_width + epsilon)
        for t in range(n_tp):
            normed[:, t * lanes : (t + 1) * lanes] = (
                gath[t].astype(jnp.float32) * scale * outg[t]
            ).astype(jnp.bfloat16)
        ct = 512
        square = None
        for c in range(D // ct):
            cols = slice(c * ct, (c + 1) * ct)
            values = split_dot(normed[...], wbuf[:, cols], NN) + resbuf[:, :, cols].reshape(
                part, ct
            ).astype(jnp.float32)
            mid[:, cols] = values
            more = jnp.sum(values * values, axis=-1, keepdims=True)
            square = more if square is None else square + more
        scale = lax.rsqrt(square / D + epsilon)
        for c in range(D // ct):
            cols = slice(c * ct, (c + 1) * ct)
            ffn[:, cols] = (mid[:, cols] * scale * ffng[0:1, cols]).astype(jnp.bfloat16)
        mid_out[...] = mid[pl.ds(pl.multiple_of(z * tok, tok), tok), :]
        for e in range(n_sp):
            hit = jnp.where(meta[:, e : e + 1] == slot_id, 1.0, 0.0).astype(jnp.bfloat16)
            for c in range(D // ct):
                cols = slice(c * ct, (c + 1) * ct)
                out_rows[e, :, cols] = split_dot(hit, ffn[:, cols], TN).astype(jnp.bfloat16)

        for copy in meta_copies + res_copies + att_copies:
            copy.wait_send()
        for step in range(1, n_sp):
            dst = sp + n_sp - step

            @pl.when(dst < n_sp)
            def _(dst=dst):
                remote(mine, mine, kv_s.at[dst], kv_r.at[sp], place.sp_id(dst)).wait_send()

    dma = pltpu.SemaphoreType.DMA
    bf, f4 = jnp.bfloat16, jnp.float32
    specs = [vmem()] * 9 + [pl.BlockSpec(memory_space=pl.ANY)] + [vmem()] * 6
    return pl.pallas_call(
        kernel,
        out_shape=(
            jax.ShapeDtypeStruct((n_sp, rows, D), bf),
            jax.ShapeDtypeStruct((n_sp, part, rows), bf),
            jax.ShapeDtypeStruct((tok, D), f4),
        ),
        in_specs=specs,
        out_specs=(vmem(),) * 3,
        scratch_shapes=[
            pltpu.VMEM((heads, 2, length, 2 * lanes), bf),
            pltpu.VMEM((n_sp, bundle, lanes), bf),
            pltpu.VMEM((heads, length, lanes), f4),
            pltpu.VMEM((heads, length, lanes), f4),
            pltpu.VMEM((length, lanes), f4),
            pltpu.VMEM((2, part, lanes), bf),
            pltpu.VMEM((n_tp, part, lanes), bf),
            pltpu.VMEM((part, n_tp * lanes), bf),
            pltpu.VMEM(out_weight.shape, bf),
            pltpu.VMEM((n_z, tok, D), bf),
            pltpu.VMEM((n_z, tok, lanes), f4),
            pltpu.VMEM((part, D), f4),
            pltpu.VMEM((part, D), bf),
            dma((1,)),
            dma((2,)),
            dma((n_sp,)),
            dma((n_sp,)),
            dma((n_z,)),
            dma((n_z,)),
            dma((n_z,)),
            dma((n_z,)),
            dma((n_tp,)),
            dma((n_tp,)),
        ],
        compiler_params=pltpu.CompilerParams(
            collective_id=0, has_side_effects=True, vmem_limit_bytes=60 << 20
        ),
        name="front",
    )(
        queries, latent, rot_key, lat_gain, key_up, value_up, q_gain, k_gain, out_gain,
        out_weight, residual, ffn_gain, routes, weights, cosine, sine,
    )


def packed_gain(gain, heads):
    nope = jnp.tile(gain[:NOPE], 2)
    rot = jnp.concatenate([jnp.tile(gain[NOPE:], heads), jnp.zeros((128 - heads * ROPE,))])
    return jnp.concatenate([nope, rot])[None, :]


def shards(
    queries, latent, rot_key, latent_gain, key_up, value_up, query_gain, key_gain, out_gain,
    out_weight, residual, ffn_gain, routes, route_weights, expert_gate, expert_up, expert_down,
):
    length = queries.shape[0]
    heads = key_up.shape[1] // NOPE
    n_sp = lax.axis_size("sp")
    n_tp = lax.axis_size("tp")
    n_z = n_tp // 2
    width = heads * VH
    first = lax.axis_index("sp") * length
    positions = (first + jnp.arange(length, dtype=jnp.int32)).astype(jnp.float32)
    inverse = rope_base ** (-jnp.arange(0, ROPE, 2, dtype=jnp.float32) / ROPE)
    angles = positions[:, None] * jnp.tile(inverse, 128 // (ROPE // 2))[None, :]
    out_gain = out_gain.reshape(n_tp, 1, width)
    if width < 128:
        spare = 128 - width
        key_up = jnp.pad(key_up, ((0, 0), (0, spare)))
        value_up = jnp.pad(value_up, ((0, 0), (0, spare)))
        out_gain = jnp.pad(out_gain, ((0, 0), (0, 0), (0, spare)))
        out_weight = jnp.pad(
            out_weight.reshape(n_tp, width, D), ((0, 0), (0, spare), (0, 0))
        ).reshape(n_tp * 128, D)
    outbound, mixer, middle = front(
        queries, latent, rot_key, latent_gain[None, :], key_up, value_up,
        packed_gain(query_gain, heads), packed_gain(key_gain, heads), out_gain, out_weight,
        residual, ffn_gain[None, :], routes, route_weights, jnp.cos(angles), jnp.sin(angles),
        n_sp, n_z, n_tp * width,
    )
    rows = outbound.shape[1]
    arrived = send_rows(outbound, n_sp, n_z)
    row_block = arrived.reshape(2 * n_sp * rows, D)
    gate_pre = jnp.dot(row_block, expert_gate[0], preferred_element_type=jnp.float32)
    up_pre = jnp.dot(row_block, expert_up[0], preferred_element_type=jnp.float32)
    hidden = (jax.nn.silu(gate_pre) * up_pre).astype(jnp.bfloat16)
    return return_rows(
        hidden.reshape(2, n_sp, rows, -1), expert_down[0], mixer, middle, n_sp, n_z
    )


def solution(mesh):
    return jax.shard_map(
        shards,
        mesh=mesh,
        in_specs=(
            P("sp", "tp"),
            P("sp", None),
            P("sp", None),
            P(),
            P(None, "tp"),
            P(None, "tp"),
            P(),
            P(),
            P(),
            P(),
            P(("sp", "tp"), None),
            P(),
            P(("sp", "tp"), None),
            P(("sp", "tp"), None),
            P("sp", None, "tp"),
            P("sp", None, "tp"),
            P("sp", "tp", None),
        ),
        out_specs=P(("sp", "tp"), None),
        check_vma=False,
    )
```

```python
import jax
import jax.numpy as jnp
import numpy as np
from jax import lax
from jax.experimental import pallas as pl
from jax.experimental.pallas import tpu as pltpu
from jax.sharding import PartitionSpec as P

D = 2048
NOPE = 64
ROPE = 32
VH = 64
TOPK = 2
QK = 96

epsilon = 1e-06
rope_base = 10000.0
MESH_ID = pl.DeviceIdType.MESH


class Place:
    def __init__(self, n_sp, n_z):
        self.n_sp, self.n_z = n_sp, n_z
        self.sp = lax.axis_index("sp")
        self.tp = lax.axis_index("tp")
        self.core = lax.rem(self.tp, 2)
        self.z = lax.div(self.tp, 2)

    def partner(self):
        return (self.sp, self.tp + 1 - 2 * self.core)

    def sp_peer(self, step):
        return lax.rem(self.sp + step, self.n_sp)

    def z_peer(self, step):
        return lax.rem(self.z + step, self.n_z)

    def sp_id(self, index):
        return (index, self.tp)

    def z_id(self, index):
        return (self.sp, 2 * index + self.core)

    def barrier(self, use_sp, use_z):
        sem = pltpu.get_barrier_semaphore()
        count = 1
        pl.semaphore_signal(sem, inc=1, device_id=self.partner(), device_id_type=MESH_ID)
        if use_sp:
            for step in range(1, self.n_sp):
                pl.semaphore_signal(
                    sem, inc=1, device_id=self.sp_id(self.sp_peer(step)), device_id_type=MESH_ID
                )
            count += self.n_sp - 1
        if use_z:
            for step in range(1, self.n_z):
                pl.semaphore_signal(
                    sem, inc=1, device_id=self.z_id(self.z_peer(step)), device_id_type=MESH_ID
                )
            count += self.n_z - 1
        pl.semaphore_wait(sem, count)


def remote(src, dst, send, recv, device):
    return pltpu.make_async_remote_copy(
        src_ref=src,
        dst_ref=dst,
        send_sem=send,
        recv_sem=recv,
        device_id=device,
        device_id_type=MESH_ID,
    )


def vmem():
    return pl.BlockSpec(memory_space=pltpu.VMEM)


def flip(value, bits):
    shift = 1
    while shift <= bits:
        if bits & shift:
            value = value + shift * (1 - 2 * lax.rem(lax.div(value, shift), 2))
        shift *= 2
    return value


CHUNKS = 8
PIECES = 3


def experts(outbound, mixer, middle, gate, up, down, n_sp, n_z):
    rows = outbound.shape[1]
    tok = middle.shape[0]
    width = D // CHUNKS
    hidden = gate.shape[1]
    shared = D // 4
    half = (D - shared) // 2
    piece = half // PIECES
    phases = [[1, 2]] + [[k] for k in range(3, n_sp)] if n_sp > 2 else [[1]]

    def kernel(
        x_in, mix_in, mid_in, gate_hbm, up_hbm, down_hbm, o_ref,
        gbuf, ubuf, dbuf, xbuf, hid, ybuf, pbuf, sbuf, rbuf, cbuf, fbuf,
        w_sem, a_s, a_r, b_s, b_r, t_s, t_r, pa_s, pa_r, pb_s, pb_r, pt_s, pt_r, po_s, po_r,
        y_s, y_r, sp_s, sp_r, z_s, z_r,
    ):
        place = Place(n_sp, n_z)
        core, z, me = place.core, place.z, place.sp
        loads = []
        for i, (src, dst) in enumerate(((gate_hbm, gbuf), (up_hbm, ubuf), (down_hbm, dbuf))):
            load = pltpu.make_async_copy(src, dst, w_sem.at[i])
            load.start()
            loads.append(load)
        place.barrier(True, True)
        side = lax.rem(z, 2)
        twin = place.z_id(z + 1 - 2 * side)
        partner = place.partner()
        both = pl.ds(0, shared)

        def strip(which, p):
            return pl.ds(pl.multiple_of(shared + which * half + p * piece, 128), piece)

        copies = []

        def push(src, dst, send, recv, device):
            copy = remote(src, dst, send, recv, device)
            copy.start()
            copies.append(copy)
            return copy

        own_in = push(
            x_in.at[me], xbuf.at[core, me], po_s.at[0], po_r.at[0], partner
        )
        strips, shares, swaps, to_pair = {}, {}, {}, {k: [] for k in range(n_sp)}
        for ks in phases:
            for p in range(PIECES):
                for k in ks:
                    dst = flip(me, k)
                    cols = strip(side, p)
                    strips[k, p] = push(
                        x_in.at[dst, :, cols], xbuf.at[core, me, :, cols],
                        a_s.at[k, p], a_r.at[k, p], place.sp_id(dst),
                    )
            for k in ks:
                dst = flip(me, k)
                shares[k] = push(
                    x_in.at[dst, :, both], xbuf.at[core, me, :, both],
                    b_s.at[k], b_r.at[k], place.sp_id(dst),
                )

        def forward_strip(k, p):
            block = xbuf.at[core, flip(me, k), :, strip(side, p)]
            strips[k, p].wait_recv()
            swaps[k, p] = push(block, block, t_s.at[k, p], t_r.at[k, p], twin)
            to_pair[k].append(push(block, block, pa_s.at[k, p], pa_r.at[k, p], partner))

        def forward_share(k):
            block = xbuf.at[core, flip(me, k), :, both]
            shares[k].wait_recv()
            to_pair[k].append(push(block, block, pb_s.at[k], pb_r.at[k], partner))

        def forward_swap(k, p):
            block = xbuf.at[core, flip(me, k), :, strip(1 - side, p)]
            swaps[k, p].wait_recv()
            to_pair[k].append(push(block, block, pt_s.at[k, p], pt_r.at[k, p], partner))

        def expert(x_ref, h_ref):
            g = jnp.dot(x_ref[...], gbuf[...], preferred_element_type=jnp.float32)
            u = jnp.dot(x_ref[...], ubuf[...], preferred_element_type=jnp.float32)
            h_ref[...] = (g / (1.0 + jnp.exp(-g)) * u).astype(jnp.bfloat16)

        def column(q):
            return pl.ds(pl.multiple_of(q * width, width), width)

        def pair_copy(k, q):
            src = flip(me, k)
            return remote(
                ybuf.at[src, :, column(q)], pbuf.at[src, :, column(q)],
                y_s.at[k, q], y_r.at[k, q], partner,
            )

        def back_copy(k, q):
            src = flip(me, k)
            return remote(
                sbuf.at[src, :, column(q)], rbuf.at[me, :, column(q)],
                sp_s.at[k, q], sp_r.at[k, q], place.sp_id(src),
            )

        def expert_own(k):
            src = flip(me, k)
            expert(x_in.at[me] if k == 0 else xbuf.at[core, src], hid.at[core, src])

        def expert_pair(k):
            src = flip(me, k)
            if k == 0:
                own_in.wait_recv()
            for copy in to_pair[k]:
                copy.wait_recv()
            expert(xbuf.at[1 - core, src], hid.at[1 - core, src])

            def body(q, carry):
                ybuf[src, :, column(q)] = jnp.dot(
                    hid[1 - core, src], dbuf[:, column(q)], preferred_element_type=jnp.float32
                ).astype(jnp.bfloat16)
                pair_copy(k, q).start()
                return carry

            lax.fori_loop(0, CHUNKS, body, 0)

        def finish(ks):
            def body(q, carry):
                for k in ks:
                    src = flip(me, k)
                    own = jnp.dot(
                        hid[core, src], dbuf[:, column(q)], preferred_element_type=jnp.float32
                    )
                    pair_copy(k, q).wait_recv()
                    total = (own + pbuf[src, :, column(q)].astype(jnp.float32)).astype(
                        jnp.bfloat16
                    )
                    if k == 0:
                        rbuf[src, :, column(q)] = total
                    else:
                        sbuf[src, :, column(q)] = total
                        back_copy(k, q).start()
                return carry

            lax.fori_loop(0, CHUNKS, body, 0)

        def arrivals(ks):
            steps = []
            for p in range(PIECES):
                steps.append(lambda p=p: [forward_strip(k, p) for k in ks])
            steps.append(lambda: [forward_share(k) for k in ks])
            return steps

        for load in loads[:2]:
            load.wait()
        waiting = arrivals(phases[0])
        expert_own(0)
        waiting.pop(0)()
        loads[2].wait()
        expert_pair(0)
        waiting.pop(0)()
        finish([0])
        for index, ks in enumerate(phases):
            while waiting:
                waiting.pop(0)()
            for p in range(PIECES):
                for k in ks:
                    forward_swap(k, p)
            waiting = arrivals(phases[index + 1]) if index + 1 < len(phases) else []
            for k in ks:
                expert_own(k)
            if waiting:
                waiting.pop(0)()
            for k in ks:
                expert_pair(k)
                if waiting:
                    waiting.pop(0)()
            finish(ks)

        def z_copy(q, step):
            dst = place.z_peer(step)
            return remote(
                cbuf.at[dst, :, column(q)], fbuf.at[z, :, column(q)],
                z_s.at[q, step], z_r.at[q, step], place.z_id(dst),
            )

        def combine(q, carry):
            for k in range(1, n_sp):
                back_copy(k, q).wait_recv()
            total = None
            for src in range(n_sp):
                more = split_dot(mix_in[src], rbuf[src, :, column(q)], TN)
                total = more if total is None else total + more
            cbuf[:, :, column(q)] = total.astype(jnp.bfloat16).reshape(n_z, tok, width)
            for step in range(1, n_z):
                z_copy(q, step).start()
            return carry

        lax.fori_loop(0, CHUNKS, combine, 0)

        def close(q, carry):
            total = mid_in[:, column(q)] + cbuf[z, :, column(q)].astype(jnp.float32)
            for step in range(1, n_z):
                z_copy(q, step).wait_recv()
                total += fbuf[lax.rem(z - step + n_z, n_z), :, column(q)].astype(jnp.float32)
            o_ref[:, column(q)] = total.astype(jnp.bfloat16)
            return carry

        lax.fori_loop(0, CHUNKS, close, 0)

        def drain(q, carry):
            for k in range(n_sp):
                pair_copy(k, q).wait_send()
            for k in range(1, n_sp):
                back_copy(k, q).wait_send()
            for step in range(1, n_z):
                z_copy(q, step).wait_send()
            return carry

        for copy in copies:
            copy.wait_send()
        lax.fori_loop(0, CHUNKS, drain, 0)

    dma = pltpu.SemaphoreType.DMA
    bf = jnp.bfloat16
    block = pltpu.VMEM((n_sp, rows, D), bf)
    zblock = pltpu.VMEM((n_z, tok, D), bf)
    any_spec = pl.BlockSpec(memory_space=pl.ANY)
    return pl.pallas_call(
        kernel,
        out_shape=jax.ShapeDtypeStruct((tok, D), bf),
        in_specs=[vmem()] * 3 + [any_spec] * 3,
        out_specs=vmem(),
        scratch_shapes=[
            pltpu.VMEM(gate.shape, bf),
            pltpu.VMEM(up.shape, bf),
            pltpu.VMEM(down.shape, bf),
            pltpu.VMEM((2, n_sp, rows, D), bf),
            pltpu.VMEM((2, n_sp, rows, hidden), bf),
            block, block, block, block, zblock, zblock,
            dma((3,)),
        ]
        + [dma((n_sp, PIECES))] * 2
        + [dma((n_sp,))] * 2
        + [dma((n_sp, PIECES))] * 4
        + [dma((n_sp,))] * 2
        + [dma((n_sp, PIECES))] * 2
        + [dma((1,))] * 2
        + [dma((n_sp, CHUNKS))] * 4
        + [dma((CHUNKS, n_z))] * 2,
        compiler_params=pltpu.CompilerParams(
            collective_id=1, has_side_effects=True, vmem_limit_bytes=62 << 20
        ),
        name="experts",
    )(outbound, mixer, middle, gate, up, down)


def split_dot(a, b, dims):
    return lax.dot_general(a, b, (dims, ((), ())), preferred_element_type=jnp.float32)


NT = ((1,), (1,))
NN = ((1,), (0,))
TN = ((0,), (0,))


def front(
    queries, latent, rot_key, lat_gain, key_up, value_up, q_gain, k_gain, out_gain,
    out_weight, residual, ffn_gain, routes, weights, n_sp, n_z, width,
):
    heads, length = queries.shape[0] // QK, queries.shape[1]
    n_tp = 2 * n_z
    tok = residual.shape[0]
    part = n_z * tok
    cap = max(2, 9 * tok * TOPK // (8 * n_sp))
    rows = n_z * cap
    bundle = 2 * length + length // 2
    half = length // 2
    lanes = 128
    att_width = width
    qt = 256
    pt = 128
    per = lanes // tok
    named_rows = -(-n_sp // 8) * 8
    freqs = ROPE // 2
    inverse = np.float32(rope_base) ** (-np.arange(0, ROPE, 2, dtype=np.float32) / np.float32(ROPE))

    def kernel(
        q_in, lat_in, rot_in, latg, kup, vup, qg, kg, outg, w_hbm, res_in, ffng, routes_in,
        weights_in, out_rows, mixer, mid_out,
        table, gains, tokens, qbuf, kv, peak, total, acc, att, gath, normed, wbuf, resbuf, metabuf, mid, ffn,
        w_sem, local_sem, kv_s, kv_r, res_s, res_r, meta_s, meta_r, att_s, att_r,
    ):
        place = Place(n_sp, n_z)
        sp, core, z, tp = place.sp, place.core, place.z, place.tp
        load_w = pltpu.make_async_copy(w_hbm, wbuf, w_sem.at[0])
        load_w.start()
        sem = pltpu.get_barrier_semaphore()
        for step in range(1, n_tp):
            pl.semaphore_signal(
                sem, inc=1, device_id=(sp, lax.rem(tp + step, n_tp)), device_id_type=MESH_ID
            )
        for step in range(1, n_sp):
            pl.semaphore_signal(
                sem, inc=1, device_id=place.sp_id(place.sp_peer(step)), device_id_type=MESH_ID
            )

        tokens[0:1, :] = jnp.full((1, lanes), -1.0, jnp.float32)
        tokens[1:2, :] = jnp.full((1, lanes), -1.0, jnp.float32)
        tokens[0:TOPK, :tok] = routes_in[...].astype(jnp.float32)
        tokens[2:4, :tok] = weights_in[...]
        expert_id = lax.broadcasted_iota(jnp.int32, (named_rows, lanes), 0).astype(jnp.float32)
        named0 = expert_id == tokens[0:1, :]
        named1 = expert_id == tokens[1:2, :]
        named = jnp.where(named0 | named1, 1.0, 0.0)
        earlier = jnp.where(
            lax.broadcasted_iota(jnp.int32, (lanes, lanes), 0)
            < lax.broadcasted_iota(jnp.int32, (lanes, lanes), 1),
            1.0,
            0.0,
        ).astype(jnp.bfloat16)
        rank = split_dot(named.astype(jnp.bfloat16), earlier, NN)
        slot = jnp.where(named0 | named1, rank + (z * cap).astype(jnp.float32), -1.0)
        share = jnp.where(named0, tokens[2:3, :], 0.0) + jnp.where(named1, tokens[3:4, :], 0.0)
        place_by = lax.rem(z, per)
        for turn_by in range(per):

            @pl.when(place_by == turn_by)
            def _(turn_by=turn_by):
                metabuf[z, :named_rows] = pltpu.roll(slot, turn_by * tok, 1) if turn_by else slot
                metabuf[z, named_rows:] = pltpu.roll(share, turn_by * tok, 1) if turn_by else share

        freq_id = lax.broadcasted_iota(jnp.int32, (freqs, pt), 0)
        freq = jnp.zeros((freqs, pt), jnp.float32)
        for i in range(freqs):
            freq = jnp.where(freq_id == i, float(inverse[i]), freq)
        spread_by = jnp.where(
            lax.broadcasted_iota(jnp.int32, (freqs, lanes), 1) % freqs
            == lax.broadcasted_iota(jnp.int32, (freqs, lanes), 0),
            1.0,
            0.0,
        )

        def make_table(i, carry):
            where = lax.broadcasted_iota(jnp.int32, (freqs, pt), 1) + (sp * length + i * pt)
            angle = where.astype(jnp.float32) * freq
            at = pl.ds(pl.multiple_of(i * pt, pt), pt)
            for which, values in enumerate((jnp.cos(angle), jnp.sin(angle))):
                table[which, at, :] = lax.dot_general(
                    values, spread_by, (TN, ((), ())), precision=lax.Precision.HIGHEST,
                    preferred_element_type=jnp.float32,
                )
            return carry

        lax.fori_loop(0, length // pt, make_table, 0)
        for i, gain in enumerate((qg, kg)):
            gains[4 + i : 5 + i, :] = jnp.zeros((1, lanes), jnp.float32)
            gains[4 + i : 5 + i, :QK] = gain[...]
        gain_lane = lax.broadcasted_iota(jnp.int32, (1, lanes), 1)
        packed = []
        for i in range(2):
            raw_gain = gains[4 + i : 5 + i, :]
            nope_gain = jnp.where(gain_lane < NOPE, raw_gain, pltpu.roll(raw_gain, NOPE, 1))
            once = jnp.where(gain_lane < ROPE, pltpu.roll(raw_gain, lanes - NOPE, 1), 0.0)
            rot_gain = once
            for h in range(1, heads):
                rot_gain = rot_gain + pltpu.roll(once, h * ROPE, 1)
            packed.append((nope_gain, rot_gain))
        (q_nope_gain, q_rot_gain), (k_nope_gain, k_rot_gain) = packed

        pl.semaphore_wait(sem, n_tp - 1 + n_sp - 1)
        sends = []

        def push(src, dst, send, recv, device):
            copy = remote(src, dst, send, recv, device)
            copy.start()
            return copy

        res_copies, meta_copies = [], []
        for step in range(1, n_z):
            to = place.z_id(place.z_peer(step))
            meta_copies.append(
                push(metabuf.at[z], metabuf.at[z], meta_s.at[step], meta_r.at[step], to)
            )
        for step in range(1, n_z):
            to = place.z_id(place.z_peer(step))
            res_copies.append(push(res_in, resbuf.at[z], res_s.at[step], res_r.at[step], to))
        local = pltpu.make_async_copy(res_in, resbuf.at[z], local_sem.at[0])
        local.start()

        lane = lax.broadcasted_iota(jnp.int32, (1, lanes), 1)
        low = lane % ROPE < ROPE // 2
        mine = kv.at[sp]

        def turn(values, cos, sin):
            return (
                values * cos
                + pltpu.roll(values, lanes - ROPE // 2, 1) * jnp.where(low, -sin, 0.0)
                + pltpu.roll(values, ROPE // 2, 1) * jnp.where(low, 0.0, sin)
            )

        sel = lax.broadcasted_iota(jnp.int32, (ROPE, lanes), 0)
        rot_sel = jnp.where(
            (lax.broadcasted_iota(jnp.int32, (ROPE, lanes), 1) % ROPE == sel)
            & (lax.broadcasted_iota(jnp.int32, (ROPE, lanes), 1) < heads * ROPE),
            1.0,
            0.0,
        ).astype(jnp.bfloat16)
        rot_parts = length // pt

        def make_keys(i, carry):
            at = pl.ds(pl.multiple_of(i * pt, pt), pt)
            lat = lat_in[at, :].astype(jnp.float32)
            scale = lax.rsqrt(jnp.mean(lat * lat, axis=-1, keepdims=True) + epsilon)
            normed_lat = (lat * scale * latg[...]).astype(jnp.bfloat16)
            nope = split_dot(normed_lat, kup[...], NN).astype(jnp.bfloat16).astype(jnp.float32)
            vals = split_dot(normed_lat, vup[...], NN).astype(jnp.bfloat16)
            kv[sp, pl.ds(pl.multiple_of(length + i * pt, pt), pt), :] = vals
            rot = split_dot(rot_in[:, at], rot_sel, TN)
            square, rot_square = nope * nope, rot * rot
            nope_scale, rot_scale = None, None
            for h in range(heads):
                in_nope = (lane >= h * NOPE) & (lane < (h + 1) * NOPE)
                in_rot = (lane >= h * ROPE) & (lane < (h + 1) * ROPE)
                one = lax.rsqrt(
                    jnp.sum(
                        jnp.where(in_nope, square, 0.0) + jnp.where(in_rot, rot_square, 0.0),
                        axis=-1,
                        keepdims=True,
                    )
                    / QK
                    + epsilon
                )
                nope_scale = one if h == 0 else jnp.where(in_nope, one, nope_scale)
                rot_scale = one if h == 0 else jnp.where(in_rot, one, rot_scale)
            kv[sp, at, :] = (nope * nope_scale * k_nope_gain).astype(jnp.bfloat16)
            turned = turn(rot * rot_scale * k_rot_gain, table[0, at, :], table[1, at, :])
            return turned

        def make_pair(i, carry):
            first = make_keys(i, carry)
            second = make_keys(i + rot_parts // 2, carry)
            packed = first + pltpu.roll(second, 64, 1)
            kv[sp, pl.ds(pl.multiple_of(2 * length + i * pt, pt), pt), :] = packed.astype(
                jnp.bfloat16
            )
            return carry

        lax.fori_loop(0, rot_parts // 2, make_pair, 0)
        for step in range(1, n_sp):
            dst = sp + n_sp - step

            @pl.when(dst < n_sp)
            def _(dst=dst):
                push(mine, mine, kv_s.at[dst], kv_r.at[sp], place.sp_id(dst))

        wide = 2 * lanes
        src_id = lax.broadcasted_iota(jnp.int32, (heads * QK, wide), 0)
        dst_id = lax.broadcasted_iota(jnp.int32, (heads * QK, wide), 1)
        pickers = []
        for h in range(heads):
            entry = src_id - h * QK
            nope_hit = (entry >= 0) & (entry < NOPE) & (dst_id == h * NOPE + entry)
            rot_hit = (
                (entry >= NOPE) & (entry < QK) & (dst_id == lanes + h * ROPE + entry - NOPE)
            )
            pickers.append(jnp.where(nope_hit | rot_hit, 1.0, 0.0).astype(jnp.bfloat16))

        def make_queries(i, carry):
            at = pl.ds(pl.multiple_of(i * pt, pt), pt)
            raw = q_in[:, at]
            for h in range(heads):
                spread = split_dot(raw, pickers[h], TN)
                scale = lax.rsqrt(
                    jnp.sum(spread * spread, axis=-1, keepdims=True) / QK + epsilon
                )
                nope = (spread[:, :lanes] * scale * q_nope_gain).astype(jnp.bfloat16)
                rot = turn(spread[:, lanes:] * scale * q_rot_gain, table[0, at, :], table[1, at, :])
                qbuf[h, 0, at, :lanes] = nope
                qbuf[h, 1, at, :lanes] = nope
                qbuf[h, 0, at, lanes:] = rot.astype(jnp.bfloat16)
                qbuf[h, 1, at, lanes:] = pltpu.roll(rot, 64, 1).astype(jnp.bfloat16)
            return carry

        lax.fori_loop(0, length // pt, make_queries, 0)

        factor = QK ** (-0.5) * 1.4426950408889634

        def attend(src, first, diagonal):
            knope = [kv[src, s * half : (s + 1) * half, :] for s in range(2)]
            krot = kv[src, 2 * length : bundle, :]
            keys = [jnp.concatenate([knope[s], krot], axis=1) for s in range(2)]
            vals = kv[src, length : 2 * length, :]

            def tile(i, carry):
                at = pl.ds(pl.multiple_of(i * qt, qt), qt)
                outs = []
                for h in range(heads):
                    scores = jnp.concatenate(
                        [split_dot(qbuf[h, s, at, :], keys[s], NT) for s in range(2)], axis=1
                    )
                    scores = scores * factor
                    if diagonal:
                        row = lax.broadcasted_iota(jnp.int32, scores.shape, 0) + i * qt
                        col = lax.broadcasted_iota(jnp.int32, scores.shape, 1)
                        scores = jnp.where(col <= row, scores, -1e30)
                    top = jnp.max(scores, axis=-1, keepdims=True)
                    if not first:
                        old = peak[h, at, :]
                        top = jnp.maximum(old[:, :1], top)
                    weight = jnp.exp2(scores - top)
                    sums = jnp.sum(weight, axis=-1, keepdims=True)
                    part_out = split_dot(weight.astype(jnp.bfloat16), vals, NN)
                    if first:
                        total[h, at, :] = jnp.broadcast_to(sums, (qt, lanes))
                        outs.append((part_out, None))
                    else:
                        fade = jnp.exp2(old[:, :1] - top)
                        total[h, at, :] = total[h, at, :] * fade + sums
                        outs.append((part_out, fade))
                    peak[h, at, :] = jnp.broadcast_to(top, (qt, lanes))
                new, fade = outs[0]
                for h in range(1, heads):
                    new = jnp.where(lane >= h * VH, outs[h][0], new)
                    if not first:
                        fade = jnp.where(lane >= h * VH, outs[h][1], fade)
                acc[at, :] = new if first else acc[at, :] * fade + new
                return carry

            lax.fori_loop(0, length // qt, tile, 0)

        attend(sp, True, True)

        def visit(step, carry):
            src = sp - step

            @pl.when(src >= 0)
            def _():
                remote(
                    kv.at[src], kv.at[src], kv_s.at[src], kv_r.at[src], place.sp_id(src)
                ).wait_recv()
                attend(src, False, False)

            return carry

        lax.fori_loop(1, n_sp, visit, 0)

        for block in range(n_tp):
            at = pl.ds(block * tok, tok)
            bottom = total[0, at, :]
            for h in range(1, heads):
                bottom = jnp.where(lane >= h * VH, total[h, at, :], bottom)
            att[block % 2, (block // 2) * tok : (block // 2 + 1) * tok, :] = (
                acc[at, :] / bottom
            ).astype(jnp.bfloat16)
        att_copies = []
        for step in range(1, n_tp):
            dst = lax.rem(tp + step, n_tp)
            att_copies.append(
                push(
                    att.at[lax.rem(dst, 2)],
                    gath.at[tp],
                    att_s.at[step],
                    att_r.at[step],
                    (sp, dst),
                )
            )
        own = pltpu.make_async_copy(att.at[core], gath.at[tp], local_sem.at[1])
        own.start()

        for copy in meta_copies:
            copy.wait_recv()
        pieces = []
        for first in range(0, n_z, per):
            piece = metabuf[first]
            for i in range(1, per):
                piece = jnp.where(lane >= i * tok, metabuf[first + i], piece)
            pieces.append(piece)
        meta = jnp.concatenate(pieces, axis=1)
        slot_id = lax.broadcasted_iota(jnp.int32, (rows, part), 0).astype(jnp.float32)
        for e in range(n_sp):
            hit = meta[e : e + 1, :] == slot_id
            mixer[e] = jnp.where(
                hit, meta[named_rows + e : named_rows + e + 1, :], 0.0
            ).astype(jnp.bfloat16)
        for copy in res_copies:
            copy.wait_recv()
        local.wait()
        load_w.wait()
        own.wait()
        for copy in att_copies:
            copy.wait_recv()

        square = None
        for t in range(n_tp):
            block = gath[t].astype(jnp.float32)
            square = block * block if square is None else square + block * block
        scale = lax.rsqrt(jnp.sum(square, axis=-1, keepdims=True) / att_width + epsilon)
        for t in range(n_tp):
            normed[:, t * lanes : (t + 1) * lanes] = (
                gath[t].astype(jnp.float32) * scale * outg[t]
            ).astype(jnp.bfloat16)
        ct = 512
        square = None
        for c in range(D // ct):
            cols = slice(c * ct, (c + 1) * ct)
            values = split_dot(normed[...], wbuf[:, cols], NN) + resbuf[:, :, cols].reshape(
                part, ct
            ).astype(jnp.float32)
            mid[:, cols] = values
            more = jnp.sum(values * values, axis=-1, keepdims=True)
            square = more if square is None else square + more
        scale = lax.rsqrt(square / D + epsilon)
        for c in range(D // ct):
            cols = slice(c * ct, (c + 1) * ct)
            ffn[:, cols] = (mid[:, cols] * scale * ffng[0:1, cols]).astype(jnp.bfloat16)
        mid_out[...] = mid[pl.ds(pl.multiple_of(z * tok, tok), tok), :]
        for e in range(n_sp):
            hit = jnp.where(meta[e : e + 1, :] == slot_id, 1.0, 0.0).astype(jnp.bfloat16)
            for c in range(D // ct):
                cols = slice(c * ct, (c + 1) * ct)
                out_rows[e, :, cols] = split_dot(hit, ffn[:, cols], NN).astype(jnp.bfloat16)

        for copy in meta_copies + res_copies + att_copies:
            copy.wait_send()
        for step in range(1, n_sp):
            dst = sp + n_sp - step

            @pl.when(dst < n_sp)
            def _(dst=dst):
                remote(mine, mine, kv_s.at[dst], kv_r.at[sp], place.sp_id(dst)).wait_send()

    dma = pltpu.SemaphoreType.DMA
    bf, f4 = jnp.bfloat16, jnp.float32
    specs = [vmem()] * 9 + [pl.BlockSpec(memory_space=pl.ANY)] + [vmem()] * 4
    return pl.pallas_call(
        kernel,
        out_shape=(
            jax.ShapeDtypeStruct((n_sp, rows, D), bf),
            jax.ShapeDtypeStruct((n_sp, rows, part), bf),
            jax.ShapeDtypeStruct((tok, D), f4),
        ),
        in_specs=specs,
        out_specs=(vmem(),) * 3,
        scratch_shapes=[
            pltpu.VMEM((2, length, lanes), f4),
            pltpu.VMEM((8, lanes), f4),
            pltpu.VMEM((8, lanes), f4),
            pltpu.VMEM((heads, 2, length, 2 * lanes), bf),
            pltpu.VMEM((n_sp, bundle, lanes), bf),
            pltpu.VMEM((heads, length, lanes), f4),
            pltpu.VMEM((heads, length, lanes), f4),
            pltpu.VMEM((length, lanes), f4),
            pltpu.VMEM((2, part, lanes), bf),
            pltpu.VMEM((n_tp, part, lanes), bf),
            pltpu.VMEM((part, n_tp * lanes), bf),
            pltpu.VMEM(out_weight.shape, bf),
            pltpu.VMEM((n_z, tok, D), bf),
            pltpu.VMEM((n_z, 2 * named_rows, lanes), f4),
            pltpu.VMEM((part, D), f4),
            pltpu.VMEM((part, D), bf),
            dma((1,)),
            dma((2,)),
            dma((n_sp,)),
            dma((n_sp,)),
            dma((n_z,)),
            dma((n_z,)),
            dma((n_z,)),
            dma((n_z,)),
            dma((n_tp,)),
            dma((n_tp,)),
        ],
        compiler_params=pltpu.CompilerParams(
            collective_id=0, has_side_effects=True, vmem_limit_bytes=60 << 20
        ),
        name="front",
    )(
        queries, latent, rot_key, lat_gain, key_up, value_up, q_gain, k_gain, out_gain,
        out_weight, residual, ffn_gain, routes, weights,
    )


def shards(
    queries, latent, rot_key, latent_gain, key_up, value_up, query_gain, key_gain, out_gain,
    out_weight, residual, ffn_gain, routes, route_weights, expert_gate, expert_up, expert_down,
):
    heads = key_up.shape[1] // NOPE
    n_sp = lax.axis_size("sp")
    n_tp = lax.axis_size("tp")
    n_z = n_tp // 2
    width = heads * VH
    out_gain = out_gain.reshape(n_tp, 1, width)
    if width < 128:
        spare = 128 - width
        key_up = jnp.pad(key_up, ((0, 0), (0, spare)))
        value_up = jnp.pad(value_up, ((0, 0), (0, spare)))
        out_gain = jnp.pad(out_gain, ((0, 0), (0, 0), (0, spare)))
        out_weight = jnp.pad(
            out_weight.reshape(n_tp, width, D), ((0, 0), (0, spare), (0, 0))
        ).reshape(n_tp * 128, D)
    outbound, mixer, middle = front(
        queries.T, latent, rot_key.T, latent_gain[None, :], key_up, value_up,
        query_gain[None, :], key_gain[None, :], out_gain, out_weight,
        residual, ffn_gain[None, :], routes.T, route_weights.T, n_sp, n_z, n_tp * width,
    )
    return experts(
        outbound, mixer, middle, expert_gate[0], expert_up[0], expert_down[0], n_sp, n_z
    )


def solution(mesh):
    return jax.shard_map(
        shards,
        mesh=mesh,
        in_specs=(
            P("sp", "tp"),
            P("sp", None),
            P("sp", None),
            P(),
            P(None, "tp"),
            P(None, "tp"),
            P(),
            P(),
            P(),
            P(),
            P(("sp", "tp"), None),
            P(),
            P(("sp", "tp"), None),
            P(("sp", "tp"), None),
            P("sp", None, "tp"),
            P("sp", None, "tp"),
            P("sp", "tp", None),
        ),
        out_specs=P(("sp", "tp"), None),
        check_vma=False,
    )
```

```python
import jax
import jax.numpy as jnp
import numpy as np
from jax import lax
from jax.experimental import pallas as pl
from jax.experimental.pallas import tpu as pltpu
from jax.sharding import PartitionSpec as P

D = 2048
NOPE = 64
ROPE = 32
VH = 64
TOPK = 2
QK = 96

epsilon = 1e-06
rope_base = 10000.0
MESH_ID = pl.DeviceIdType.MESH


class Place:
    def __init__(self, n_sp, n_z):
        self.n_sp, self.n_z = n_sp, n_z
        self.sp = lax.axis_index("sp")
        self.tp = lax.axis_index("tp")
        self.core = lax.rem(self.tp, 2)
        self.z = lax.div(self.tp, 2)

    def partner(self):
        return (self.sp, self.tp + 1 - 2 * self.core)

    def sp_peer(self, step):
        return lax.rem(self.sp + step, self.n_sp)

    def z_peer(self, step):
        return lax.rem(self.z + step, self.n_z)

    def sp_id(self, index):
        return (index, self.tp)

    def z_id(self, index):
        return (self.sp, 2 * index + self.core)

    def barrier(self, use_sp, use_z):
        sem = pltpu.get_barrier_semaphore()
        count = 1
        pl.semaphore_signal(sem, inc=1, device_id=self.partner(), device_id_type=MESH_ID)
        if use_sp:
            for step in range(1, self.n_sp):
                pl.semaphore_signal(
                    sem, inc=1, device_id=self.sp_id(self.sp_peer(step)), device_id_type=MESH_ID
                )
            count += self.n_sp - 1
        if use_z:
            for step in range(1, self.n_z):
                pl.semaphore_signal(
                    sem, inc=1, device_id=self.z_id(self.z_peer(step)), device_id_type=MESH_ID
                )
            count += self.n_z - 1
        pl.semaphore_wait(sem, count)


def remote(src, dst, send, recv, device):
    return pltpu.make_async_remote_copy(
        src_ref=src,
        dst_ref=dst,
        send_sem=send,
        recv_sem=recv,
        device_id=device,
        device_id_type=MESH_ID,
    )


def vmem():
    return pl.BlockSpec(memory_space=pltpu.VMEM)


def flip(value, bits):
    shift = 1
    while shift <= bits:
        if bits & shift:
            value = value + shift * (1 - 2 * lax.rem(lax.div(value, shift), 2))
        shift *= 2
    return value


CHUNKS = 8
PIECES = 3
WIDE = 512
LEAD = 3


def expert_plan(rows, tok, gate, up, down, n_sp, n_z):
    width = D // CHUNKS
    hidden = gate.shape[1]
    shared = D // 4
    half = (D - shared) // 2
    piece = half // PIECES
    phases = [[1, 2]] + [[k] for k in range(3, n_sp)] if n_sp > 2 else [[1]]

    def loads_of(ins, scratch):
        return [
            pltpu.make_async_copy(src, dst, scratch[-9].at[i])
            for i, (src, dst) in enumerate(zip(ins, scratch[:3]))
        ]

    def body(place, given, ins, o_ref, scratch):
        x_in, mix_in, mid_in = given
        (
            gbuf, ubuf, dbuf, xbuf, hid, ybuf, pbuf, sbuf, rbuf, cbuf, fbuf,
            w_sem, sent, a_r, b_r, t_r, p_r, y_r, sp_r, z_r,
        ) = scratch
        core, z, me = place.core, place.z, place.sp
        loads = loads_of(ins, scratch)
        side = lax.rem(z, 2)
        twin = place.z_id(z + 1 - 2 * side)
        partner = place.partner()
        both = pl.ds(0, shared)

        def strip(which, p):
            return pl.ds(pl.multiple_of(shared + which * half + p * piece, 128), piece)

        def push(src, dst, kind, recv, device):
            copy = remote(src, dst, sent.at[kind], recv, device)
            copy.start()
            return copy

        push(x_in.at[me], xbuf.at[core, me], 3, p_r.at[0], partner)
        strips, shares, swaps = {}, {}, {}
        for ks in phases:
            for p in range(PIECES):
                for k in ks:
                    dst = flip(me, k)
                    cols = strip(side, p)
                    strips[k, p] = push(
                        x_in.at[dst, :, cols], xbuf.at[core, me, :, cols], 0, a_r.at[k, p],
                        place.sp_id(dst),
                    )
            for k in ks:
                dst = flip(me, k)
                shares[k] = push(
                    x_in.at[dst, :, both], xbuf.at[core, me, :, both], 1, b_r.at[k],
                    place.sp_id(dst),
                )

        def forward_strip(k, p):
            block = xbuf.at[core, flip(me, k), :, strip(side, p)]
            strips[k, p].wait_recv()
            swaps[k, p] = push(block, block, 2, t_r.at[k, p], twin)
            push(block, block, 3, p_r.at[k], partner)

        def forward_share(k):
            block = xbuf.at[core, flip(me, k), :, both]
            shares[k].wait_recv()
            push(block, block, 3, p_r.at[k], partner)

        def forward_swap(k, p):
            block = xbuf.at[core, flip(me, k), :, strip(1 - side, p)]
            swaps[k, p].wait_recv()
            push(block, block, 3, p_r.at[k], partner)

        def expert(x_ref, h_ref):
            g = jnp.dot(x_ref[...], gbuf[...], preferred_element_type=jnp.float32)
            u = jnp.dot(x_ref[...], ubuf[...], preferred_element_type=jnp.float32)
            h_ref[...] = (g / (1.0 + jnp.exp(-g)) * u).astype(jnp.bfloat16)

        def column(q):
            return pl.ds(pl.multiple_of(q * width, width), width)

        def back_copy(k, q):
            src = flip(me, k)
            return remote(
                pbuf.at[src, :, column(q)], rbuf.at[me, :, column(q)],
                sent.at[5], sp_r.at[k, q], place.sp_id(src),
            )

        def whole(k, buf, recv):
            block = buf.at[flip(me, k)]
            return remote(block, block, sent.at[4], recv.at[k], partner)

        def expert_own(k):
            src = flip(me, k)
            expert(x_in.at[me] if k == 0 else xbuf.at[core, src], hid.at[core, src])

        def expert_pair(k):
            src = flip(me, k)
            whole(k, xbuf.at[1 - core], p_r).wait_recv()
            expert(xbuf.at[1 - core, src], hid.at[1 - core, src])
            for w in range(D // WIDE):
                cols = slice(w * WIDE, (w + 1) * WIDE)
                ybuf[src, :, cols] = jnp.dot(
                    hid[1 - core, src], dbuf[:, cols], preferred_element_type=jnp.float32
                ).astype(jnp.bfloat16)
                remote(
                    ybuf.at[src, :, cols], pbuf.at[src, :, cols], sent.at[4], y_r.at[k], partner
                ).start()

        def down_own(k):
            src = flip(me, k)
            for w in range(D // WIDE):
                cols = slice(w * WIDE, (w + 1) * WIDE)
                sbuf[src, :, cols] = jnp.dot(
                    hid[core, src], dbuf[:, cols], preferred_element_type=jnp.float32
                ).astype(jnp.bfloat16)

        def settle(k, q):
            src = flip(me, k)
            total = sbuf[src, :, column(q)].astype(jnp.float32) + pbuf[
                src, :, column(q)
            ].astype(jnp.float32)
            if k == 0:
                rbuf[src, :, column(q)] = total.astype(jnp.bfloat16)
            else:
                pbuf[src, :, column(q)] = total.astype(jnp.bfloat16)
                back_copy(k, q).start()

        def finish(ks, first, last):
            def body(q, carry):
                for k in ks:
                    settle(k, q)
                return carry

            lax.fori_loop(first, last, body, 0)

        def take_pair(ks):
            for k in ks:
                whole(k, pbuf, y_r).wait_recv()

        def arrivals(ks):
            steps = []
            for p in range(PIECES):
                steps.append(lambda p=p: [forward_strip(k, p) for k in ks])
            steps.append(lambda: [forward_share(k) for k in ks])
            return steps

        for load in loads[:2]:
            load.wait()
        waiting = arrivals(phases[0])
        expert_own(0)
        waiting.pop(0)()
        loads[2].wait()
        expert_pair(0)
        waiting.pop(0)()
        down_own(0)
        take_pair([0])
        finish([0], 0, CHUNKS)
        for index, ks in enumerate(phases):
            while waiting:
                waiting.pop(0)()
            waiting = arrivals(phases[index + 1]) if index + 1 < len(phases) else []
            for p in range(PIECES):
                for k in ks:
                    forward_swap(k, p)
                if waiting and p < 2:
                    waiting.pop(0)()
            for k in ks:
                expert_own(k)
            for k in ks:
                down_own(k)
            for k in ks:
                expert_pair(k)
                if waiting:
                    waiting.pop(0)()
            take_pair(ks)
            if index + 1 == len(phases) and index:

                def last(q, carry, ks=ks):
                    for k in ks:
                        settle(k, q)
                    for k in phases[-2]:
                        settle(k, q + LEAD)
                    return carry

                lax.fori_loop(0, CHUNKS - LEAD, last, 0)
                finish(ks, CHUNKS - LEAD, CHUNKS)
            else:
                finish(ks, 0, LEAD if index + 2 == len(phases) else CHUNKS)

        def z_copy(q, step):
            dst = place.z_peer(step)
            return remote(
                cbuf.at[dst, :, column(q)], fbuf.at[z, :, column(q)],
                sent.at[6], z_r.at[q, step], place.z_id(dst),
            )

        def combine(q, carry):
            for k in range(1, n_sp):
                back_copy(k, q).wait_recv()
            total = None
            for src in range(n_sp):
                more = split_dot(mix_in[src], rbuf[src, :, column(q)], TN)
                total = more if total is None else total + more
            cbuf[:, :, column(q)] = total.astype(jnp.bfloat16).reshape(n_z, tok, width)
            for step in range(1, n_z):
                z_copy(q, step).start()
            return carry

        lax.fori_loop(0, CHUNKS, combine, 0)

        def close(q, carry):
            total = mid_in[:, column(q)] + cbuf[z, :, column(q)].astype(jnp.float32)
            for step in range(1, n_z):
                z_copy(q, step).wait_recv()
                total += fbuf[lax.rem(z - step + n_z, n_z), :, column(q)].astype(jnp.float32)
            o_ref[:, column(q)] = total.astype(jnp.bfloat16)
            return carry

        lax.fori_loop(0, CHUNKS, close, 0)

        others = pl.ds(0, n_sp - 1)
        strip_bytes = xbuf.at[0, others, :, pl.ds(shared, half)]
        for kind, block in enumerate(
            (
                strip_bytes, xbuf.at[0, others, :, both], strip_bytes, ybuf, ybuf,
                ybuf.at[others], fbuf.at[pl.ds(0, n_z - 1)],
            )
        ):
            remote(block, block, sent.at[kind], z_r.at[0, 0], partner).wait_send()

    dma = pltpu.SemaphoreType.DMA
    bf = jnp.bfloat16
    block = pltpu.VMEM((n_sp, rows, D), bf)
    zblock = pltpu.VMEM((n_z, tok, D), bf)
    return dict(
        body=body,
        loads=loads_of,
        ins=(gate, up, down),
        scratch=[
            pltpu.VMEM(gate.shape, bf),
            pltpu.VMEM(up.shape, bf),
            pltpu.VMEM(down.shape, bf),
            pltpu.VMEM((2, n_sp, rows, D), bf),
            pltpu.VMEM((2, n_sp, rows, hidden), bf),
            block, block, block, block, zblock, zblock,
            dma((3,)),
            dma((7,)),
            dma((n_sp, PIECES)),
            dma((n_sp,)),
            dma((n_sp, PIECES)),
            dma((n_sp,)),
            dma((n_sp,)),
            dma((n_sp, CHUNKS)),
            dma((CHUNKS, n_z)),
        ],
    )


VMEM_ROOM = 63 << 20


def run_plans(first, second, tok, n_sp, n_z):
    hbm = pl.BlockSpec(memory_space=pl.ANY)
    out_shape = jax.ShapeDtypeStruct((tok, D), jnp.bfloat16)
    n_ins, n_first, n_given = len(first["ins"]), len(first["scratch"]), len(first["outs"])
    given = [pltpu.VMEM(shape, dtype) for shape, dtype in first["outs"]]
    sizes = first["scratch"] + second["scratch"] + given
    need = sum(
        int(np.prod(one.inner_aval.shape)) * one.inner_aval.dtype.itemsize
        for one in sizes
        if "vmem" in str(one.memory_space)
    )

    def params(number, room):
        return pltpu.CompilerParams(
            collective_id=number, has_side_effects=True, vmem_limit_bytes=room
        )

    def merged(*refs):
        place = Place(n_sp, n_z)
        ins, weights, refs = refs[:n_ins], refs[n_ins : n_ins + 3], refs[n_ins + 3 :]
        o_ref, held, refs = refs[0], refs[1 : 1 + n_given], refs[1 + n_given :]
        drain = first["body"](place, ins, held, refs[:n_first], second["loads"](weights, refs[n_first:]))
        second["body"](place, held, weights, o_ref, refs[n_first:])
        drain()

    if need < 52 << 20:
        return pl.pallas_call(
            merged,
            out_shape=out_shape,
            in_specs=first["in_specs"] + [hbm] * 3,
            out_specs=vmem(),
            scratch_shapes=given + first["scratch"] + second["scratch"],
            compiler_params=params(0, VMEM_ROOM),
            name="layer",
        )(*first["ins"], *second["ins"])

    def head(*refs):
        place = Place(n_sp, n_z)
        ins, outs = refs[:n_ins], refs[n_ins : n_ins + n_given]
        first["body"](place, ins, outs, refs[n_ins + n_given :], [])()

    def tail(*refs):
        place = Place(n_sp, n_z)
        scratch = refs[n_given + 4 :]
        for load in second["loads"](refs[n_given : n_given + 3], scratch):
            load.start()
        place.barrier(True, True)
        second["body"](
            place, refs[:n_given], refs[n_given : n_given + 3], refs[n_given + 3], scratch
        )

    held = pl.pallas_call(
        head,
        out_shape=tuple(jax.ShapeDtypeStruct(*one) for one in first["outs"]),
        in_specs=first["in_specs"],
        out_specs=(vmem(),) * n_given,
        scratch_shapes=first["scratch"],
        compiler_params=params(0, VMEM_ROOM),
        name="front",
    )(*first["ins"])
    return pl.pallas_call(
        tail,
        out_shape=out_shape,
        in_specs=[vmem()] * n_given + [hbm] * 3,
        out_specs=vmem(),
        scratch_shapes=second["scratch"],
        compiler_params=params(1, VMEM_ROOM),
        name="experts",
    )(*held, *second["ins"])


RES_PARTS = 4


def split_dot(a, b, dims):
    return lax.dot_general(a, b, (dims, ((), ())), preferred_element_type=jnp.float32)


NT = ((1,), (1,))
NN = ((1,), (0,))
TN = ((0,), (0,))


def front_plan(
    queries, latent, rot_key, lat_gain, key_up, value_up, q_gain, k_gain, out_gain,
    out_weight, residual, ffn_gain, routes, weights, n_sp, n_z, width,
):
    heads, length = queries.shape[0] // QK, queries.shape[1]
    n_tp = 2 * n_z
    tok = residual.shape[0]
    part = n_z * tok
    cap = max(2, 9 * tok * TOPK // (8 * n_sp))
    rows = n_z * cap
    bundle = 2 * length + length // 2
    half = length // 2
    lanes = 128
    att_width = width
    qt = 256
    pt = 128
    per = lanes // tok
    named_rows = -(-n_sp // 8) * 8
    freqs = ROPE // 2
    inverse = np.float32(rope_base) ** (-np.arange(0, ROPE, 2, dtype=np.float32) / np.float32(ROPE))

    def body(place, ins, outs, scratch, more_loads):
        (
            q_hbm, lat_hbm, rot_in, latg, kup_hbm, vup_hbm, qg, kg, outg, w_hbm, res_hbm, ffng,
            routes_in, weights_in,
        ) = ins
        out_rows, mixer, mid_out = outs
        (
            q_in, lat_in, kup, vup, table, gains, tokens, qbuf, kv, peak, total, acc, att, gath,
            normed, wbuf, resbuf, metabuf, mid, ffn, load_sem, sent, kv_s, kv_r, res_r, meta_r,
            att_r,
        ) = scratch
        sp, core, z, tp = place.sp, place.core, place.z, place.tp
        sem = pltpu.get_barrier_semaphore()
        for step in range(1, n_tp):
            pl.semaphore_signal(
                sem, inc=1, device_id=(sp, lax.rem(tp + step, n_tp)), device_id_type=MESH_ID
            )
        for step in range(1, n_sp):
            pl.semaphore_signal(
                sem, inc=1, device_id=place.sp_id(place.sp_peer(step)), device_id_type=MESH_ID
            )
        loads = []
        for i, (src, dst) in enumerate(
            (
                (lat_hbm, lat_in), (kup_hbm, kup), (vup_hbm, vup), (q_hbm, q_in),
                (res_hbm, resbuf.at[z]), (w_hbm, wbuf),
            )
        ):
            load = pltpu.make_async_copy(src, dst, load_sem.at[i])
            load.start()
            loads.append(load)
        for load in more_loads:
            load.start()

        tokens[0:1, :] = jnp.full((1, lanes), -1.0, jnp.float32)
        tokens[1:2, :] = jnp.full((1, lanes), -1.0, jnp.float32)
        tokens[0:TOPK, :tok] = routes_in[...].astype(jnp.float32)
        tokens[2:4, :tok] = weights_in[...]
        expert_id = lax.broadcasted_iota(jnp.int32, (named_rows, lanes), 0).astype(jnp.float32)
        named0 = expert_id == tokens[0:1, :]
        named1 = expert_id == tokens[1:2, :]
        named = jnp.where(named0 | named1, 1.0, 0.0)
        earlier = jnp.where(
            lax.broadcasted_iota(jnp.int32, (lanes, lanes), 0)
            < lax.broadcasted_iota(jnp.int32, (lanes, lanes), 1),
            1.0,
            0.0,
        ).astype(jnp.bfloat16)
        rank = split_dot(named.astype(jnp.bfloat16), earlier, NN)
        slot = jnp.where(named0 | named1, rank + (z * cap).astype(jnp.float32), -1.0)
        share = jnp.where(named0, tokens[2:3, :], 0.0) + jnp.where(named1, tokens[3:4, :], 0.0)
        place_by = lax.rem(z, per)
        for turn_by in range(per):

            @pl.when(place_by == turn_by)
            def _(turn_by=turn_by):
                metabuf[z, :named_rows] = pltpu.roll(slot, turn_by * tok, 1) if turn_by else slot
                metabuf[z, named_rows:] = pltpu.roll(share, turn_by * tok, 1) if turn_by else share

        freq_id = lax.broadcasted_iota(jnp.int32, (freqs, length), 0)
        freq = jnp.zeros((freqs, length), jnp.float32)
        for i in range(freqs):
            freq = jnp.where(freq_id == i, float(inverse[i]), freq)
        where = lax.broadcasted_iota(jnp.int32, (freqs, length), 1) + sp * length
        angle = where.astype(jnp.float32) * freq
        spread_by = jnp.where(
            lax.broadcasted_iota(jnp.int32, (freqs, lanes), 1) % freqs
            == lax.broadcasted_iota(jnp.int32, (freqs, lanes), 0),
            1.0,
            0.0,
        )

        for which, values in enumerate((jnp.cos(angle), jnp.sin(angle))):
            table[which] = lax.dot_general(
                values, spread_by, (TN, ((), ())), precision=lax.Precision.HIGHEST,
                preferred_element_type=jnp.float32,
            )
        for i, gain in enumerate((qg, kg)):
            gains[4 + i : 5 + i, :] = jnp.zeros((1, lanes), jnp.float32)
            gains[4 + i : 5 + i, :QK] = gain[...]
        gain_lane = lax.broadcasted_iota(jnp.int32, (1, lanes), 1)
        packed = []
        for i in range(2):
            raw_gain = gains[4 + i : 5 + i, :]
            nope_gain = jnp.where(gain_lane < NOPE, raw_gain, pltpu.roll(raw_gain, NOPE, 1))
            once = jnp.where(gain_lane < ROPE, pltpu.roll(raw_gain, lanes - NOPE, 1), 0.0)
            rot_gain = once
            for h in range(1, heads):
                rot_gain = rot_gain + pltpu.roll(once, h * ROPE, 1)
            packed.append((nope_gain, rot_gain))
        (q_nope_gain, q_rot_gain), (k_nope_gain, k_rot_gain) = packed

        pl.semaphore_wait(sem, n_tp - 1 + n_sp - 1)
        def push(src, dst, kind, recv, device):
            copy = remote(src, dst, sent.at[kind], recv, device)
            copy.start()
            return copy

        parts = [slice(i * D // RES_PARTS, (i + 1) * D // RES_PARTS) for i in range(RES_PARTS)]

        def res_copy(src, i, to, src_ref=None):
            block = resbuf.at[src, :, parts[i]]
            from_ref = block if src_ref is None else src_ref.at[:, parts[i]]
            return remote(
                from_ref, block, sent.at[0], res_r.at[src, i], place.z_id(to)
            )

        for i in range(RES_PARTS):
            for away in (2, -2, 1, -1):
                to = z + away

                @pl.when((to >= 0) & (to < n_z))
                def _(to=to, i=i):
                    res_copy(z, i, to, res_hbm).start()

        for step in range(1, n_z):
            to = place.z_id(place.z_peer(step))
            push(metabuf.at[z], metabuf.at[z], 1, meta_r.at[z], to)

        def pass_on(away, i):
            for sign in (1, -1):
                src, to = z - sign * away, z + sign

                @pl.when((src >= 0) & (src < n_z) & (to >= 0) & (to < n_z))
                def _(src=src, to=to):
                    res_copy(src, i, z).wait_recv()
                    res_copy(src, i, to).start()

        lane = lax.broadcasted_iota(jnp.int32, (1, lanes), 1)
        low = lane % ROPE < ROPE // 2
        mine = kv.at[sp]
        for load in loads[:3]:
            load.wait()

        def turn(values, cos, sin):
            return (
                values * cos
                + pltpu.roll(values, lanes - ROPE // 2, 1) * jnp.where(low, -sin, 0.0)
                + pltpu.roll(values, ROPE // 2, 1) * jnp.where(low, 0.0, sin)
            )

        sel = lax.broadcasted_iota(jnp.int32, (ROPE, lanes), 0)
        rot_sel = jnp.where(
            (lax.broadcasted_iota(jnp.int32, (ROPE, lanes), 1) % ROPE == sel)
            & (lax.broadcasted_iota(jnp.int32, (ROPE, lanes), 1) < heads * ROPE),
            1.0,
            0.0,
        ).astype(jnp.bfloat16)
        rot_parts = length // pt

        def make_keys(i, carry):
            at = pl.ds(pl.multiple_of(i * pt, pt), pt)
            lat = lat_in[at, :].astype(jnp.float32)
            scale = lax.rsqrt(jnp.mean(lat * lat, axis=-1, keepdims=True) + epsilon)
            normed_lat = (lat * scale * latg[...]).astype(jnp.bfloat16)
            nope = split_dot(normed_lat, kup[...], NN).astype(jnp.bfloat16).astype(jnp.float32)
            vals = split_dot(normed_lat, vup[...], NN).astype(jnp.bfloat16)
            kv[sp, pl.ds(pl.multiple_of(length + i * pt, pt), pt), :] = vals
            rot = split_dot(rot_in[:, at], rot_sel, TN)
            square, rot_square = nope * nope, rot * rot
            nope_scale, rot_scale = None, None
            for h in range(heads):
                in_nope = (lane >= h * NOPE) & (lane < (h + 1) * NOPE)
                in_rot = (lane >= h * ROPE) & (lane < (h + 1) * ROPE)
                one = lax.rsqrt(
                    jnp.sum(
                        jnp.where(in_nope, square, 0.0) + jnp.where(in_rot, rot_square, 0.0),
                        axis=-1,
                        keepdims=True,
                    )
                    / QK
                    + epsilon
                )
                nope_scale = one if h == 0 else jnp.where(in_nope, one, nope_scale)
                rot_scale = one if h == 0 else jnp.where(in_rot, one, rot_scale)
            kv[sp, at, :] = (nope * nope_scale * k_nope_gain).astype(jnp.bfloat16)
            turned = turn(rot * rot_scale * k_rot_gain, table[0, at, :], table[1, at, :])
            return turned

        def make_pair(i, carry):
            first = make_keys(i, carry)
            second = make_keys(i + rot_parts // 2, carry)
            packed = first + pltpu.roll(second, 64, 1)
            kv[sp, pl.ds(pl.multiple_of(2 * length + i * pt, pt), pt), :] = packed.astype(
                jnp.bfloat16
            )
            return carry

        lax.fori_loop(0, rot_parts // 2, make_pair, 0)
        for step in range(1, n_sp):
            dst = sp + n_sp - step

            @pl.when(dst < n_sp)
            def _(dst=dst):
                remote(mine, mine, kv_s.at[dst], kv_r.at[sp], place.sp_id(dst)).start()

        wide = 2 * lanes
        src_id = lax.broadcasted_iota(jnp.int32, (heads * QK, wide), 0)
        dst_id = lax.broadcasted_iota(jnp.int32, (heads * QK, wide), 1)
        pickers = []
        for h in range(heads):
            entry = src_id - h * QK
            nope_hit = (entry >= 0) & (entry < NOPE) & (dst_id == h * NOPE + entry)
            rot_hit = (
                (entry >= NOPE) & (entry < QK) & (dst_id == lanes + h * ROPE + entry - NOPE)
            )
            pickers.append(jnp.where(nope_hit | rot_hit, 1.0, 0.0).astype(jnp.bfloat16))

        loads[3].wait()

        def make_queries(i, carry):
            at = pl.ds(pl.multiple_of(i * pt, pt), pt)
            raw = q_in[:, at]
            for h in range(heads):
                spread = split_dot(raw, pickers[h], TN)
                scale = lax.rsqrt(
                    jnp.sum(spread * spread, axis=-1, keepdims=True) / QK + epsilon
                )
                nope = (spread[:, :lanes] * scale * q_nope_gain).astype(jnp.bfloat16)
                rot = turn(spread[:, lanes:] * scale * q_rot_gain, table[0, at, :], table[1, at, :])
                qbuf[h, 0, at, :lanes] = nope
                qbuf[h, 1, at, :lanes] = nope
                qbuf[h, 0, at, lanes:] = rot.astype(jnp.bfloat16)
                qbuf[h, 1, at, lanes:] = pltpu.roll(rot, 64, 1).astype(jnp.bfloat16)
            return carry

        lax.fori_loop(0, length // pt, make_queries, 0)

        factor = QK ** (-0.5) * 1.4426950408889634

        def attend(src, first, diagonal):
            knope = [kv[src, s * half : (s + 1) * half, :] for s in range(2)]
            krot = kv[src, 2 * length : bundle, :]
            keys = [jnp.concatenate([knope[s], krot], axis=1) for s in range(2)]
            vals = kv[src, length : 2 * length, :]

            def tile(i, carry):
                at = pl.ds(pl.multiple_of(i * qt, qt), qt)
                outs = []
                for h in range(heads):
                    scores = jnp.concatenate(
                        [split_dot(qbuf[h, s, at, :], keys[s], NT) for s in range(2)], axis=1
                    )
                    scores = scores * factor
                    if diagonal:
                        row = lax.broadcasted_iota(jnp.int32, scores.shape, 0) + i * qt
                        col = lax.broadcasted_iota(jnp.int32, scores.shape, 1)
                        scores = jnp.where(col <= row, scores, -1e30)
                    top = jnp.max(scores, axis=-1, keepdims=True)
                    if not first:
                        old = peak[h, at, :]
                        top = jnp.maximum(old[:, :1], top)
                    weight = jnp.exp2(scores - top)
                    sums = jnp.sum(weight, axis=-1, keepdims=True)
                    part_out = split_dot(weight.astype(jnp.bfloat16), vals, NN)
                    if first:
                        total[h, at, :] = jnp.broadcast_to(sums, (qt, lanes))
                        outs.append((part_out, None))
                    else:
                        fade = jnp.exp2(old[:, :1] - top)
                        total[h, at, :] = total[h, at, :] * fade + sums
                        outs.append((part_out, fade))
                    peak[h, at, :] = jnp.broadcast_to(top, (qt, lanes))
                new, fade = outs[0]
                for h in range(1, heads):
                    new = jnp.where(lane >= h * VH, outs[h][0], new)
                    if not first:
                        fade = jnp.where(lane >= h * VH, outs[h][1], fade)
                acc[at, :] = new if first else acc[at, :] * fade + new
                return carry

            lax.fori_loop(0, length // qt, tile, 0)

        attend(sp, True, True)

        def visit(step, carry):
            src = sp - step

            @pl.when(src >= 0)
            def _():
                remote(
                    kv.at[src], kv.at[src], kv_s.at[src], kv_r.at[src], place.sp_id(src)
                ).wait_recv()
                attend(src, False, False)

            return carry

        hops = [(away, i) for away in range(2, n_z - 1) for i in range(RES_PARTS)]
        head = RES_PARTS // 2
        for away, i in hops[:head]:
            pass_on(away, i)
        lax.fori_loop(1, 2, visit, 0)
        for away, i in hops[head:RES_PARTS]:
            pass_on(away, i)
        lax.fori_loop(2, n_sp, visit, 0)
        for away, i in hops[RES_PARTS:]:
            pass_on(away, i)

        for block in range(n_tp):
            at = pl.ds(block * tok, tok)
            bottom = total[0, at, :]
            for h in range(1, heads):
                bottom = jnp.where(lane >= h * VH, total[h, at, :], bottom)
            att[block % 2, (block // 2) * tok : (block // 2 + 1) * tok, :] = (
                acc[at, :] / bottom
            ).astype(jnp.bfloat16)
        for step in range(n_tp - 1, 0, -1):
            dst = lax.rem(tp + step, n_tp)
            push(att.at[lax.rem(dst, 2)], gath.at[tp], 2, att_r.at[tp], (sp, dst))
        own = pltpu.make_async_copy(att.at[core], gath.at[tp], load_sem.at[6])
        own.start()

        partner = place.partner()
        for step in range(1, n_z):
            block = metabuf.at[place.z_peer(step)]
            remote(block, block, sent.at[1], meta_r.at[place.z_peer(step)], partner).wait_recv()
        pieces = []
        for first in range(0, n_z, per):
            piece = metabuf[first]
            for i in range(1, per):
                piece = jnp.where(lane >= i * tok, metabuf[first + i], piece)
            pieces.append(piece)
        meta = jnp.concatenate(pieces, axis=1)
        slot_id = lax.broadcasted_iota(jnp.int32, (rows, part), 0).astype(jnp.float32)
        for e in range(n_sp):
            hit = meta[e : e + 1, :] == slot_id
            mixer[e] = jnp.where(
                hit, meta[named_rows + e : named_rows + e + 1, :], 0.0
            ).astype(jnp.bfloat16)
        for i in range(RES_PARTS):
            for src in range(n_z):
                away = z - src
                passed = ((away >= 2) & (z + 1 < n_z)) | ((away <= -2) & (z > 0))

                @pl.when((away != 0) & jnp.logical_not(passed))
                def _(src=src, i=i):
                    res_copy(src, i, z).wait_recv()

        for load in loads[4:]:
            load.wait()
        own.wait()
        for step in range(1, n_tp):
            src = lax.rem(tp + step, n_tp)
            block = gath.at[src]
            remote(block, block, sent.at[2], att_r.at[src], partner).wait_recv()
        square = None
        for t in range(n_tp):
            block = gath[t].astype(jnp.float32)
            square = block * block if square is None else square + block * block
        scale = lax.rsqrt(jnp.sum(square, axis=-1, keepdims=True) / att_width + epsilon)
        for t in range(n_tp):
            normed[:, t * lanes : (t + 1) * lanes] = (
                gath[t].astype(jnp.float32) * scale * outg[t]
            ).astype(jnp.bfloat16)
        ct = 512
        square = None
        for c in range(D // ct):
            cols = slice(c * ct, (c + 1) * ct)
            values = split_dot(normed[...], wbuf[:, cols], NN) + resbuf[:, :, cols].reshape(
                part, ct
            ).astype(jnp.float32)
            mid[:, cols] = values
            more = jnp.sum(values * values, axis=-1, keepdims=True)
            square = more if square is None else square + more
        scale = lax.rsqrt(square / D + epsilon)
        for c in range(D // ct):
            cols = slice(c * ct, (c + 1) * ct)
            ffn[:, cols] = (mid[:, cols] * scale * ffng[0:1, cols]).astype(jnp.bfloat16)
        mid_out[...] = mid[pl.ds(pl.multiple_of(z * tok, tok), tok), :]
        for e in range(n_sp):
            hit = jnp.where(meta[e : e + 1, :] == slot_id, 1.0, 0.0).astype(jnp.bfloat16)
            for c in range(D // ct):
                cols = slice(c * ct, (c + 1) * ct)
                out_rows[e, :, cols] = split_dot(hit, ffn[:, cols], NN).astype(jnp.bfloat16)

        def drain():
            for i in range(RES_PARTS):
                block = resbuf.at[0, :, parts[i]]
                one = remote(block, block, sent.at[0], res_r.at[0, 0], partner)
                for away in (2, -2, 1, -1):

                    @pl.when((z + away >= 0) & (z + away < n_z))
                    def _(one=one):
                        one.wait_send()

            for away, i in hops:
                block = resbuf.at[0, :, parts[i]]
                one = remote(block, block, sent.at[0], res_r.at[0, 0], partner)
                for sign in (1, -1):
                    src, to = z - sign * away, z + sign

                    @pl.when((src >= 0) & (src < n_z) & (to >= 0) & (to < n_z))
                    def _(one=one):
                        one.wait_send()

            block = metabuf.at[pl.ds(0, n_z - 1)]
            remote(block, block, sent.at[1], meta_r.at[0], partner).wait_send()
            block = gath.at[pl.ds(0, n_tp - 1)]
            remote(block, block, sent.at[2], att_r.at[0], partner).wait_send()
            for step in range(1, n_sp):
                dst = sp + n_sp - step

                @pl.when(dst < n_sp)
                def _(dst=dst):
                    remote(mine, mine, kv_s.at[dst], kv_r.at[sp], place.sp_id(dst)).wait_send()

        return drain

    dma = pltpu.SemaphoreType.DMA
    bf, f4 = jnp.bfloat16, jnp.float32
    hbm = pl.BlockSpec(memory_space=pl.ANY)
    return dict(
        body=body,
        ins=(
            queries, latent, rot_key, lat_gain, key_up, value_up, q_gain, k_gain, out_gain,
            out_weight, residual, ffn_gain, routes, weights,
        ),
        in_specs=[
            hbm, hbm, vmem(), vmem(), hbm, hbm, vmem(), vmem(), vmem(), hbm, hbm, vmem(),
            vmem(), vmem(),
        ],
        outs=[((n_sp, rows, D), bf), ((n_sp, rows, part), bf), ((tok, D), f4)],
        scratch=[
            pltpu.VMEM(queries.shape, bf),
            pltpu.VMEM(latent.shape, bf),
            pltpu.VMEM(key_up.shape, bf),
            pltpu.VMEM(value_up.shape, bf),
            pltpu.VMEM((2, length, lanes), f4),
            pltpu.VMEM((8, lanes), f4),
            pltpu.VMEM((8, lanes), f4),
            pltpu.VMEM((heads, 2, length, 2 * lanes), bf),
            pltpu.VMEM((n_sp, bundle, lanes), bf),
            pltpu.VMEM((heads, length, lanes), f4),
            pltpu.VMEM((heads, length, lanes), f4),
            pltpu.VMEM((length, lanes), f4),
            pltpu.VMEM((2, part, lanes), bf),
            pltpu.VMEM((n_tp, part, lanes), bf),
            pltpu.VMEM((part, n_tp * lanes), bf),
            pltpu.VMEM(out_weight.shape, bf),
            pltpu.VMEM((n_z, tok, D), bf),
            pltpu.VMEM((n_z, 2 * named_rows, lanes), f4),
            pltpu.VMEM((part, D), f4),
            pltpu.VMEM((part, D), bf),
            dma((7,)),
            dma((3,)),
            dma((n_sp,)),
            dma((n_sp,)),
            dma((n_z, RES_PARTS)),
            dma((n_z,)),
            dma((n_tp,)),
        ],
    )


def shards(
    queries, latent, rot_key, latent_gain, key_up, value_up, query_gain, key_gain, out_gain,
    out_weight, residual, ffn_gain, routes, route_weights, expert_gate, expert_up, expert_down,
):
    heads = key_up.shape[1] // NOPE
    n_sp = lax.axis_size("sp")
    n_tp = lax.axis_size("tp")
    n_z = n_tp // 2
    width = heads * VH
    out_gain = out_gain.reshape(n_tp, 1, width)
    if width < 128:
        spare = 128 - width
        key_up = jnp.pad(key_up, ((0, 0), (0, spare)))
        value_up = jnp.pad(value_up, ((0, 0), (0, spare)))
        out_gain = jnp.pad(out_gain, ((0, 0), (0, 0), (0, spare)))
        out_weight = jnp.pad(
            out_weight.reshape(n_tp, width, D), ((0, 0), (0, spare), (0, 0))
        ).reshape(n_tp * 128, D)
    first = front_plan(
        queries.T, latent, rot_key.T, latent_gain[None, :], key_up, value_up,
        query_gain[None, :], key_gain[None, :], out_gain, out_weight,
        residual, ffn_gain[None, :], routes.T, route_weights.T, n_sp, n_z, n_tp * width,
    )
    cap = max(2, 9 * residual.shape[0] * TOPK // (8 * n_sp))
    second = expert_plan(
        n_z * cap, residual.shape[0], expert_gate[0], expert_up[0], expert_down[0], n_sp, n_z
    )
    return run_plans(first, second, residual.shape[0], n_sp, n_z)


def solution(mesh):
    return jax.shard_map(
        shards,
        mesh=mesh,
        in_specs=(
            P("sp", "tp"),
            P("sp", None),
            P("sp", None),
            P(),
            P(None, "tp"),
            P(None, "tp"),
            P(),
            P(),
            P(),
            P(),
            P(("sp", "tp"), None),
            P(),
            P(("sp", "tp"), None),
            P(("sp", "tp"), None),
            P("sp", None, "tp"),
            P("sp", None, "tp"),
            P("sp", "tp", None),
        ),
        out_specs=P(("sp", "tp"), None),
        check_vma=False,
    )
```

```python
import jax
import jax.numpy as jnp
import numpy as np
from jax import lax
from jax.experimental import pallas as pl
from jax.experimental.pallas import tpu as pltpu
from jax.sharding import PartitionSpec as P

D = 2048
NOPE = 64
ROPE = 32
VH = 64
TOPK = 2
QK = 96

epsilon = 1e-06
rope_base = 10000.0
MESH_ID = pl.DeviceIdType.MESH


class Place:
    def __init__(self, n_sp, n_z):
        self.n_sp, self.n_z = n_sp, n_z
        self.sp = lax.axis_index("sp")
        self.tp = lax.axis_index("tp")
        self.core = lax.rem(self.tp, 2)
        self.z = lax.div(self.tp, 2)

    def partner(self):
        return (self.sp, self.tp + 1 - 2 * self.core)

    def sp_peer(self, step):
        return lax.rem(self.sp + step, self.n_sp)

    def z_peer(self, step):
        return lax.rem(self.z + step, self.n_z)

    def sp_id(self, index):
        return (index, self.tp)

    def z_id(self, index):
        return (self.sp, 2 * index + self.core)

    def barrier(self, use_sp, use_z):
        sem = pltpu.get_barrier_semaphore()
        count = 1
        pl.semaphore_signal(sem, inc=1, device_id=self.partner(), device_id_type=MESH_ID)
        if use_sp:
            for step in range(1, self.n_sp):
                pl.semaphore_signal(
                    sem, inc=1, device_id=self.sp_id(self.sp_peer(step)), device_id_type=MESH_ID
                )
            count += self.n_sp - 1
        if use_z:
            for step in range(1, self.n_z):
                pl.semaphore_signal(
                    sem, inc=1, device_id=self.z_id(self.z_peer(step)), device_id_type=MESH_ID
                )
            count += self.n_z - 1
        pl.semaphore_wait(sem, count)


def remote(src, dst, send, recv, device):
    return pltpu.make_async_remote_copy(
        src_ref=src,
        dst_ref=dst,
        send_sem=send,
        recv_sem=recv,
        device_id=device,
        device_id_type=MESH_ID,
    )


def vmem():
    return pl.BlockSpec(memory_space=pltpu.VMEM)


def flip(value, bits):
    shift = 1
    while shift <= bits:
        if bits & shift:
            value = value + shift * (1 - 2 * lax.rem(lax.div(value, shift), 2))
        shift *= 2
    return value


CHUNKS = 8
PIECES = 4
WIDE = 512
LEAD = 5
LAG = 2


def expert_plan(rows, tok, gate, up, down, n_sp, n_z):
    width = D // CHUNKS
    hidden = gate.shape[1]
    quarter = D // 4
    phases = [[1, 2]] + [[k] for k in range(3, n_sp)] if n_sp > 2 else [[1]]

    def weight_refs(place, ins, scratch):
        own = pl.ds(pl.multiple_of(place.core * hidden, 128), hidden)
        gbuf, ubuf, dbuf = scratch[:3]
        return list(zip(ins, (gbuf.at[:, own], ubuf.at[:, own], dbuf.at[own, :])))

    def loads_of(place, ins, scratch):
        return [
            pltpu.make_async_copy(src, dst, scratch[-7].at[i])
            for i, (src, dst) in enumerate(weight_refs(place, ins, scratch))
        ]

    def shares_of(place, ins, scratch):
        return [
            remote(src, dst, scratch[-7].at[3 + i], scratch[-7].at[6 + i], place.partner())
            for i, (src, dst) in enumerate(weight_refs(place, ins, scratch))
        ]

    def body(place, given, ins, o_ref, scratch):
        x_in, mix_in, mid_in = given
        (
            gbuf, ubuf, dbuf, xbuf, hid, sbuf, rbuf, cbuf, fbuf,
            w_sem, sent, a_r, b_r, t_r, sp_r, z_r,
        ) = scratch
        core, z, me = place.core, place.z, place.sp
        loads = loads_of(place, ins, scratch)
        traded = shares_of(place, ins, scratch)
        side = lax.rem(z, 2)
        twin = place.z_id(z + 1 - 2 * side)
        final = phases[-1] if n_sp > 2 else []

        def share(k):
            return 0 if k in final else 2 * quarter

        both = [pl.ds(i * quarter, quarter) for i in range(2)]

        def strip(which, k, p):
            half = (D - share(k)) // 2
            piece = half // PIECES
            return pl.ds(pl.multiple_of(share(k) + which * half + p * piece, 128), piece)

        def push(src, dst, kind, recv, device):
            copy = remote(src, dst, sent.at[kind], recv, device)
            copy.start()
            return copy

        strips, shares, swaps = {}, {}, {}
        order = [(k, p) for ks in phases for p in range(PIECES) for k in ks]
        halves = [(k, i) for ks in phases for i in range(2) for k in ks if k not in final]

        def push_strip(k, p):
            dst = flip(me, k)
            cols = strip(side, k, p)
            strips[k, p] = push(
                x_in.at[dst, :, cols], xbuf.at[me, :, cols], 0, a_r.at[k, p], place.sp_id(dst)
            )

        near = [one for one in order if one[0] not in final]
        far = [one for one in order if one[0] in final]
        for k, p in near:
            push_strip(k, p)
        for k, i in halves:
            dst = flip(me, k)
            shares[k, i] = push(
                x_in.at[dst, :, both[i]], xbuf.at[me, :, both[i]], 1, b_r.at[k, i],
                place.sp_id(dst),
            )
        for k, p in far:
            push_strip(k, p)

        def forward_strip(k, p):
            block = xbuf.at[flip(me, k), :, strip(side, k, p)]
            strips[k, p].wait_recv()
            swaps[k, p] = push(block, block, 2, t_r.at[k, p], twin)

        def expert(x_ref, h_ref):
            g = jnp.dot(x_ref[...], gbuf[...], preferred_element_type=jnp.float32)
            u = jnp.dot(x_ref[...], ubuf[...], preferred_element_type=jnp.float32)
            h_ref[...] = (g / (1.0 + jnp.exp(-g)) * u).astype(jnp.bfloat16)

        def column(q):
            return pl.ds(pl.multiple_of(q * width, width), width)

        def back_copy(k, q):
            src = flip(me, k)
            return remote(
                sbuf.at[src, :, column(q)], rbuf.at[me, :, column(q)],
                sent.at[3], sp_r.at[k, q], place.sp_id(src),
            )

        def serve(k):
            src = flip(me, k)
            expert(x_in.at[me] if k == 0 else xbuf.at[src], hid.at[0])
            for w in range(D // WIDE):
                cols = slice(w * WIDE, (w + 1) * WIDE)
                total = jnp.dot(
                    hid[0], dbuf[:, cols], preferred_element_type=jnp.float32
                ).astype(jnp.bfloat16)
                if k == 0:
                    rbuf[src, :, cols] = total
                else:
                    sbuf[src, :, cols] = total

        def reply(ks, first, last):
            def body(q, carry):
                for k in ks:
                    back_copy(k, q).start()
                return carry

            lax.fori_loop(first, last, body, 0)

        for copy in loads:
            copy.wait()
        for copy in traded:
            copy.wait_recv()
        head = len(phases[0])
        for k, p in near[:head]:
            forward_strip(k, p)
        serve(0)
        for k, p in near[head:]:
            forward_strip(k, p)
        for k, p in near:
            swaps[k, p].wait_recv()
        for k, i in halves:
            shares[k, i].wait_recv()
        rest = [k for ks in phases for k in ks if k not in final]
        coming = list(far)
        for k in rest:
            if coming:
                forward_strip(*coming.pop(0))
            serve(k)
            reply([k], 0, LEAD)
        while coming:
            forward_strip(*coming.pop(0))
        for k, p in far:
            swaps[k, p].wait_recv()
        for k in final:
            serve(k)

        def rest_of(q, carry):
            for k in final:
                back_copy(k, q).start()
            for k in rest:
                back_copy(k, q + LEAD).start()
            return carry

        lax.fori_loop(0, CHUNKS - LEAD, rest_of, 0)
        reply(final, CHUNKS - LEAD, CHUNKS)

        levels = n_z.bit_length() - 1

        def z_blocks(level):
            span = 2 << level
            keep = lax.rem(z, span)
            base = n_z - (n_z >> level)
            return [
                (j * span + keep, j * span + flip(keep, 1 << level), base + j)
                for j in range(n_z // span)
            ]

        def z_copy(q, level, sent_block, slot):
            return remote(
                cbuf.at[sent_block, :, column(q)], fbuf.at[slot, :, column(q)],
                sent.at[4], z_r.at[q, slot], place.z_id(flip(z, 1 << level)),
            )

        def combine(q):
            for k in range(1, n_sp):
                back_copy(k, q).wait_recv()
            total = None
            for src in range(n_sp):
                more = split_dot(mix_in[src], rbuf[src, :, column(q)], TN)
                total = more if total is None else total + more
            cbuf[:, :, column(q)] = total.astype(jnp.bfloat16).reshape(n_z, tok, width)
            for _, sent_block, slot in z_blocks(0):
                z_copy(q, 0, sent_block, slot).start()

        def add_level(q, level):
            for kept, sent_block, slot in z_blocks(level):
                z_copy(q, level, sent_block, slot).wait_recv()
                total = cbuf[kept, :, column(q)].astype(jnp.float32) + fbuf[
                    slot, :, column(q)
                ].astype(jnp.float32)
                if level + 1 == levels:
                    o_ref[:, column(q)] = (total + mid_in[:, column(q)]).astype(jnp.bfloat16)
                else:
                    cbuf[kept, :, column(q)] = total.astype(jnp.bfloat16)
            if level + 1 < levels:
                for _, sent_block, slot in z_blocks(level + 1):
                    z_copy(q, level + 1, sent_block, slot).start()

        def wave(i, carry):
            for stage in range(levels + 1):
                q = i - LAG * stage

                @pl.when((q >= 0) & (q < CHUNKS))
                def _(q=q, stage=stage):
                    if stage == 0:
                        combine(q)
                    else:
                        add_level(q, stage - 1)

            return carry

        lax.fori_loop(0, CHUNKS, wave, 0)
        lax.fori_loop(CHUNKS, CHUNKS + LAG * levels, wave, 0)
        strip_bytes = xbuf.at[:, :, pl.ds(0, quarter)]
        for kind, block in enumerate(
            (
                strip_bytes, xbuf.at[pl.ds(0, n_sp - 2), :, pl.ds(0, 2 * quarter)],
                strip_bytes, sbuf.at[pl.ds(0, n_sp - 1)], fbuf.at[pl.ds(0, n_z - 1)],
            )
        ):
            remote(block, block, sent.at[kind], z_r.at[0, 0], place.partner()).wait_send()
        for copy in traded:
            copy.wait_send()

    dma = pltpu.SemaphoreType.DMA
    bf = jnp.bfloat16
    block = pltpu.VMEM((n_sp, rows, D), bf)
    zblock = pltpu.VMEM((n_z, tok, D), bf)
    return dict(
        body=body,
        loads=loads_of,
        shares=shares_of,
        ins=(gate, up, down),
        scratch=[
            pltpu.VMEM((D, 2 * hidden), bf),
            pltpu.VMEM((D, 2 * hidden), bf),
            pltpu.VMEM((2 * hidden, D), bf),
            block,
            pltpu.VMEM((1, rows, 2 * hidden), bf),
            block, block, zblock, zblock,
            dma((9,)),
            dma((5,)),
            dma((n_sp, PIECES)),
            dma((n_sp, 2)),
            dma((n_sp, PIECES)),
            dma((n_sp, CHUNKS)),
            dma((CHUNKS, n_z)),
        ],
    )


VMEM_ROOM = 63 << 20


def run_plans(first, second, tok, n_sp, n_z):
    hbm = pl.BlockSpec(memory_space=pl.ANY)
    out_shape = jax.ShapeDtypeStruct((tok, D), jnp.bfloat16)
    n_ins, n_first, n_given = len(first["ins"]), len(first["scratch"]), len(first["outs"])
    given = [pltpu.VMEM(shape, dtype) for shape, dtype in first["outs"]]
    sizes = first["scratch"] + second["scratch"] + given
    need = sum(
        int(np.prod(one.inner_aval.shape)) * one.inner_aval.dtype.itemsize
        for one in sizes
        if "vmem" in str(one.memory_space)
    )

    def params(number, room):
        return pltpu.CompilerParams(
            collective_id=number, has_side_effects=True, vmem_limit_bytes=room
        )

    def merged(*refs):
        place = Place(n_sp, n_z)
        ins, weights, refs = refs[:n_ins], refs[n_ins : n_ins + 3], refs[n_ins + 3 :]
        o_ref, held, refs = refs[0], refs[1 : 1 + n_given], refs[1 + n_given :]
        later = refs[n_first:]
        drain = first["body"](
            place, ins, held, refs[:n_first], second["loads"](place, weights, later),
            second["shares"](place, weights, later),
        )
        second["body"](place, held, weights, o_ref, refs[n_first:])
        drain()

    if need < 52 << 20:
        return pl.pallas_call(
            merged,
            out_shape=out_shape,
            in_specs=first["in_specs"] + [hbm] * 3,
            out_specs=vmem(),
            scratch_shapes=given + first["scratch"] + second["scratch"],
            compiler_params=params(0, VMEM_ROOM),
            name="layer",
        )(*first["ins"], *second["ins"])

    def head(*refs):
        place = Place(n_sp, n_z)
        ins, outs = refs[:n_ins], refs[n_ins : n_ins + n_given]
        first["body"](place, ins, outs, refs[n_ins + n_given :], [], [])()

    def tail(*refs):
        place = Place(n_sp, n_z)
        scratch = refs[n_given + 4 :]
        for load in second["loads"](place, refs[n_given : n_given + 3], scratch):
            load.start()
        place.barrier(True, True)
        for copy in second["shares"](place, refs[n_given : n_given + 3], scratch):
            copy.start()
        second["body"](
            place, refs[:n_given], refs[n_given : n_given + 3], refs[n_given + 3], scratch
        )

    held = pl.pallas_call(
        head,
        out_shape=tuple(jax.ShapeDtypeStruct(*one) for one in first["outs"]),
        in_specs=first["in_specs"],
        out_specs=(vmem(),) * n_given,
        scratch_shapes=first["scratch"],
        compiler_params=params(0, VMEM_ROOM),
        name="front",
    )(*first["ins"])
    return pl.pallas_call(
        tail,
        out_shape=out_shape,
        in_specs=[vmem()] * n_given + [hbm] * 3,
        out_specs=vmem(),
        scratch_shapes=second["scratch"],
        compiler_params=params(1, VMEM_ROOM),
        name="experts",
    )(*held, *second["ins"])


RES_PARTS = 4


def split_dot(a, b, dims):
    return lax.dot_general(a, b, (dims, ((), ())), preferred_element_type=jnp.float32)


NT = ((1,), (1,))
NN = ((1,), (0,))
TN = ((0,), (0,))


def front_plan(
    queries, latent, rot_key, lat_gain, key_up, value_up, q_gain, k_gain, out_gain,
    out_weight, residual, ffn_gain, routes, weights, n_sp, n_z, width,
):
    heads, length = queries.shape[0] // QK, queries.shape[1]
    n_tp = 2 * n_z
    tok = residual.shape[0]
    part = n_z * tok
    cap = max(2, 9 * tok * TOPK // (8 * n_sp))
    rows = n_z * cap
    bundle = 2 * length + length // 2
    half = length // 2
    lanes = 128
    att_width = width
    qt = 256
    pt = 128
    per = lanes // tok
    named_rows = -(-n_sp // 8) * 8
    freqs = ROPE // 2
    inverse = np.float32(rope_base) ** (-np.arange(0, ROPE, 2, dtype=np.float32) / np.float32(ROPE))

    def body(place, ins, outs, scratch, more_loads, more_sends):
        (
            q_hbm, lat_hbm, rot_in, latg, kup_hbm, vup_hbm, qg, kg, outg, w_hbm, res_hbm, ffng,
            routes_in, weights_in,
        ) = ins
        out_rows, mixer, mid_out = outs
        (
            q_in, lat_in, kup, vup, table, gains, tokens, qbuf, kv, peak, total, acc, att, gath,
            normed, wbuf, resbuf, metabuf, mid, ffn, load_sem, sent, kv_s, kv_r, res_r, meta_r,
            att_r,
        ) = scratch
        sp, core, z, tp = place.sp, place.core, place.z, place.tp
        sem = pltpu.get_barrier_semaphore()
        for step in range(1, n_tp):
            pl.semaphore_signal(
                sem, inc=1, device_id=(sp, lax.rem(tp + step, n_tp)), device_id_type=MESH_ID
            )
        for step in range(1, n_sp):
            pl.semaphore_signal(
                sem, inc=1, device_id=place.sp_id(place.sp_peer(step)), device_id_type=MESH_ID
            )
        loads = []
        for i, (src, dst) in enumerate(
            (
                (lat_hbm, lat_in), (kup_hbm, kup), (vup_hbm, vup), (q_hbm, q_in),
                (res_hbm, resbuf.at[z]), (w_hbm, wbuf),
            )
        ):
            load = pltpu.make_async_copy(src, dst, load_sem.at[i])
            load.start()
            loads.append(load)
        for load in more_loads:
            load.start()

        tokens[0:1, :] = jnp.full((1, lanes), -1.0, jnp.float32)
        tokens[1:2, :] = jnp.full((1, lanes), -1.0, jnp.float32)
        tokens[0:TOPK, :tok] = routes_in[...].astype(jnp.float32)
        tokens[2:4, :tok] = weights_in[...]
        expert_id = lax.broadcasted_iota(jnp.int32, (named_rows, lanes), 0).astype(jnp.float32)
        named0 = expert_id == tokens[0:1, :]
        named1 = expert_id == tokens[1:2, :]
        named = jnp.where(named0 | named1, 1.0, 0.0)
        earlier = jnp.where(
            lax.broadcasted_iota(jnp.int32, (lanes, lanes), 0)
            < lax.broadcasted_iota(jnp.int32, (lanes, lanes), 1),
            1.0,
            0.0,
        ).astype(jnp.bfloat16)
        rank = split_dot(named.astype(jnp.bfloat16), earlier, NN)
        slot = jnp.where(named0 | named1, rank + (z * cap).astype(jnp.float32), -1.0)
        share = jnp.where(named0, tokens[2:3, :], 0.0) + jnp.where(named1, tokens[3:4, :], 0.0)
        place_by = lax.rem(z, per)
        for turn_by in range(per):

            @pl.when(place_by == turn_by)
            def _(turn_by=turn_by):
                metabuf[z, :named_rows] = pltpu.roll(slot, turn_by * tok, 1) if turn_by else slot
                metabuf[z, named_rows:] = pltpu.roll(share, turn_by * tok, 1) if turn_by else share

        freq_id = lax.broadcasted_iota(jnp.int32, (freqs, length), 0)
        freq = jnp.zeros((freqs, length), jnp.float32)
        for i in range(freqs):
            freq = jnp.where(freq_id == i, float(inverse[i]), freq)
        where = lax.broadcasted_iota(jnp.int32, (freqs, length), 1) + sp * length
        angle = where.astype(jnp.float32) * freq
        spread_by = jnp.where(
            lax.broadcasted_iota(jnp.int32, (freqs, lanes), 1) % freqs
            == lax.broadcasted_iota(jnp.int32, (freqs, lanes), 0),
            1.0,
            0.0,
        )

        for which, values in enumerate((jnp.cos(angle), jnp.sin(angle))):
            table[which] = lax.dot_general(
                values, spread_by, (TN, ((), ())), precision=lax.Precision.HIGHEST,
                preferred_element_type=jnp.float32,
            )
        for i, gain in enumerate((qg, kg)):
            gains[4 + i : 5 + i, :] = jnp.zeros((1, lanes), jnp.float32)
            gains[4 + i : 5 + i, :QK] = gain[...]
        gain_lane = lax.broadcasted_iota(jnp.int32, (1, lanes), 1)
        packed = []
        for i in range(2):
            raw_gain = gains[4 + i : 5 + i, :]
            nope_gain = jnp.where(gain_lane < NOPE, raw_gain, pltpu.roll(raw_gain, NOPE, 1))
            once = jnp.where(gain_lane < ROPE, pltpu.roll(raw_gain, lanes - NOPE, 1), 0.0)
            rot_gain = once
            for h in range(1, heads):
                rot_gain = rot_gain + pltpu.roll(once, h * ROPE, 1)
            packed.append((nope_gain, rot_gain))
        (q_nope_gain, q_rot_gain), (k_nope_gain, k_rot_gain) = packed

        pl.semaphore_wait(sem, n_tp - 1 + n_sp - 1)
        for copy in more_sends:
            copy.start()

        def push(src, dst, kind, recv, device):
            copy = remote(src, dst, sent.at[kind], recv, device)
            copy.start()
            return copy

        parts = [slice(i * D // RES_PARTS, (i + 1) * D // RES_PARTS) for i in range(RES_PARTS)]

        def res_copy(src, i, to, src_ref=None):
            block = resbuf.at[src, :, parts[i]]
            from_ref = block if src_ref is None else src_ref.at[:, parts[i]]
            return remote(
                from_ref, block, sent.at[0], res_r.at[src, i], place.z_id(to)
            )

        for i in range(RES_PARTS):
            for away in (2, -2, 1, -1):
                to = z + away

                @pl.when((to >= 0) & (to < n_z))
                def _(to=to, i=i):
                    res_copy(z, i, to, res_hbm).start()

        for step in range(1, n_z):
            to = place.z_id(place.z_peer(step))
            push(metabuf.at[z], metabuf.at[z], 1, meta_r.at[z], to)

        def pass_on(away, i):
            for sign in (1, -1):
                src, to = z - sign * away, z + sign

                @pl.when((src >= 0) & (src < n_z) & (to >= 0) & (to < n_z))
                def _(src=src, to=to):
                    res_copy(src, i, z).wait_recv()
                    res_copy(src, i, to).start()

        lane = lax.broadcasted_iota(jnp.int32, (1, lanes), 1)
        low = lane % ROPE < ROPE // 2
        mine = kv.at[sp]
        for load in loads[:3]:
            load.wait()

        def turn(values, cos, sin):
            return (
                values * cos
                + pltpu.roll(values, lanes - ROPE // 2, 1) * jnp.where(low, -sin, 0.0)
                + pltpu.roll(values, ROPE // 2, 1) * jnp.where(low, 0.0, sin)
            )

        sel = lax.broadcasted_iota(jnp.int32, (ROPE, lanes), 0)
        rot_sel = jnp.where(
            (lax.broadcasted_iota(jnp.int32, (ROPE, lanes), 1) % ROPE == sel)
            & (lax.broadcasted_iota(jnp.int32, (ROPE, lanes), 1) < heads * ROPE),
            1.0,
            0.0,
        ).astype(jnp.bfloat16)
        rot_parts = length // pt

        def make_keys(i, carry):
            at = pl.ds(pl.multiple_of(i * pt, pt), pt)
            lat = lat_in[at, :].astype(jnp.float32)
            scale = lax.rsqrt(jnp.mean(lat * lat, axis=-1, keepdims=True) + epsilon)
            normed_lat = (lat * scale * latg[...]).astype(jnp.bfloat16)
            nope = split_dot(normed_lat, kup[...], NN).astype(jnp.bfloat16).astype(jnp.float32)
            vals = split_dot(normed_lat, vup[...], NN).astype(jnp.bfloat16)
            kv[sp, pl.ds(pl.multiple_of(length + i * pt, pt), pt), :] = vals
            rot = split_dot(rot_in[:, at], rot_sel, TN)
            square, rot_square = nope * nope, rot * rot
            nope_scale, rot_scale = None, None
            for h in range(heads):
                in_nope = (lane >= h * NOPE) & (lane < (h + 1) * NOPE)
                in_rot = (lane >= h * ROPE) & (lane < (h + 1) * ROPE)
                one = lax.rsqrt(
                    jnp.sum(
                        jnp.where(in_nope, square, 0.0) + jnp.where(in_rot, rot_square, 0.0),
                        axis=-1,
                        keepdims=True,
                    )
                    / QK
                    + epsilon
                )
                nope_scale = one if h == 0 else jnp.where(in_nope, one, nope_scale)
                rot_scale = one if h == 0 else jnp.where(in_rot, one, rot_scale)
            kv[sp, at, :] = (nope * nope_scale * k_nope_gain).astype(jnp.bfloat16)
            turned = turn(rot * rot_scale * k_rot_gain, table[0, at, :], table[1, at, :])
            return turned

        def make_pair(i, carry):
            first = make_keys(i, carry)
            second = make_keys(i + rot_parts // 2, carry)
            packed = first + pltpu.roll(second, 64, 1)
            kv[sp, pl.ds(pl.multiple_of(2 * length + i * pt, pt), pt), :] = packed.astype(
                jnp.bfloat16
            )
            return carry

        lax.fori_loop(0, rot_parts // 2, make_pair, 0)
        for step in range(1, n_sp):
            dst = sp + n_sp - step

            @pl.when(dst < n_sp)
            def _(dst=dst):
                remote(mine, mine, kv_s.at[dst], kv_r.at[sp], place.sp_id(dst)).start()

        wide = 2 * lanes
        src_id = lax.broadcasted_iota(jnp.int32, (heads * QK, wide), 0)
        dst_id = lax.broadcasted_iota(jnp.int32, (heads * QK, wide), 1)
        pickers = []
        for h in range(heads):
            entry = src_id - h * QK
            nope_hit = (entry >= 0) & (entry < NOPE) & (dst_id == h * NOPE + entry)
            rot_hit = (
                (entry >= NOPE) & (entry < QK) & (dst_id == lanes + h * ROPE + entry - NOPE)
            )
            pickers.append(jnp.where(nope_hit | rot_hit, 1.0, 0.0).astype(jnp.bfloat16))

        loads[3].wait()

        def make_queries(i, carry):
            at = pl.ds(pl.multiple_of(i * pt, pt), pt)
            raw = q_in[:, at]
            for h in range(heads):
                spread = split_dot(raw, pickers[h], TN)
                scale = lax.rsqrt(
                    jnp.sum(spread * spread, axis=-1, keepdims=True) / QK + epsilon
                )
                nope = (spread[:, :lanes] * scale * q_nope_gain).astype(jnp.bfloat16)
                rot = turn(spread[:, lanes:] * scale * q_rot_gain, table[0, at, :], table[1, at, :])
                qbuf[h, 0, at, :lanes] = nope
                qbuf[h, 1, at, :lanes] = nope
                qbuf[h, 0, at, lanes:] = rot.astype(jnp.bfloat16)
                qbuf[h, 1, at, lanes:] = pltpu.roll(rot, 64, 1).astype(jnp.bfloat16)
            return carry

        lax.fori_loop(0, length // pt, make_queries, 0)

        factor = QK ** (-0.5) * 1.4426950408889634

        def attend(src, first, diagonal):
            knope = [kv[src, s * half : (s + 1) * half, :] for s in range(2)]
            krot = kv[src, 2 * length : bundle, :]
            keys = [jnp.concatenate([knope[s], krot], axis=1) for s in range(2)]
            vals = kv[src, length : 2 * length, :]

            def tile(i, carry):
                at = pl.ds(pl.multiple_of(i * qt, qt), qt)
                outs = []
                for h in range(heads):
                    scores = jnp.concatenate(
                        [split_dot(qbuf[h, s, at, :], keys[s], NT) for s in range(2)], axis=1
                    )
                    scores = scores * factor
                    if diagonal:
                        row = lax.broadcasted_iota(jnp.int32, scores.shape, 0) + i * qt
                        col = lax.broadcasted_iota(jnp.int32, scores.shape, 1)
                        scores = jnp.where(col <= row, scores, -1e30)
                    top = jnp.max(scores, axis=-1, keepdims=True)
                    if not first:
                        old = peak[h, at, :]
                        top = jnp.maximum(old[:, :1], top)
                    weight = jnp.exp2(scores - top)
                    sums = jnp.sum(weight, axis=-1, keepdims=True)
                    part_out = split_dot(weight.astype(jnp.bfloat16), vals, NN)
                    if first:
                        total[h, at, :] = jnp.broadcast_to(sums, (qt, lanes))
                        outs.append((part_out, None))
                    else:
                        fade = jnp.exp2(old[:, :1] - top)
                        total[h, at, :] = total[h, at, :] * fade + sums
                        outs.append((part_out, fade))
                    peak[h, at, :] = jnp.broadcast_to(top, (qt, lanes))
                new, fade = outs[0]
                for h in range(1, heads):
                    new = jnp.where(lane >= h * VH, outs[h][0], new)
                    if not first:
                        fade = jnp.where(lane >= h * VH, outs[h][1], fade)
                acc[at, :] = new if first else acc[at, :] * fade + new
                return carry

            lax.fori_loop(0, length // qt, tile, 0, unroll=2)

        attend(sp, True, True)

        def visit(step, carry):
            src = sp - step

            @pl.when(src >= 0)
            def _():
                remote(
                    kv.at[src], kv.at[src], kv_s.at[src], kv_r.at[src], place.sp_id(src)
                ).wait_recv()
                attend(src, False, False)

            return carry

        hops = [(away, i) for away in range(2, n_z - 1) for i in range(RES_PARTS)]
        head = RES_PARTS // 2
        for away, i in hops[:head]:
            pass_on(away, i)
        lax.fori_loop(1, 2, visit, 0)
        for away, i in hops[head:RES_PARTS]:
            pass_on(away, i)
        lax.fori_loop(2, n_sp, visit, 0)
        for away, i in hops[RES_PARTS:]:
            pass_on(away, i)

        for block in range(n_tp):
            at = pl.ds(block * tok, tok)
            bottom = total[0, at, :]
            for h in range(1, heads):
                bottom = jnp.where(lane >= h * VH, total[h, at, :], bottom)
            att[block % 2, (block // 2) * tok : (block // 2 + 1) * tok, :] = (
                acc[at, :] / bottom
            ).astype(jnp.bfloat16)
        def att_copy(src, parity, to_z, to_core, src_ref=None):
            block = gath.at[src]
            from_ref = block if src_ref is None else src_ref.at[parity]
            return remote(
                from_ref, block, sent.at[2], att_r.at[src], (sp, 2 * to_z + to_core)
            )

        for away in (2, -2, 1, -1):
            to = z + away

            @pl.when((to >= 0) & (to < n_z))
            def _(to=to):
                for parity in range(2):
                    att_copy(tp, parity, to, parity, att).start()

        remote(
            att.at[1 - core], gath.at[tp], sent.at[2], att_r.at[tp], place.partner()
        ).start()
        own = pltpu.make_async_copy(att.at[core], gath.at[tp], load_sem.at[6])
        own.start()

        partner = place.partner()
        for step in range(1, n_z):
            block = metabuf.at[place.z_peer(step)]
            remote(block, block, sent.at[1], meta_r.at[place.z_peer(step)], partner).wait_recv()
        pieces = []
        for first in range(0, n_z, per):
            piece = metabuf[first]
            for i in range(1, per):
                piece = jnp.where(lane >= i * tok, metabuf[first + i], piece)
            pieces.append(piece)
        meta = jnp.concatenate(pieces, axis=1)
        slot_id = lax.broadcasted_iota(jnp.int32, (rows, part), 0).astype(jnp.float32)
        for e in range(n_sp):
            hit = meta[e : e + 1, :] == slot_id
            mixer[e] = jnp.where(
                hit, meta[named_rows + e : named_rows + e + 1, :], 0.0
            ).astype(jnp.bfloat16)
        for i in range(RES_PARTS):
            for src in range(n_z):
                away = z - src
                passed = ((away >= 2) & (z + 1 < n_z)) | ((away <= -2) & (z > 0))

                @pl.when((away != 0) & jnp.logical_not(passed))
                def _(src=src, i=i):
                    res_copy(src, i, z).wait_recv()

        for load in loads[4:]:
            load.wait()
        own.wait()
        for away in range(2, n_z - 1):
            for sign in (1, -1):
                src, to = z - sign * away, z + sign

                @pl.when((src >= 0) & (src < n_z) & (to >= 0) & (to < n_z))
                def _(src=src, to=to):
                    for which in range(2):
                        att_copy(2 * src + which, core, z, core).wait_recv()
                        att_copy(2 * src + which, core, to, core).start()

        for src in range(n_tp):
            away = z - src // 2
            passed = ((away >= 2) & (z + 1 < n_z)) | ((away <= -2) & (z > 0))

            @pl.when((tp != src) & jnp.logical_not(passed))
            def _(src=src):
                att_copy(src, core, z, core).wait_recv()

        square = None
        for t in range(n_tp):
            block = gath[t].astype(jnp.float32)
            square = block * block if square is None else square + block * block
        scale = lax.rsqrt(jnp.sum(square, axis=-1, keepdims=True) / att_width + epsilon)
        for t in range(n_tp):
            normed[:, t * lanes : (t + 1) * lanes] = (
                gath[t].astype(jnp.float32) * scale * outg[t]
            ).astype(jnp.bfloat16)
        ct = 512
        square = None
        for c in range(D // ct):
            cols = slice(c * ct, (c + 1) * ct)
            values = split_dot(normed[...], wbuf[:, cols], NN) + resbuf[:, :, cols].reshape(
                part, ct
            ).astype(jnp.float32)
            mid[:, cols] = values
            more = jnp.sum(values * values, axis=-1, keepdims=True)
            square = more if square is None else square + more
        scale = lax.rsqrt(square / D + epsilon)
        for c in range(D // ct):
            cols = slice(c * ct, (c + 1) * ct)
            ffn[:, cols] = (mid[:, cols] * scale * ffng[0:1, cols]).astype(jnp.bfloat16)
        mid_out[...] = mid[pl.ds(pl.multiple_of(z * tok, tok), tok), :]
        for e in range(n_sp):
            hit = jnp.where(meta[e : e + 1, :] == slot_id, 1.0, 0.0).astype(jnp.bfloat16)
            for c in range(D // ct):
                cols = slice(c * ct, (c + 1) * ct)
                out_rows[e, :, cols] = split_dot(hit, ffn[:, cols], NN).astype(jnp.bfloat16)

        def drain():
            for i in range(RES_PARTS):
                block = resbuf.at[0, :, parts[i]]
                one = remote(block, block, sent.at[0], res_r.at[0, 0], partner)
                for away in (2, -2, 1, -1):

                    @pl.when((z + away >= 0) & (z + away < n_z))
                    def _(one=one):
                        one.wait_send()

            for away, i in hops:
                block = resbuf.at[0, :, parts[i]]
                one = remote(block, block, sent.at[0], res_r.at[0, 0], partner)
                for sign in (1, -1):
                    src, to = z - sign * away, z + sign

                    @pl.when((src >= 0) & (src < n_z) & (to >= 0) & (to < n_z))
                    def _(one=one):
                        one.wait_send()

            block = metabuf.at[pl.ds(0, n_z - 1)]
            remote(block, block, sent.at[1], meta_r.at[0], partner).wait_send()
            one = att_copy(tp, core, z, core)
            one.wait_send()
            for away in (2, -2, 1, -1):

                @pl.when((z + away >= 0) & (z + away < n_z))
                def _():
                    one.wait_send()
                    one.wait_send()

            for away in range(2, n_z - 1):
                for sign in (1, -1):
                    src, to = z - sign * away, z + sign

                    @pl.when((src >= 0) & (src < n_z) & (to >= 0) & (to < n_z))
                    def _():
                        one.wait_send()
                        one.wait_send()

            for step in range(1, n_sp):
                dst = sp + n_sp - step

                @pl.when(dst < n_sp)
                def _(dst=dst):
                    remote(mine, mine, kv_s.at[dst], kv_r.at[sp], place.sp_id(dst)).wait_send()

        return drain

    dma = pltpu.SemaphoreType.DMA
    bf, f4 = jnp.bfloat16, jnp.float32
    hbm = pl.BlockSpec(memory_space=pl.ANY)
    return dict(
        body=body,
        ins=(
            queries, latent, rot_key, lat_gain, key_up, value_up, q_gain, k_gain, out_gain,
            out_weight, residual, ffn_gain, routes, weights,
        ),
        in_specs=[
            hbm, hbm, vmem(), vmem(), hbm, hbm, vmem(), vmem(), vmem(), hbm, hbm, vmem(),
            vmem(), vmem(),
        ],
        outs=[((n_sp, rows, D), bf), ((n_sp, rows, part), bf), ((tok, D), f4)],
        scratch=[
            pltpu.VMEM(queries.shape, bf),
            pltpu.VMEM(latent.shape, bf),
            pltpu.VMEM(key_up.shape, bf),
            pltpu.VMEM(value_up.shape, bf),
            pltpu.VMEM((2, length, lanes), f4),
            pltpu.VMEM((8, lanes), f4),
            pltpu.VMEM((8, lanes), f4),
            pltpu.VMEM((heads, 2, length, 2 * lanes), bf),
            pltpu.VMEM((n_sp, bundle, lanes), bf),
            pltpu.VMEM((heads, length, lanes), f4),
            pltpu.VMEM((heads, length, lanes), f4),
            pltpu.VMEM((length, lanes), f4),
            pltpu.VMEM((2, part, lanes), bf),
            pltpu.VMEM((n_tp, part, lanes), bf),
            pltpu.VMEM((part, n_tp * lanes), bf),
            pltpu.VMEM(out_weight.shape, bf),
            pltpu.VMEM((n_z, tok, D), bf),
            pltpu.VMEM((n_z, 2 * named_rows, lanes), f4),
            pltpu.VMEM((part, D), f4),
            pltpu.VMEM((part, D), bf),
            dma((7,)),
            dma((3,)),
            dma((n_sp,)),
            dma((n_sp,)),
            dma((n_z, RES_PARTS)),
            dma((n_z,)),
            dma((n_tp,)),
        ],
    )


def shards(
    queries, latent, rot_key, latent_gain, key_up, value_up, query_gain, key_gain, out_gain,
    out_weight, residual, ffn_gain, routes, route_weights, expert_gate, expert_up, expert_down,
):
    heads = key_up.shape[1] // NOPE
    n_sp = lax.axis_size("sp")
    n_tp = lax.axis_size("tp")
    n_z = n_tp // 2
    width = heads * VH
    out_gain = out_gain.reshape(n_tp, 1, width)
    if width < 128:
        spare = 128 - width
        key_up = jnp.pad(key_up, ((0, 0), (0, spare)))
        value_up = jnp.pad(value_up, ((0, 0), (0, spare)))
        out_gain = jnp.pad(out_gain, ((0, 0), (0, 0), (0, spare)))
        out_weight = jnp.pad(
            out_weight.reshape(n_tp, width, D), ((0, 0), (0, spare), (0, 0))
        ).reshape(n_tp * 128, D)
    first = front_plan(
        queries.T, latent, rot_key.T, latent_gain[None, :], key_up, value_up,
        query_gain[None, :], key_gain[None, :], out_gain, out_weight,
        residual, ffn_gain[None, :], routes.T, route_weights.T, n_sp, n_z, n_tp * width,
    )
    cap = max(2, 9 * residual.shape[0] * TOPK // (8 * n_sp))
    second = expert_plan(
        n_z * cap, residual.shape[0], expert_gate[0], expert_up[0], expert_down[0], n_sp, n_z
    )
    return run_plans(first, second, residual.shape[0], n_sp, n_z)


def solution(mesh):
    return jax.shard_map(
        shards,
        mesh=mesh,
        in_specs=(
            P("sp", "tp"),
            P("sp", None),
            P("sp", None),
            P(),
            P(None, "tp"),
            P(None, "tp"),
            P(),
            P(),
            P(),
            P(),
            P(("sp", "tp"), None),
            P(),
            P(("sp", "tp"), None),
            P(("sp", "tp"), None),
            P("sp", None, "tp"),
            P("sp", None, "tp"),
            P("sp", "tp", None),
        ),
        out_specs=P(("sp", "tp"), None),
        check_vma=False,
    )
```

```python
import jax
import jax.numpy as jnp
import numpy as np
from jax import lax
from jax.experimental import pallas as pl
from jax.experimental.pallas import tpu as pltpu
from jax.sharding import PartitionSpec as P

D = 2048
NOPE = 64
ROPE = 32
VH = 64
TOPK = 2
QK = 96

epsilon = 1e-06
rope_base = 10000.0
MESH_ID = pl.DeviceIdType.MESH


class Place:
    def __init__(self, n_sp, n_z):
        self.n_sp, self.n_z = n_sp, n_z
        self.sp = lax.axis_index("sp")
        self.tp = lax.axis_index("tp")
        self.core = lax.rem(self.tp, 2)
        self.z = lax.div(self.tp, 2)

    def partner(self):
        return (self.sp, self.tp + 1 - 2 * self.core)

    def sp_peer(self, step):
        return lax.rem(self.sp + step, self.n_sp)

    def z_peer(self, step):
        return lax.rem(self.z + step, self.n_z)

    def sp_id(self, index):
        return (index, self.tp)

    def z_id(self, index):
        return (self.sp, 2 * index + self.core)

    def barrier(self, use_sp, use_z):
        sem = pltpu.get_barrier_semaphore()
        count = 1
        pl.semaphore_signal(sem, inc=1, device_id=self.partner(), device_id_type=MESH_ID)
        if use_sp:
            for step in range(1, self.n_sp):
                pl.semaphore_signal(
                    sem, inc=1, device_id=self.sp_id(self.sp_peer(step)), device_id_type=MESH_ID
                )
            count += self.n_sp - 1
        if use_z:
            for step in range(1, self.n_z):
                pl.semaphore_signal(
                    sem, inc=1, device_id=self.z_id(self.z_peer(step)), device_id_type=MESH_ID
                )
            count += self.n_z - 1
        pl.semaphore_wait(sem, count)


def remote(src, dst, send, recv, device):
    return pltpu.make_async_remote_copy(
        src_ref=src,
        dst_ref=dst,
        send_sem=send,
        recv_sem=recv,
        device_id=device,
        device_id_type=MESH_ID,
    )


def vmem():
    return pl.BlockSpec(memory_space=pltpu.VMEM)


def flip(value, bits):
    shift = 1
    while shift <= bits:
        if bits & shift:
            value = value + shift * (1 - 2 * lax.rem(lax.div(value, shift), 2))
        shift *= 2
    return value


CHUNKS = 8
PIECES = 4
WIDE = 512
LEAD = 5
LAG = 2


def expert_plan(rows, tok, gate, up, down, n_sp, n_z):
    width = D // CHUNKS
    hidden = gate.shape[1]
    quarter = D // 4
    phases = [[1, 2]] + [[k] for k in range(3, n_sp)] if n_sp > 2 else [[1]]

    def weight_refs(place, ins, scratch):
        own = pl.ds(pl.multiple_of(place.core * hidden, 128), hidden)
        gbuf, ubuf, dbuf = scratch[:3]
        return list(zip(ins, (gbuf.at[:, own], ubuf.at[:, own], dbuf.at[own, :])))

    def loads_of(place, ins, scratch):
        return [
            pltpu.make_async_copy(src, dst, scratch[-7].at[i])
            for i, (src, dst) in enumerate(weight_refs(place, ins, scratch))
        ]

    def shares_of(place, ins, scratch):
        return [
            remote(src, dst, scratch[-7].at[3 + i], scratch[-7].at[6 + i], place.partner())
            for i, (src, dst) in enumerate(weight_refs(place, ins, scratch))
        ]

    def body(place, given, ins, o_ref, scratch):
        x_in, mix_in, mid_in = given
        (
            gbuf, ubuf, dbuf, xbuf, hid, sbuf, rbuf, cbuf, fbuf,
            w_sem, sent, a_r, b_r, t_r, sp_r, z_r,
        ) = scratch
        core, z, me = place.core, place.z, place.sp
        loads = loads_of(place, ins, scratch)
        traded = shares_of(place, ins, scratch)
        side = lax.rem(z, 2)
        twin = place.z_id(z + 1 - 2 * side)
        final = phases[-1] if n_sp > 2 else []

        def share(k):
            return 0 if k in final else 2 * quarter

        both = [pl.ds(i * quarter, quarter) for i in range(2)]

        def strip(which, k, p):
            half = (D - share(k)) // 2
            piece = half // PIECES
            return pl.ds(pl.multiple_of(share(k) + which * half + p * piece, 128), piece)

        def push(src, dst, kind, recv, device):
            copy = remote(src, dst, sent.at[kind], recv, device)
            copy.start()
            return copy

        strips, shares, swaps = {}, {}, {}
        order = [(k, p) for ks in phases for p in range(PIECES) for k in ks]
        halves = [(k, i) for ks in phases for i in range(2) for k in ks if k not in final]

        def push_strip(k, p):
            dst = flip(me, k)
            cols = strip(side, k, p)
            strips[k, p] = push(
                x_in.at[dst, :, cols], xbuf.at[me, :, cols], 0, a_r.at[k, p], place.sp_id(dst)
            )

        near = [one for one in order if one[0] not in final]
        far = [one for one in order if one[0] in final]
        for k, p in near:
            push_strip(k, p)
        for k, i in halves:
            dst = flip(me, k)
            shares[k, i] = push(
                x_in.at[dst, :, both[i]], xbuf.at[me, :, both[i]], 1, b_r.at[k, i],
                place.sp_id(dst),
            )
        for k, p in far:
            push_strip(k, p)

        def forward_strip(k, p):
            block = xbuf.at[flip(me, k), :, strip(side, k, p)]
            strips[k, p].wait_recv()
            swaps[k, p] = push(block, block, 2, t_r.at[k, p], twin)

        def expert(x_ref, h_ref):
            g = jnp.dot(x_ref[...], gbuf[...], preferred_element_type=jnp.float32)
            u = jnp.dot(x_ref[...], ubuf[...], preferred_element_type=jnp.float32)
            h_ref[...] = (g / (1.0 + jnp.exp(-g)) * u).astype(jnp.bfloat16)

        def column(q):
            return pl.ds(pl.multiple_of(q * width, width), width)

        def back_copy(k, q):
            src = flip(me, k)
            return remote(
                sbuf.at[src, :, column(q)], rbuf.at[me, :, column(q)],
                sent.at[3], sp_r.at[k, q], place.sp_id(src),
            )

        def serve(k):
            src = flip(me, k)
            expert(x_in.at[me] if k == 0 else xbuf.at[src], hid.at[0])
            for w in range(D // WIDE):
                cols = slice(w * WIDE, (w + 1) * WIDE)
                total = jnp.dot(
                    hid[0], dbuf[:, cols], preferred_element_type=jnp.float32
                ).astype(jnp.bfloat16)
                if k == 0:
                    rbuf[src, :, cols] = total
                else:
                    sbuf[src, :, cols] = total

        def reply(ks, first, last):
            def body(q, carry):
                for k in ks:
                    back_copy(k, q).start()
                return carry

            lax.fori_loop(first, last, body, 0)

        for copy in loads:
            copy.wait()
        for copy in traded:
            copy.wait_recv()
        head = len(phases[0])
        for k, p in near[:head]:
            forward_strip(k, p)
        serve(0)
        for k, p in near[head:]:
            forward_strip(k, p)
        for k, p in near:
            swaps[k, p].wait_recv()
        rest = [k for ks in phases for k in ks if k not in final]
        coming = list(far)
        forward_strip(*coming.pop(0))
        for k in rest:
            for i in range(2):
                shares[k, i].wait_recv()
            if coming:
                forward_strip(*coming.pop(0))
            serve(k)
            reply([k], 0, LEAD)
        while coming:
            forward_strip(*coming.pop(0))
        for k, p in far:
            swaps[k, p].wait_recv()
        for k in final:
            serve(k)

        def rest_of(q, carry):
            for k in final:
                back_copy(k, q).start()
            for k in rest:
                back_copy(k, q + LEAD).start()
            return carry

        lax.fori_loop(0, CHUNKS - LEAD, rest_of, 0)
        reply(final, CHUNKS - LEAD, CHUNKS)

        levels = n_z.bit_length() - 1

        def z_blocks(level):
            span = 2 << level
            keep = lax.rem(z, span)
            base = n_z - (n_z >> level)
            return [
                (j * span + keep, j * span + flip(keep, 1 << level), base + j)
                for j in range(n_z // span)
            ]

        def z_copy(q, level, sent_block, slot):
            return remote(
                cbuf.at[sent_block, :, column(q)], fbuf.at[slot, :, column(q)],
                sent.at[4], z_r.at[q, slot], place.z_id(flip(z, 1 << level)),
            )

        def combine(q):
            for k in range(1, n_sp):
                back_copy(k, q).wait_recv()
            total = None
            for src in range(n_sp):
                more = split_dot(mix_in[src], rbuf[src, :, column(q)], TN)
                total = more if total is None else total + more
            cbuf[:, :, column(q)] = total.astype(jnp.bfloat16).reshape(n_z, tok, width)
            for _, sent_block, slot in z_blocks(0):
                z_copy(q, 0, sent_block, slot).start()

        def add_level(q, level):
            for kept, sent_block, slot in z_blocks(level):
                z_copy(q, level, sent_block, slot).wait_recv()
                total = cbuf[kept, :, column(q)].astype(jnp.float32) + fbuf[
                    slot, :, column(q)
                ].astype(jnp.float32)
                if level + 1 == levels:
                    o_ref[:, column(q)] = (total + mid_in[:, column(q)]).astype(jnp.bfloat16)
                else:
                    cbuf[kept, :, column(q)] = total.astype(jnp.bfloat16)
            if level + 1 < levels:
                for _, sent_block, slot in z_blocks(level + 1):
                    z_copy(q, level + 1, sent_block, slot).start()

        def wave(i, carry):
            for stage in range(levels + 1):
                q = i - LAG * stage

                @pl.when((q >= 0) & (q < CHUNKS))
                def _(q=q, stage=stage):
                    if stage == 0:
                        combine(q)
                    else:
                        add_level(q, stage - 1)

            return carry

        lax.fori_loop(0, CHUNKS, wave, 0)
        lax.fori_loop(CHUNKS, CHUNKS + LAG * levels, wave, 0)
        strip_bytes = xbuf.at[:, :, pl.ds(0, quarter)]
        for kind, block in enumerate(
            (
                strip_bytes, xbuf.at[pl.ds(0, n_sp - 2), :, pl.ds(0, 2 * quarter)],
                strip_bytes, sbuf.at[pl.ds(0, n_sp - 1)], fbuf.at[pl.ds(0, n_z - 1)],
            )
        ):
            remote(block, block, sent.at[kind], z_r.at[0, 0], place.partner()).wait_send()
        for copy in traded:
            copy.wait_send()

    dma = pltpu.SemaphoreType.DMA
    bf = jnp.bfloat16
    block = pltpu.VMEM((n_sp, rows, D), bf)
    zblock = pltpu.VMEM((n_z, tok, D), bf)
    return dict(
        body=body,
        loads=loads_of,
        shares=shares_of,
        ins=(gate, up, down),
        scratch=[
            pltpu.VMEM((D, 2 * hidden), bf),
            pltpu.VMEM((D, 2 * hidden), bf),
            pltpu.VMEM((2 * hidden, D), bf),
            block,
            pltpu.VMEM((1, rows, 2 * hidden), bf),
            block, block, zblock, zblock,
            dma((9,)),
            dma((5,)),
            dma((n_sp, PIECES)),
            dma((n_sp, 2)),
            dma((n_sp, PIECES)),
            dma((n_sp, CHUNKS)),
            dma((CHUNKS, n_z)),
        ],
    )


VMEM_ROOM = 63 << 20


def run_plans(first, second, tok, n_sp, n_z):
    hbm = pl.BlockSpec(memory_space=pl.ANY)
    out_shape = jax.ShapeDtypeStruct((tok, D), jnp.bfloat16)
    n_ins, n_first, n_given = len(first["ins"]), len(first["scratch"]), len(first["outs"])
    given = [pltpu.VMEM(shape, dtype) for shape, dtype in first["outs"]]
    sizes = first["scratch"] + second["scratch"] + given
    need = sum(
        int(np.prod(one.inner_aval.shape)) * one.inner_aval.dtype.itemsize
        for one in sizes
        if "vmem" in str(one.memory_space)
    )

    def params(number, room):
        return pltpu.CompilerParams(
            collective_id=number, has_side_effects=True, vmem_limit_bytes=room
        )

    def merged(*refs):
        place = Place(n_sp, n_z)
        ins, weights, refs = refs[:n_ins], refs[n_ins : n_ins + 3], refs[n_ins + 3 :]
        o_ref, held, refs = refs[0], refs[1 : 1 + n_given], refs[1 + n_given :]
        later = refs[n_first:]
        drain = first["body"](
            place, ins, held, refs[:n_first], second["loads"](place, weights, later),
            second["shares"](place, weights, later),
        )
        second["body"](place, held, weights, o_ref, refs[n_first:])
        drain()

    if need < 52 << 20:
        return pl.pallas_call(
            merged,
            out_shape=out_shape,
            in_specs=first["in_specs"] + [hbm] * 3,
            out_specs=vmem(),
            scratch_shapes=given + first["scratch"] + second["scratch"],
            compiler_params=params(0, VMEM_ROOM),
            name="layer",
        )(*first["ins"], *second["ins"])

    def head(*refs):
        place = Place(n_sp, n_z)
        ins, outs = refs[:n_ins], refs[n_ins : n_ins + n_given]
        first["body"](place, ins, outs, refs[n_ins + n_given :], [], [])()

    def tail(*refs):
        place = Place(n_sp, n_z)
        scratch = refs[n_given + 4 :]
        for load in second["loads"](place, refs[n_given : n_given + 3], scratch):
            load.start()
        place.barrier(True, True)
        for copy in second["shares"](place, refs[n_given : n_given + 3], scratch):
            copy.start()
        second["body"](
            place, refs[:n_given], refs[n_given : n_given + 3], refs[n_given + 3], scratch
        )

    held = pl.pallas_call(
        head,
        out_shape=tuple(jax.ShapeDtypeStruct(*one) for one in first["outs"]),
        in_specs=first["in_specs"],
        out_specs=(vmem(),) * n_given,
        scratch_shapes=first["scratch"],
        compiler_params=params(0, VMEM_ROOM),
        name="front",
    )(*first["ins"])
    return pl.pallas_call(
        tail,
        out_shape=out_shape,
        in_specs=[vmem()] * n_given + [hbm] * 3,
        out_specs=vmem(),
        scratch_shapes=second["scratch"],
        compiler_params=params(1, VMEM_ROOM),
        name="experts",
    )(*held, *second["ins"])


RES_PARTS = 4


def split_dot(a, b, dims):
    return lax.dot_general(a, b, (dims, ((), ())), preferred_element_type=jnp.float32)


NT = ((1,), (1,))
NN = ((1,), (0,))
TN = ((0,), (0,))


def front_plan(
    queries, latent, rot_key, lat_gain, key_up, value_up, q_gain, k_gain, out_gain,
    out_weight, residual, ffn_gain, routes, weights, n_sp, n_z, width,
):
    heads, length = queries.shape[0] // QK, queries.shape[1]
    n_tp = 2 * n_z
    tok = residual.shape[0]
    part = n_z * tok
    cap = max(2, 9 * tok * TOPK // (8 * n_sp))
    rows = n_z * cap
    bundle = 2 * length + length // 2
    half = length // 2
    lanes = 128
    att_width = width
    qt = 256
    pt = 128
    per = lanes // tok
    named_rows = -(-n_sp // 8) * 8
    freqs = ROPE // 2
    inverse = np.float32(rope_base) ** (-np.arange(0, ROPE, 2, dtype=np.float32) / np.float32(ROPE))

    def body(place, ins, outs, scratch, more_loads, more_sends):
        (
            q_hbm, lat_hbm, rot_in, latg, kup_hbm, vup_hbm, qg, kg, outg, w_hbm, res_hbm, ffng,
            routes_in, weights_in,
        ) = ins
        out_rows, mixer, mid_out = outs
        (
            q_in, lat_in, kup, vup, table, gains, tokens, qbuf, kv, peak, total, acc, att, gath,
            normed, wbuf, resbuf, metabuf, mid, ffn, load_sem, sent, kv_s, kv_r, res_r, meta_r,
            att_r,
        ) = scratch
        sp, core, z, tp = place.sp, place.core, place.z, place.tp
        sem = pltpu.get_barrier_semaphore()
        for step in range(1, n_tp):
            pl.semaphore_signal(
                sem, inc=1, device_id=(sp, lax.rem(tp + step, n_tp)), device_id_type=MESH_ID
            )
        for step in range(1, n_sp):
            pl.semaphore_signal(
                sem, inc=1, device_id=place.sp_id(place.sp_peer(step)), device_id_type=MESH_ID
            )
        loads = []
        for i, (src, dst) in enumerate(
            (
                (lat_hbm, lat_in), (kup_hbm, kup), (vup_hbm, vup), (q_hbm, q_in),
                (res_hbm, resbuf.at[z]), (w_hbm, wbuf),
            )
        ):
            load = pltpu.make_async_copy(src, dst, load_sem.at[i])
            load.start()
            loads.append(load)
        for load in more_loads:
            load.start()

        tokens[0:1, :] = jnp.full((1, lanes), -1.0, jnp.float32)
        tokens[1:2, :] = jnp.full((1, lanes), -1.0, jnp.float32)
        tokens[0:TOPK, :tok] = routes_in[...].astype(jnp.float32)
        tokens[2:4, :tok] = weights_in[...]
        expert_id = lax.broadcasted_iota(jnp.int32, (named_rows, lanes), 0).astype(jnp.float32)
        named0 = expert_id == tokens[0:1, :]
        named1 = expert_id == tokens[1:2, :]
        named = jnp.where(named0 | named1, 1.0, 0.0)
        earlier = jnp.where(
            lax.broadcasted_iota(jnp.int32, (lanes, lanes), 0)
            < lax.broadcasted_iota(jnp.int32, (lanes, lanes), 1),
            1.0,
            0.0,
        ).astype(jnp.bfloat16)
        rank = split_dot(named.astype(jnp.bfloat16), earlier, NN)
        slot = jnp.where(named0 | named1, rank + (z * cap).astype(jnp.float32), -1.0)
        share = jnp.where(named0, tokens[2:3, :], 0.0) + jnp.where(named1, tokens[3:4, :], 0.0)
        place_by = lax.rem(z, per)
        for turn_by in range(per):

            @pl.when(place_by == turn_by)
            def _(turn_by=turn_by):
                metabuf[z, :named_rows] = pltpu.roll(slot, turn_by * tok, 1) if turn_by else slot
                metabuf[z, named_rows:] = pltpu.roll(share, turn_by * tok, 1) if turn_by else share

        freq_id = lax.broadcasted_iota(jnp.int32, (freqs, length), 0)
        freq = jnp.zeros((freqs, length), jnp.float32)
        for i in range(freqs):
            freq = jnp.where(freq_id == i, float(inverse[i]), freq)
        where = lax.broadcasted_iota(jnp.int32, (freqs, length), 1) + sp * length
        angle = where.astype(jnp.float32) * freq
        spread_by = jnp.where(
            lax.broadcasted_iota(jnp.int32, (freqs, lanes), 1) % freqs
            == lax.broadcasted_iota(jnp.int32, (freqs, lanes), 0),
            1.0,
            0.0,
        )

        for which, values in enumerate((jnp.cos(angle), jnp.sin(angle))):
            table[which] = lax.dot_general(
                values, spread_by, (TN, ((), ())), precision=lax.Precision.HIGHEST,
                preferred_element_type=jnp.float32,
            )
        for i, gain in enumerate((qg, kg)):
            gains[4 + i : 5 + i, :] = jnp.zeros((1, lanes), jnp.float32)
            gains[4 + i : 5 + i, :QK] = gain[...]
        gain_lane = lax.broadcasted_iota(jnp.int32, (1, lanes), 1)
        packed = []
        for i in range(2):
            raw_gain = gains[4 + i : 5 + i, :]
            nope_gain = jnp.where(gain_lane < NOPE, raw_gain, pltpu.roll(raw_gain, NOPE, 1))
            once = jnp.where(gain_lane < ROPE, pltpu.roll(raw_gain, lanes - NOPE, 1), 0.0)
            rot_gain = once
            for h in range(1, heads):
                rot_gain = rot_gain + pltpu.roll(once, h * ROPE, 1)
            packed.append((nope_gain, rot_gain))
        (q_nope_gain, q_rot_gain), (k_nope_gain, k_rot_gain) = packed

        pl.semaphore_wait(sem, n_tp - 1 + n_sp - 1)
        for copy in more_sends:
            copy.start()

        def push(src, dst, kind, recv, device):
            copy = remote(src, dst, sent.at[kind], recv, device)
            copy.start()
            return copy

        parts = [slice(i * D // RES_PARTS, (i + 1) * D // RES_PARTS) for i in range(RES_PARTS)]

        def res_copy(src, i, to, src_ref=None):
            block = resbuf.at[src, :, parts[i]]
            from_ref = block if src_ref is None else src_ref.at[:, parts[i]]
            return remote(
                from_ref, block, sent.at[0], res_r.at[src, i], place.z_id(to)
            )

        for i in range(RES_PARTS):
            for away in (2, -2, 1, -1):
                to = z + away

                @pl.when((to >= 0) & (to < n_z))
                def _(to=to, i=i):
                    res_copy(z, i, to, res_hbm).start()

        for step in range(1, n_z):
            to = place.z_id(place.z_peer(step))
            push(metabuf.at[z], metabuf.at[z], 1, meta_r.at[z], to)

        def pass_on(away, i):
            for sign in (1, -1):
                src, to = z - sign * away, z + sign

                @pl.when((src >= 0) & (src < n_z) & (to >= 0) & (to < n_z))
                def _(src=src, to=to):
                    res_copy(src, i, z).wait_recv()
                    res_copy(src, i, to).start()

        lane = lax.broadcasted_iota(jnp.int32, (1, lanes), 1)
        low = lane % ROPE < ROPE // 2
        mine = kv.at[sp]
        for load in loads[:3]:
            load.wait()

        def turn(values, cos, sin):
            return (
                values * cos
                + pltpu.roll(values, lanes - ROPE // 2, 1) * jnp.where(low, -sin, 0.0)
                + pltpu.roll(values, ROPE // 2, 1) * jnp.where(low, 0.0, sin)
            )

        sel = lax.broadcasted_iota(jnp.int32, (ROPE, lanes), 0)
        rot_sel = jnp.where(
            (lax.broadcasted_iota(jnp.int32, (ROPE, lanes), 1) % ROPE == sel)
            & (lax.broadcasted_iota(jnp.int32, (ROPE, lanes), 1) < heads * ROPE),
            1.0,
            0.0,
        ).astype(jnp.bfloat16)
        rot_parts = length // pt

        def make_keys(i, carry):
            at = pl.ds(pl.multiple_of(i * pt, pt), pt)
            lat = lat_in[at, :].astype(jnp.float32)
            scale = lax.rsqrt(jnp.mean(lat * lat, axis=-1, keepdims=True) + epsilon)
            normed_lat = (lat * scale * latg[...]).astype(jnp.bfloat16)
            nope = split_dot(normed_lat, kup[...], NN).astype(jnp.bfloat16).astype(jnp.float32)
            vals = split_dot(normed_lat, vup[...], NN).astype(jnp.bfloat16)
            kv[sp, pl.ds(pl.multiple_of(length + i * pt, pt), pt), :] = vals
            rot = split_dot(rot_in[:, at], rot_sel, TN)
            square, rot_square = nope * nope, rot * rot
            nope_scale, rot_scale = None, None
            for h in range(heads):
                in_nope = (lane >= h * NOPE) & (lane < (h + 1) * NOPE)
                in_rot = (lane >= h * ROPE) & (lane < (h + 1) * ROPE)
                one = lax.rsqrt(
                    jnp.sum(
                        jnp.where(in_nope, square, 0.0) + jnp.where(in_rot, rot_square, 0.0),
                        axis=-1,
                        keepdims=True,
                    )
                    / QK
                    + epsilon
                )
                nope_scale = one if h == 0 else jnp.where(in_nope, one, nope_scale)
                rot_scale = one if h == 0 else jnp.where(in_rot, one, rot_scale)
            kv[sp, at, :] = (nope * nope_scale * k_nope_gain).astype(jnp.bfloat16)
            turned = turn(rot * rot_scale * k_rot_gain, table[0, at, :], table[1, at, :])
            return turned

        def make_pair(i, carry):
            first = make_keys(i, carry)
            second = make_keys(i + rot_parts // 2, carry)
            packed = first + pltpu.roll(second, 64, 1)
            kv[sp, pl.ds(pl.multiple_of(2 * length + i * pt, pt), pt), :] = packed.astype(
                jnp.bfloat16
            )
            return carry

        lax.fori_loop(0, rot_parts // 2, make_pair, 0)
        for step in range(1, n_sp):
            dst = sp + n_sp - step

            @pl.when(dst < n_sp)
            def _(dst=dst):
                remote(mine, mine, kv_s.at[dst], kv_r.at[sp], place.sp_id(dst)).start()

        wide = 2 * lanes
        src_id = lax.broadcasted_iota(jnp.int32, (heads * QK, wide), 0)
        dst_id = lax.broadcasted_iota(jnp.int32, (heads * QK, wide), 1)
        pickers = []
        for h in range(heads):
            entry = src_id - h * QK
            nope_hit = (entry >= 0) & (entry < NOPE) & (dst_id == h * NOPE + entry)
            rot_hit = (
                (entry >= NOPE) & (entry < QK) & (dst_id == lanes + h * ROPE + entry - NOPE)
            )
            pickers.append(jnp.where(nope_hit | rot_hit, 1.0, 0.0).astype(jnp.bfloat16))

        loads[3].wait()

        def make_queries(i, carry):
            at = pl.ds(pl.multiple_of(i * pt, pt), pt)
            raw = q_in[:, at]
            for h in range(heads):
                spread = split_dot(raw, pickers[h], TN)
                scale = lax.rsqrt(
                    jnp.sum(spread * spread, axis=-1, keepdims=True) / QK + epsilon
                )
                nope = (spread[:, :lanes] * scale * q_nope_gain).astype(jnp.bfloat16)
                rot = turn(spread[:, lanes:] * scale * q_rot_gain, table[0, at, :], table[1, at, :])
                qbuf[h, 0, at, :lanes] = nope
                qbuf[h, 1, at, :lanes] = nope
                qbuf[h, 0, at, lanes:] = rot.astype(jnp.bfloat16)
                qbuf[h, 1, at, lanes:] = pltpu.roll(rot, 64, 1).astype(jnp.bfloat16)
            return carry

        lax.fori_loop(0, length // pt, make_queries, 0)

        factor = QK ** (-0.5) * 1.4426950408889634

        def attend(src, first, diagonal):
            knope = [kv[src, s * half : (s + 1) * half, :] for s in range(2)]
            krot = kv[src, 2 * length : bundle, :]
            keys = [jnp.concatenate([knope[s], krot], axis=1) for s in range(2)]
            vals = kv[src, length : 2 * length, :]

            def tile(i, carry):
                at = pl.ds(pl.multiple_of(i * qt, qt), qt)
                outs = []
                for h in range(heads):
                    scores = jnp.concatenate(
                        [split_dot(qbuf[h, s, at, :], keys[s], NT) for s in range(2)], axis=1
                    )
                    scores = scores * factor
                    if diagonal:
                        row = lax.broadcasted_iota(jnp.int32, scores.shape, 0) + i * qt
                        col = lax.broadcasted_iota(jnp.int32, scores.shape, 1)
                        scores = jnp.where(col <= row, scores, -1e30)
                    top = jnp.max(scores, axis=-1, keepdims=True)
                    if not first:
                        old = peak[h, at, :]
                        top = jnp.maximum(old[:, :1], top)
                    weight = jnp.exp2(scores - top)
                    sums = jnp.sum(weight, axis=-1, keepdims=True)
                    part_out = split_dot(weight.astype(jnp.bfloat16), vals, NN)
                    if first:
                        total[h, at, :] = jnp.broadcast_to(sums, (qt, lanes))
                        outs.append((part_out, None))
                    else:
                        fade = jnp.exp2(old[:, :1] - top)
                        total[h, at, :] = total[h, at, :] * fade + sums
                        outs.append((part_out, fade))
                    peak[h, at, :] = jnp.broadcast_to(top, (qt, lanes))
                new, fade = outs[0]
                for h in range(1, heads):
                    new = jnp.where(lane >= h * VH, outs[h][0], new)
                    if not first:
                        fade = jnp.where(lane >= h * VH, outs[h][1], fade)
                acc[at, :] = new if first else acc[at, :] * fade + new
                return carry

            lax.fori_loop(0, length // qt, tile, 0, unroll=2)

        attend(sp, True, True)

        def visit(step, carry):
            src = sp - step

            @pl.when(src >= 0)
            def _():
                remote(
                    kv.at[src], kv.at[src], kv_s.at[src], kv_r.at[src], place.sp_id(src)
                ).wait_recv()
                attend(src, False, False)

            return carry

        hops = [(away, i) for away in range(2, n_z - 1) for i in range(RES_PARTS)]
        head = RES_PARTS // 2
        for away, i in hops[:head]:
            pass_on(away, i)
        lax.fori_loop(1, 2, visit, 0)
        for away, i in hops[head:RES_PARTS]:
            pass_on(away, i)
        lax.fori_loop(2, n_sp, visit, 0)
        for away, i in hops[RES_PARTS:]:
            pass_on(away, i)

        for block in range(n_tp):
            at = pl.ds(block * tok, tok)
            bottom = total[0, at, :]
            for h in range(1, heads):
                bottom = jnp.where(lane >= h * VH, total[h, at, :], bottom)
            att[block % 2, (block // 2) * tok : (block // 2 + 1) * tok, :] = (
                acc[at, :] / bottom
            ).astype(jnp.bfloat16)
        def att_copy(src, parity, to_z, to_core, src_ref=None):
            block = gath.at[src]
            from_ref = block if src_ref is None else src_ref.at[parity]
            return remote(
                from_ref, block, sent.at[2], att_r.at[src], (sp, 2 * to_z + to_core)
            )

        for away in (2, -2, 1, -1):
            to = z + away

            @pl.when((to >= 0) & (to < n_z))
            def _(to=to):
                for parity in range(2):
                    att_copy(tp, parity, to, parity, att).start()

        remote(
            att.at[1 - core], gath.at[tp], sent.at[2], att_r.at[tp], place.partner()
        ).start()
        own = pltpu.make_async_copy(att.at[core], gath.at[tp], load_sem.at[6])
        own.start()

        partner = place.partner()
        for step in range(1, n_z):
            block = metabuf.at[place.z_peer(step)]
            remote(block, block, sent.at[1], meta_r.at[place.z_peer(step)], partner).wait_recv()
        pieces = []
        for first in range(0, n_z, per):
            piece = metabuf[first]
            for i in range(1, per):
                piece = jnp.where(lane >= i * tok, metabuf[first + i], piece)
            pieces.append(piece)
        meta = jnp.concatenate(pieces, axis=1)
        slot_id = lax.broadcasted_iota(jnp.int32, (rows, part), 0).astype(jnp.float32)
        for e in range(n_sp):
            hit = meta[e : e + 1, :] == slot_id
            mixer[e] = jnp.where(
                hit, meta[named_rows + e : named_rows + e + 1, :], 0.0
            ).astype(jnp.bfloat16)
        for i in range(RES_PARTS):
            for src in range(n_z):
                away = z - src
                passed = ((away >= 2) & (z + 1 < n_z)) | ((away <= -2) & (z > 0))

                @pl.when((away != 0) & jnp.logical_not(passed))
                def _(src=src, i=i):
                    res_copy(src, i, z).wait_recv()

        for load in loads[4:]:
            load.wait()
        own.wait()
        for away in range(2, n_z - 1):
            for sign in (1, -1):
                src, to = z - sign * away, z + sign

                @pl.when((src >= 0) & (src < n_z) & (to >= 0) & (to < n_z))
                def _(src=src, to=to):
                    for which in range(2):
                        att_copy(2 * src + which, core, z, core).wait_recv()
                        att_copy(2 * src + which, core, to, core).start()

        for src in range(n_tp):
            away = z - src // 2
            passed = ((away >= 2) & (z + 1 < n_z)) | ((away <= -2) & (z > 0))

            @pl.when((tp != src) & jnp.logical_not(passed))
            def _(src=src):
                att_copy(src, core, z, core).wait_recv()

        square = None
        for t in range(n_tp):
            block = gath[t].astype(jnp.float32)
            square = block * block if square is None else square + block * block
        scale = lax.rsqrt(jnp.sum(square, axis=-1, keepdims=True) / att_width + epsilon)
        for t in range(n_tp):
            normed[:, t * lanes : (t + 1) * lanes] = (
                gath[t].astype(jnp.float32) * scale * outg[t]
            ).astype(jnp.bfloat16)
        ct = 512
        square = None
        for c in range(D // ct):
            cols = slice(c * ct, (c + 1) * ct)
            values = split_dot(normed[...], wbuf[:, cols], NN) + resbuf[:, :, cols].reshape(
                part, ct
            ).astype(jnp.float32)
            mid[:, cols] = values
            more = jnp.sum(values * values, axis=-1, keepdims=True)
            square = more if square is None else square + more
        scale = lax.rsqrt(square / D + epsilon)
        for c in range(D // ct):
            cols = slice(c * ct, (c + 1) * ct)
            ffn[:, cols] = (mid[:, cols] * scale * ffng[0:1, cols]).astype(jnp.bfloat16)
        mid_out[...] = mid[pl.ds(pl.multiple_of(z * tok, tok), tok), :]
        for e in range(n_sp):
            hit = jnp.where(meta[e : e + 1, :] == slot_id, 1.0, 0.0).astype(jnp.bfloat16)
            for c in range(D // ct):
                cols = slice(c * ct, (c + 1) * ct)
                out_rows[e, :, cols] = split_dot(hit, ffn[:, cols], NN).astype(jnp.bfloat16)

        def drain():
            for i in range(RES_PARTS):
                block = resbuf.at[0, :, parts[i]]
                one = remote(block, block, sent.at[0], res_r.at[0, 0], partner)
                for away in (2, -2, 1, -1):

                    @pl.when((z + away >= 0) & (z + away < n_z))
                    def _(one=one):
                        one.wait_send()

            for away, i in hops:
                block = resbuf.at[0, :, parts[i]]
                one = remote(block, block, sent.at[0], res_r.at[0, 0], partner)
                for sign in (1, -1):
                    src, to = z - sign * away, z + sign

                    @pl.when((src >= 0) & (src < n_z) & (to >= 0) & (to < n_z))
                    def _(one=one):
                        one.wait_send()

            block = metabuf.at[pl.ds(0, n_z - 1)]
            remote(block, block, sent.at[1], meta_r.at[0], partner).wait_send()
            one = att_copy(tp, core, z, core)
            one.wait_send()
            for away in (2, -2, 1, -1):

                @pl.when((z + away >= 0) & (z + away < n_z))
                def _():
                    one.wait_send()
                    one.wait_send()

            for away in range(2, n_z - 1):
                for sign in (1, -1):
                    src, to = z - sign * away, z + sign

                    @pl.when((src >= 0) & (src < n_z) & (to >= 0) & (to < n_z))
                    def _():
                        one.wait_send()
                        one.wait_send()

            for step in range(1, n_sp):
                dst = sp + n_sp - step

                @pl.when(dst < n_sp)
                def _(dst=dst):
                    remote(mine, mine, kv_s.at[dst], kv_r.at[sp], place.sp_id(dst)).wait_send()

        return drain

    dma = pltpu.SemaphoreType.DMA
    bf, f4 = jnp.bfloat16, jnp.float32
    hbm = pl.BlockSpec(memory_space=pl.ANY)
    return dict(
        body=body,
        ins=(
            queries, latent, rot_key, lat_gain, key_up, value_up, q_gain, k_gain, out_gain,
            out_weight, residual, ffn_gain, routes, weights,
        ),
        in_specs=[
            hbm, hbm, vmem(), vmem(), hbm, hbm, vmem(), vmem(), vmem(), hbm, hbm, vmem(),
            vmem(), vmem(),
        ],
        outs=[((n_sp, rows, D), bf), ((n_sp, rows, part), bf), ((tok, D), f4)],
        scratch=[
            pltpu.VMEM(queries.shape, bf),
            pltpu.VMEM(latent.shape, bf),
            pltpu.VMEM(key_up.shape, bf),
            pltpu.VMEM(value_up.shape, bf),
            pltpu.VMEM((2, length, lanes), f4),
            pltpu.VMEM((8, lanes), f4),
            pltpu.VMEM((8, lanes), f4),
            pltpu.VMEM((heads, 2, length, 2 * lanes), bf),
            pltpu.VMEM((n_sp, bundle, lanes), bf),
            pltpu.VMEM((heads, length, lanes), f4),
            pltpu.VMEM((heads, length, lanes), f4),
            pltpu.VMEM((length, lanes), f4),
            pltpu.VMEM((2, part, lanes), bf),
            pltpu.VMEM((n_tp, part, lanes), bf),
            pltpu.VMEM((part, n_tp * lanes), bf),
            pltpu.VMEM(out_weight.shape, bf),
            pltpu.VMEM((n_z, tok, D), bf),
            pltpu.VMEM((n_z, 2 * named_rows, lanes), f4),
            pltpu.VMEM((part, D), f4),
            pltpu.VMEM((part, D), bf),
            dma((7,)),
            dma((3,)),
            dma((n_sp,)),
            dma((n_sp,)),
            dma((n_z, RES_PARTS)),
            dma((n_z,)),
            dma((n_tp,)),
        ],
    )


def shards(
    queries, latent, rot_key, latent_gain, key_up, value_up, query_gain, key_gain, out_gain,
    out_weight, residual, ffn_gain, routes, route_weights, expert_gate, expert_up, expert_down,
):
    heads = key_up.shape[1] // NOPE
    n_sp = lax.axis_size("sp")
    n_tp = lax.axis_size("tp")
    n_z = n_tp // 2
    width = heads * VH
    out_gain = out_gain.reshape(n_tp, 1, width)
    if width < 128:
        spare = 128 - width
        key_up = jnp.pad(key_up, ((0, 0), (0, spare)))
        value_up = jnp.pad(value_up, ((0, 0), (0, spare)))
        out_gain = jnp.pad(out_gain, ((0, 0), (0, 0), (0, spare)))
        out_weight = jnp.pad(
            out_weight.reshape(n_tp, width, D), ((0, 0), (0, spare), (0, 0))
        ).reshape(n_tp * 128, D)
    first = front_plan(
        queries.T, latent, rot_key.T, latent_gain[None, :], key_up, value_up,
        query_gain[None, :], key_gain[None, :], out_gain, out_weight,
        residual, ffn_gain[None, :], routes.T, route_weights.T, n_sp, n_z, n_tp * width,
    )
    cap = max(2, 9 * residual.shape[0] * TOPK // (8 * n_sp))
    second = expert_plan(
        n_z * cap, residual.shape[0], expert_gate[0], expert_up[0], expert_down[0], n_sp, n_z
    )
    return run_plans(first, second, residual.shape[0], n_sp, n_z)


def solution(mesh):
    return jax.shard_map(
        shards,
        mesh=mesh,
        in_specs=(
            P("sp", "tp"),
            P("sp", None),
            P("sp", None),
            P(),
            P(None, "tp"),
            P(None, "tp"),
            P(),
            P(),
            P(),
            P(),
            P(("sp", "tp"), None),
            P(),
            P(("sp", "tp"), None),
            P(("sp", "tp"), None),
            P("sp", None, "tp"),
            P("sp", None, "tp"),
            P("sp", "tp", None),
        ),
        out_specs=P(("sp", "tp"), None),
        check_vma=False,
    )
```

```python
import jax
import jax.numpy as jnp
import numpy as np
from jax import lax
from jax.experimental import pallas as pl
from jax.experimental.pallas import tpu as pltpu
from jax.sharding import PartitionSpec as P

D = 2048
NOPE = 64
ROPE = 32
VH = 64
TOPK = 2
QK = 96

epsilon = 1e-06
rope_base = 10000.0
MESH_ID = pl.DeviceIdType.MESH


class Place:
    def __init__(self, n_sp, n_z):
        self.n_sp, self.n_z = n_sp, n_z
        self.sp = lax.axis_index("sp")
        self.tp = lax.axis_index("tp")
        self.core = lax.rem(self.tp, 2)
        self.z = lax.div(self.tp, 2)

    def partner(self):
        return (self.sp, self.tp + 1 - 2 * self.core)

    def sp_peer(self, step):
        return lax.rem(self.sp + step, self.n_sp)

    def z_peer(self, step):
        return lax.rem(self.z + step, self.n_z)

    def sp_id(self, index):
        return (index, self.tp)

    def z_id(self, index):
        return (self.sp, 2 * index + self.core)

    def barrier(self, use_sp, use_z):
        sem = pltpu.get_barrier_semaphore()
        count = 1
        pl.semaphore_signal(sem, inc=1, device_id=self.partner(), device_id_type=MESH_ID)
        if use_sp:
            for step in range(1, self.n_sp):
                pl.semaphore_signal(
                    sem, inc=1, device_id=self.sp_id(self.sp_peer(step)), device_id_type=MESH_ID
                )
            count += self.n_sp - 1
        if use_z:
            for step in range(1, self.n_z):
                pl.semaphore_signal(
                    sem, inc=1, device_id=self.z_id(self.z_peer(step)), device_id_type=MESH_ID
                )
            count += self.n_z - 1
        pl.semaphore_wait(sem, count)


def remote(src, dst, send, recv, device):
    return pltpu.make_async_remote_copy(
        src_ref=src,
        dst_ref=dst,
        send_sem=send,
        recv_sem=recv,
        device_id=device,
        device_id_type=MESH_ID,
    )


def vmem():
    return pl.BlockSpec(memory_space=pltpu.VMEM)


def flip(value, bits):
    shift = 1
    while shift <= bits:
        if bits & shift:
            value = value + shift * (1 - 2 * lax.rem(lax.div(value, shift), 2))
        shift *= 2
    return value


CHUNKS = 8
PIECES = 4
WIDE = 512
LEAD = 3
LAG = 2


def expert_plan(rows, tok, gate, up, down, n_sp, n_z):
    width = D // CHUNKS
    hidden = gate.shape[1]
    quarter = D // 4
    phases = [[1, 2]] + [[k] for k in range(3, n_sp)] if n_sp > 2 else [[1]]

    def weight_refs(place, ins, scratch):
        own = pl.ds(pl.multiple_of(place.core * hidden, 128), hidden)
        gbuf, ubuf, dbuf = scratch[:3]
        return list(zip(ins, (gbuf.at[:, own], ubuf.at[:, own], dbuf.at[own, :])))

    def loads_of(place, ins, scratch):
        return [
            pltpu.make_async_copy(src, dst, scratch[-7].at[i])
            for i, (src, dst) in enumerate(weight_refs(place, ins, scratch))
        ]

    def shares_of(place, ins, scratch):
        return [
            remote(src, dst, scratch[-7].at[3 + i], scratch[-7].at[6 + i], place.partner())
            for i, (src, dst) in enumerate(weight_refs(place, ins, scratch))
        ]

    def body(place, given, ins, o_ref, scratch):
        x_in, mix_in, mid_in = given
        (
            gbuf, ubuf, dbuf, xbuf, hid, sbuf, rbuf, cbuf, fbuf,
            w_sem, sent, a_r, b_r, t_r, sp_r, z_r,
        ) = scratch
        core, z, me = place.core, place.z, place.sp
        loads = loads_of(place, ins, scratch)
        traded = shares_of(place, ins, scratch)
        side = lax.rem(z, 2)
        twin = place.z_id(z + 1 - 2 * side)
        final = phases[-1] if n_sp > 2 else []

        def share(k):
            return 0 if k in final else 2 * quarter

        both = [pl.ds(i * quarter, quarter) for i in range(2)]

        def strip(which, k, p):
            half = (D - share(k)) // 2
            piece = half // PIECES
            return pl.ds(pl.multiple_of(share(k) + which * half + p * piece, 128), piece)

        def push(src, dst, kind, recv, device):
            copy = remote(src, dst, sent.at[kind], recv, device)
            copy.start()
            return copy

        strips, shares, swaps = {}, {}, {}
        order = [(k, p) for ks in phases for p in range(PIECES) for k in ks]
        halves = [(k, i) for ks in phases for i in range(2) for k in ks if k not in final]

        def push_strip(k, p):
            dst = flip(me, k)
            cols = strip(side, k, p)
            strips[k, p] = push(
                x_in.at[dst, :, cols], xbuf.at[me, :, cols], 0, a_r.at[k, p], place.sp_id(dst)
            )

        near = [one for one in order if one[0] not in final]
        far = [one for one in order if one[0] in final]
        for k, p in near:
            push_strip(k, p)
        for i in range(2):
            for k, which in halves:
                if which == i:
                    dst = flip(me, k)
                    shares[k, i] = push(
                        x_in.at[dst, :, both[i]], xbuf.at[me, :, both[i]], 1, b_r.at[k, i],
                        place.sp_id(dst),
                    )
            for k, p in far[i * PIECES // 2 : (i + 1) * PIECES // 2]:
                push_strip(k, p)

        def forward_strip(k, p):
            block = xbuf.at[flip(me, k), :, strip(side, k, p)]
            strips[k, p].wait_recv()
            swaps[k, p] = push(block, block, 2, t_r.at[k, p], twin)

        def expert(x_ref, h_ref):
            g = jnp.dot(x_ref[...], gbuf[...], preferred_element_type=jnp.float32)
            u = jnp.dot(x_ref[...], ubuf[...], preferred_element_type=jnp.float32)
            h_ref[...] = (g / (1.0 + jnp.exp(-g)) * u).astype(jnp.bfloat16)

        def column(q):
            return pl.ds(pl.multiple_of(q * width, width), width)

        def back_copy(k, q):
            src = flip(me, k)
            return remote(
                sbuf.at[src, :, column(q)], rbuf.at[me, :, column(q)],
                sent.at[3], sp_r.at[k, q], place.sp_id(src),
            )

        def serve(k):
            src = flip(me, k)
            expert(x_in.at[me] if k == 0 else xbuf.at[src], hid.at[0])
            for w in range(D // WIDE):
                cols = slice(w * WIDE, (w + 1) * WIDE)
                total = jnp.dot(
                    hid[0], dbuf[:, cols], preferred_element_type=jnp.float32
                ).astype(jnp.bfloat16)
                if k == 0:
                    rbuf[src, :, cols] = total
                else:
                    sbuf[src, :, cols] = total

        def reply(ks, first, last):
            def body(q, carry):
                for k in ks:
                    back_copy(k, q).start()
                return carry

            lax.fori_loop(first, last, body, 0)

        for copy in loads:
            copy.wait()
        for copy in traded:
            copy.wait_recv()
        head = len(phases[0])
        for k, p in near[:head]:
            forward_strip(k, p)
        serve(0)
        for k, p in near[head:]:
            forward_strip(k, p)
        for k, p in near:
            swaps[k, p].wait_recv()
        rest = [k for ks in phases for k in ks if k not in final]
        coming = list(far)
        for _ in range(PIECES // 2 if coming else 0):
            forward_strip(*coming.pop(0))
        for k in rest:
            for i in range(2):
                shares[k, i].wait_recv()
            serve(k)
            reply([k], 0, LEAD)
            if coming:
                forward_strip(*coming.pop(0))
        while coming:
            forward_strip(*coming.pop(0))
        for k, p in far:
            swaps[k, p].wait_recv()
        for k in final:
            serve(k)

        def rest_of(q, carry):
            for k in final:
                back_copy(k, q).start()
            for k in rest:
                back_copy(k, q + LEAD).start()
            return carry

        lax.fori_loop(0, CHUNKS - LEAD, rest_of, 0)
        reply(final, CHUNKS - LEAD, CHUNKS)

        levels = n_z.bit_length() - 1

        def z_blocks(level):
            span = 2 << level
            keep = lax.rem(z, span)
            base = n_z - (n_z >> level)
            return [
                (j * span + keep, j * span + flip(keep, 1 << level), base + j)
                for j in range(n_z // span)
            ]

        def z_copy(q, level, sent_block, slot):
            return remote(
                cbuf.at[sent_block, :, column(q)], fbuf.at[slot, :, column(q)],
                sent.at[4], z_r.at[q, slot], place.z_id(flip(z, 1 << level)),
            )

        def combine(q):
            for k in range(1, n_sp):
                back_copy(k, q).wait_recv()
            total = None
            for src in range(n_sp):
                more = split_dot(mix_in[src], rbuf[src, :, column(q)], TN)
                total = more if total is None else total + more
            cbuf[:, :, column(q)] = total.astype(jnp.bfloat16).reshape(n_z, tok, width)
            for _, sent_block, slot in z_blocks(0):
                z_copy(q, 0, sent_block, slot).start()

        def add_level(q, level):
            for kept, sent_block, slot in z_blocks(level):
                z_copy(q, level, sent_block, slot).wait_recv()
                total = cbuf[kept, :, column(q)].astype(jnp.float32) + fbuf[
                    slot, :, column(q)
                ].astype(jnp.float32)
                if level + 1 == levels:
                    o_ref[:, column(q)] = (total + mid_in[:, column(q)]).astype(jnp.bfloat16)
                else:
                    cbuf[kept, :, column(q)] = total.astype(jnp.bfloat16)
            if level + 1 < levels:
                for _, sent_block, slot in z_blocks(level + 1):
                    z_copy(q, level + 1, sent_block, slot).start()

        def wave(i, carry):
            for stage in range(levels + 1):
                q = i - LAG * stage

                @pl.when((q >= 0) & (q < CHUNKS))
                def _(q=q, stage=stage):
                    if stage == 0:
                        combine(q)
                    else:
                        add_level(q, stage - 1)

            return carry

        lax.fori_loop(0, CHUNKS, wave, 0)
        lax.fori_loop(CHUNKS, CHUNKS + LAG * levels, wave, 0)
        strip_bytes = xbuf.at[:, :, pl.ds(0, quarter)]
        for kind, block in enumerate(
            (
                strip_bytes, xbuf.at[pl.ds(0, n_sp - 2), :, pl.ds(0, 2 * quarter)],
                strip_bytes, sbuf.at[pl.ds(0, n_sp - 1)], fbuf.at[pl.ds(0, n_z - 1)],
            )
        ):
            remote(block, block, sent.at[kind], z_r.at[0, 0], place.partner()).wait_send()
        for copy in traded:
            copy.wait_send()

    dma = pltpu.SemaphoreType.DMA
    bf = jnp.bfloat16
    block = pltpu.VMEM((n_sp, rows, D), bf)
    zblock = pltpu.VMEM((n_z, tok, D), bf)
    return dict(
        body=body,
        loads=loads_of,
        shares=shares_of,
        ins=(gate, up, down),
        scratch=[
            pltpu.VMEM((D, 2 * hidden), bf),
            pltpu.VMEM((D, 2 * hidden), bf),
            pltpu.VMEM((2 * hidden, D), bf),
            block,
            pltpu.VMEM((1, rows, 2 * hidden), bf),
            block, block, zblock, zblock,
            dma((9,)),
            dma((5,)),
            dma((n_sp, PIECES)),
            dma((n_sp, 2)),
            dma((n_sp, PIECES)),
            dma((n_sp, CHUNKS)),
            dma((CHUNKS, n_z)),
        ],
    )


VMEM_ROOM = 63 << 20


def run_plans(first, second, tok, n_sp, n_z):
    hbm = pl.BlockSpec(memory_space=pl.ANY)
    out_shape = jax.ShapeDtypeStruct((tok, D), jnp.bfloat16)
    n_ins, n_first, n_given = len(first["ins"]), len(first["scratch"]), len(first["outs"])
    given = [pltpu.VMEM(shape, dtype) for shape, dtype in first["outs"]]
    sizes = first["scratch"] + second["scratch"] + given
    need = sum(
        int(np.prod(one.inner_aval.shape)) * one.inner_aval.dtype.itemsize
        for one in sizes
        if "vmem" in str(one.memory_space)
    )

    def params(number, room):
        return pltpu.CompilerParams(
            collective_id=number, has_side_effects=True, vmem_limit_bytes=room
        )

    def merged(*refs):
        place = Place(n_sp, n_z)
        ins, weights, refs = refs[:n_ins], refs[n_ins : n_ins + 3], refs[n_ins + 3 :]
        o_ref, held, refs = refs[0], refs[1 : 1 + n_given], refs[1 + n_given :]
        later = refs[n_first:]
        drain = first["body"](
            place, ins, held, refs[:n_first], second["loads"](place, weights, later),
            second["shares"](place, weights, later),
        )
        second["body"](place, held, weights, o_ref, refs[n_first:])
        drain()

    if need < 52 << 20:
        return pl.pallas_call(
            merged,
            out_shape=out_shape,
            in_specs=first["in_specs"] + [hbm] * 3,
            out_specs=vmem(),
            scratch_shapes=given + first["scratch"] + second["scratch"],
            compiler_params=params(0, VMEM_ROOM),
            name="layer",
        )(*first["ins"], *second["ins"])

    def head(*refs):
        place = Place(n_sp, n_z)
        ins, outs = refs[:n_ins], refs[n_ins : n_ins + n_given]
        first["body"](place, ins, outs, refs[n_ins + n_given :], [], [])()

    def tail(*refs):
        place = Place(n_sp, n_z)
        scratch = refs[n_given + 4 :]
        for load in second["loads"](place, refs[n_given : n_given + 3], scratch):
            load.start()
        place.barrier(True, True)
        for copy in second["shares"](place, refs[n_given : n_given + 3], scratch):
            copy.start()
        second["body"](
            place, refs[:n_given], refs[n_given : n_given + 3], refs[n_given + 3], scratch
        )

    held = pl.pallas_call(
        head,
        out_shape=tuple(jax.ShapeDtypeStruct(*one) for one in first["outs"]),
        in_specs=first["in_specs"],
        out_specs=(vmem(),) * n_given,
        scratch_shapes=first["scratch"],
        compiler_params=params(0, VMEM_ROOM),
        name="front",
    )(*first["ins"])
    return pl.pallas_call(
        tail,
        out_shape=out_shape,
        in_specs=[vmem()] * n_given + [hbm] * 3,
        out_specs=vmem(),
        scratch_shapes=second["scratch"],
        compiler_params=params(1, VMEM_ROOM),
        name="experts",
    )(*held, *second["ins"])


RES_PARTS = 4


def split_dot(a, b, dims):
    return lax.dot_general(a, b, (dims, ((), ())), preferred_element_type=jnp.float32)


NT = ((1,), (1,))
NN = ((1,), (0,))
TN = ((0,), (0,))


def front_plan(
    queries, latent, rot_key, lat_gain, key_up, value_up, q_gain, k_gain, out_gain,
    out_weight, residual, ffn_gain, routes, weights, n_sp, n_z, width,
):
    heads, length = queries.shape[0] // QK, queries.shape[1]
    n_tp = 2 * n_z
    tok = residual.shape[0]
    part = n_z * tok
    cap = max(2, 9 * tok * TOPK // (8 * n_sp))
    rows = n_z * cap
    bundle = 2 * length + length // 2
    half = length // 2
    lanes = 128
    att_width = width
    qt = 256
    pt = 128
    per = lanes // tok
    named_rows = -(-n_sp // 8) * 8
    freqs = ROPE // 2
    inverse = np.float32(rope_base) ** (-np.arange(0, ROPE, 2, dtype=np.float32) / np.float32(ROPE))

    def body(place, ins, outs, scratch, more_loads, more_sends):
        (
            q_hbm, lat_hbm, rot_in, latg, kup_hbm, vup_hbm, qg, kg, outg, w_hbm, res_hbm, ffng,
            routes_in, weights_in,
        ) = ins
        out_rows, mixer, mid_out = outs
        (
            q_in, lat_in, kup, vup, table, gains, tokens, qbuf, kv, peak, total, acc, att, gath,
            normed, wbuf, resbuf, metabuf, mid, ffn, load_sem, sent, kv_s, kv_r, res_r, meta_r,
            att_r,
        ) = scratch
        sp, core, z, tp = place.sp, place.core, place.z, place.tp
        sem = pltpu.get_barrier_semaphore()
        for step in range(1, n_tp):
            pl.semaphore_signal(
                sem, inc=1, device_id=(sp, lax.rem(tp + step, n_tp)), device_id_type=MESH_ID
            )
        for step in range(1, n_sp):
            pl.semaphore_signal(
                sem, inc=1, device_id=place.sp_id(place.sp_peer(step)), device_id_type=MESH_ID
            )
        loads = []
        for i, (src, dst) in enumerate(
            (
                (lat_hbm, lat_in), (kup_hbm, kup), (vup_hbm, vup), (q_hbm, q_in),
                (res_hbm, resbuf.at[z]), (w_hbm, wbuf),
            )
        ):
            load = pltpu.make_async_copy(src, dst, load_sem.at[i])
            load.start()
            loads.append(load)
        for load in more_loads:
            load.start()

        tokens[0:1, :] = jnp.full((1, lanes), -1.0, jnp.float32)
        tokens[1:2, :] = jnp.full((1, lanes), -1.0, jnp.float32)
        tokens[0:TOPK, :tok] = routes_in[...].astype(jnp.float32)
        tokens[2:4, :tok] = weights_in[...]
        expert_id = lax.broadcasted_iota(jnp.int32, (named_rows, lanes), 0).astype(jnp.float32)
        named0 = expert_id == tokens[0:1, :]
        named1 = expert_id == tokens[1:2, :]
        named = jnp.where(named0 | named1, 1.0, 0.0)
        earlier = jnp.where(
            lax.broadcasted_iota(jnp.int32, (lanes, lanes), 0)
            < lax.broadcasted_iota(jnp.int32, (lanes, lanes), 1),
            1.0,
            0.0,
        ).astype(jnp.bfloat16)
        rank = split_dot(named.astype(jnp.bfloat16), earlier, NN)
        slot = jnp.where(named0 | named1, rank + (z * cap).astype(jnp.float32), -1.0)
        share = jnp.where(named0, tokens[2:3, :], 0.0) + jnp.where(named1, tokens[3:4, :], 0.0)
        place_by = lax.rem(z, per)
        for turn_by in range(per):

            @pl.when(place_by == turn_by)
            def _(turn_by=turn_by):
                metabuf[z, :named_rows] = pltpu.roll(slot, turn_by * tok, 1) if turn_by else slot
                metabuf[z, named_rows:] = pltpu.roll(share, turn_by * tok, 1) if turn_by else share

        freq_id = lax.broadcasted_iota(jnp.int32, (freqs, length), 0)
        freq = jnp.zeros((freqs, length), jnp.float32)
        for i in range(freqs):
            freq = jnp.where(freq_id == i, float(inverse[i]), freq)
        where = lax.broadcasted_iota(jnp.int32, (freqs, length), 1) + sp * length
        angle = where.astype(jnp.float32) * freq
        spread_by = jnp.where(
            lax.broadcasted_iota(jnp.int32, (freqs, lanes), 1) % freqs
            == lax.broadcasted_iota(jnp.int32, (freqs, lanes), 0),
            1.0,
            0.0,
        )

        for which, values in enumerate((jnp.cos(angle), jnp.sin(angle))):
            table[which] = lax.dot_general(
                values, spread_by, (TN, ((), ())), precision=lax.Precision.HIGHEST,
                preferred_element_type=jnp.float32,
            )
        for i, gain in enumerate((qg, kg)):
            gains[4 + i : 5 + i, :] = jnp.zeros((1, lanes), jnp.float32)
            gains[4 + i : 5 + i, :QK] = gain[...]
        gain_lane = lax.broadcasted_iota(jnp.int32, (1, lanes), 1)
        packed = []
        for i in range(2):
            raw_gain = gains[4 + i : 5 + i, :]
            nope_gain = jnp.where(gain_lane < NOPE, raw_gain, pltpu.roll(raw_gain, NOPE, 1))
            once = jnp.where(gain_lane < ROPE, pltpu.roll(raw_gain, lanes - NOPE, 1), 0.0)
            rot_gain = once
            for h in range(1, heads):
                rot_gain = rot_gain + pltpu.roll(once, h * ROPE, 1)
            packed.append((nope_gain, rot_gain))
        (q_nope_gain, q_rot_gain), (k_nope_gain, k_rot_gain) = packed

        pl.semaphore_wait(sem, n_tp - 1 + n_sp - 1)
        for copy in more_sends:
            copy.start()

        def push(src, dst, kind, recv, device):
            copy = remote(src, dst, sent.at[kind], recv, device)
            copy.start()
            return copy

        parts = [slice(i * D // RES_PARTS, (i + 1) * D // RES_PARTS) for i in range(RES_PARTS)]

        def res_copy(src, i, to, src_ref=None):
            block = resbuf.at[src, :, parts[i]]
            from_ref = block if src_ref is None else src_ref.at[:, parts[i]]
            return remote(
                from_ref, block, sent.at[0], res_r.at[src, i], place.z_id(to)
            )

        for i in range(RES_PARTS):
            for away in (2, -2, 1, -1):
                to = z + away

                @pl.when((to >= 0) & (to < n_z))
                def _(to=to, i=i):
                    res_copy(z, i, to, res_hbm).start()

        for step in range(1, n_z):
            to = place.z_id(place.z_peer(step))
            push(metabuf.at[z], metabuf.at[z], 1, meta_r.at[z], to)

        def pass_on(away, i):
            for sign in (1, -1):
                src, to = z - sign * away, z + sign

                @pl.when((src >= 0) & (src < n_z) & (to >= 0) & (to < n_z))
                def _(src=src, to=to):
                    res_copy(src, i, z).wait_recv()
                    res_copy(src, i, to).start()

        lane = lax.broadcasted_iota(jnp.int32, (1, lanes), 1)
        low = lane % ROPE < ROPE // 2
        mine = kv.at[sp]
        for load in loads[:3]:
            load.wait()

        def turn(values, cos, sin):
            return (
                values * cos
                + pltpu.roll(values, lanes - ROPE // 2, 1) * jnp.where(low, -sin, 0.0)
                + pltpu.roll(values, ROPE // 2, 1) * jnp.where(low, 0.0, sin)
            )

        sel = lax.broadcasted_iota(jnp.int32, (ROPE, lanes), 0)
        rot_sel = jnp.where(
            (lax.broadcasted_iota(jnp.int32, (ROPE, lanes), 1) % ROPE == sel)
            & (lax.broadcasted_iota(jnp.int32, (ROPE, lanes), 1) < heads * ROPE),
            1.0,
            0.0,
        ).astype(jnp.bfloat16)
        rot_parts = length // pt

        def make_keys(i, carry):
            at = pl.ds(pl.multiple_of(i * pt, pt), pt)
            lat = lat_in[at, :].astype(jnp.float32)
            scale = lax.rsqrt(jnp.mean(lat * lat, axis=-1, keepdims=True) + epsilon)
            normed_lat = (lat * scale * latg[...]).astype(jnp.bfloat16)
            nope = split_dot(normed_lat, kup[...], NN).astype(jnp.bfloat16).astype(jnp.float32)
            vals = split_dot(normed_lat, vup[...], NN).astype(jnp.bfloat16)
            kv[sp, pl.ds(pl.multiple_of(length + i * pt, pt), pt), :] = vals
            rot = split_dot(rot_in[:, at], rot_sel, TN)
            square, rot_square = nope * nope, rot * rot
            nope_scale, rot_scale = None, None
            for h in range(heads):
                in_nope = (lane >= h * NOPE) & (lane < (h + 1) * NOPE)
                in_rot = (lane >= h * ROPE) & (lane < (h + 1) * ROPE)
                one = lax.rsqrt(
                    jnp.sum(
                        jnp.where(in_nope, square, 0.0) + jnp.where(in_rot, rot_square, 0.0),
                        axis=-1,
                        keepdims=True,
                    )
                    / QK
                    + epsilon
                )
                nope_scale = one if h == 0 else jnp.where(in_nope, one, nope_scale)
                rot_scale = one if h == 0 else jnp.where(in_rot, one, rot_scale)
            kv[sp, at, :] = (nope * nope_scale * k_nope_gain).astype(jnp.bfloat16)
            turned = turn(rot * rot_scale * k_rot_gain, table[0, at, :], table[1, at, :])
            return turned

        def make_pair(i, carry):
            first = make_keys(i, carry)
            second = make_keys(i + rot_parts // 2, carry)
            packed = first + pltpu.roll(second, 64, 1)
            kv[sp, pl.ds(pl.multiple_of(2 * length + i * pt, pt), pt), :] = packed.astype(
                jnp.bfloat16
            )
            return carry

        lax.fori_loop(0, rot_parts // 2, make_pair, 0)
        for step in range(1, n_sp):
            dst = sp + n_sp - step

            @pl.when(dst < n_sp)
            def _(dst=dst):
                remote(mine, mine, kv_s.at[dst], kv_r.at[sp], place.sp_id(dst)).start()

        wide = 2 * lanes
        src_id = lax.broadcasted_iota(jnp.int32, (heads * QK, wide), 0)
        dst_id = lax.broadcasted_iota(jnp.int32, (heads * QK, wide), 1)
        pickers = []
        for h in range(heads):
            entry = src_id - h * QK
            nope_hit = (entry >= 0) & (entry < NOPE) & (dst_id == h * NOPE + entry)
            rot_hit = (
                (entry >= NOPE) & (entry < QK) & (dst_id == lanes + h * ROPE + entry - NOPE)
            )
            pickers.append(jnp.where(nope_hit | rot_hit, 1.0, 0.0).astype(jnp.bfloat16))

        loads[3].wait()

        def make_queries(i, carry):
            at = pl.ds(pl.multiple_of(i * pt, pt), pt)
            raw = q_in[:, at]
            for h in range(heads):
                spread = split_dot(raw, pickers[h], TN)
                scale = lax.rsqrt(
                    jnp.sum(spread * spread, axis=-1, keepdims=True) / QK + epsilon
                )
                nope = (spread[:, :lanes] * scale * q_nope_gain).astype(jnp.bfloat16)
                rot = turn(spread[:, lanes:] * scale * q_rot_gain, table[0, at, :], table[1, at, :])
                qbuf[h, 0, at, :lanes] = nope
                qbuf[h, 1, at, :lanes] = nope
                qbuf[h, 0, at, lanes:] = rot.astype(jnp.bfloat16)
                qbuf[h, 1, at, lanes:] = pltpu.roll(rot, 64, 1).astype(jnp.bfloat16)
            return carry

        lax.fori_loop(0, length // pt, make_queries, 0)

        factor = QK ** (-0.5) * 1.4426950408889634

        def attend(src, first, diagonal):
            knope = [kv[src, s * half : (s + 1) * half, :] for s in range(2)]
            krot = kv[src, 2 * length : bundle, :]
            keys = [jnp.concatenate([knope[s], krot], axis=1) for s in range(2)]
            vals = kv[src, length : 2 * length, :]

            def tile(i, carry):
                at = pl.ds(pl.multiple_of(i * qt, qt), qt)
                outs = []
                for h in range(heads):
                    scores = jnp.concatenate(
                        [split_dot(qbuf[h, s, at, :], keys[s], NT) for s in range(2)], axis=1
                    )
                    scores = scores * factor
                    if diagonal:
                        row = lax.broadcasted_iota(jnp.int32, scores.shape, 0) + i * qt
                        col = lax.broadcasted_iota(jnp.int32, scores.shape, 1)
                        scores = jnp.where(col <= row, scores, -1e30)
                    top = jnp.max(scores, axis=-1, keepdims=True)
                    if not first:
                        old = peak[h, at, :]
                        top = jnp.maximum(old[:, :1], top)
                    weight = jnp.exp2(scores - top)
                    sums = jnp.sum(weight, axis=-1, keepdims=True)
                    part_out = split_dot(weight.astype(jnp.bfloat16), vals, NN)
                    if first:
                        total[h, at, :] = jnp.broadcast_to(sums, (qt, lanes))
                        outs.append((part_out, None))
                    else:
                        fade = jnp.exp2(old[:, :1] - top)
                        total[h, at, :] = total[h, at, :] * fade + sums
                        outs.append((part_out, fade))
                    peak[h, at, :] = jnp.broadcast_to(top, (qt, lanes))
                new, fade = outs[0]
                for h in range(1, heads):
                    new = jnp.where(lane >= h * VH, outs[h][0], new)
                    if not first:
                        fade = jnp.where(lane >= h * VH, outs[h][1], fade)
                acc[at, :] = new if first else acc[at, :] * fade + new
                return carry

            lax.fori_loop(0, length // qt, tile, 0, unroll=2)

        attend(sp, True, True)

        def visit(step, carry):
            src = sp - step

            @pl.when(src >= 0)
            def _():
                remote(
                    kv.at[src], kv.at[src], kv_s.at[src], kv_r.at[src], place.sp_id(src)
                ).wait_recv()
                attend(src, False, False)

            return carry

        hops = [(away, i) for away in range(2, n_z - 1) for i in range(RES_PARTS)]
        head = RES_PARTS // 2
        for away, i in hops[:head]:
            pass_on(away, i)
        lax.fori_loop(1, 2, visit, 0)
        for away, i in hops[head:RES_PARTS]:
            pass_on(away, i)
        lax.fori_loop(2, n_sp, visit, 0)
        for away, i in hops[RES_PARTS:]:
            pass_on(away, i)

        for block in range(n_tp):
            at = pl.ds(block * tok, tok)
            bottom = total[0, at, :]
            for h in range(1, heads):
                bottom = jnp.where(lane >= h * VH, total[h, at, :], bottom)
            att[block % 2, (block // 2) * tok : (block // 2 + 1) * tok, :] = (
                acc[at, :] / bottom
            ).astype(jnp.bfloat16)
        def att_copy(src, parity, to_z, to_core, src_ref=None):
            block = gath.at[src]
            from_ref = block if src_ref is None else src_ref.at[parity]
            return remote(
                from_ref, block, sent.at[2], att_r.at[src], (sp, 2 * to_z + to_core)
            )

        for away in (2, -2, 1, -1):
            to = z + away

            @pl.when((to >= 0) & (to < n_z))
            def _(to=to):
                for parity in range(2):
                    att_copy(tp, parity, to, parity, att).start()

        remote(
            att.at[1 - core], gath.at[tp], sent.at[2], att_r.at[tp], place.partner()
        ).start()
        own = pltpu.make_async_copy(att.at[core], gath.at[tp], load_sem.at[6])
        own.start()

        partner = place.partner()
        for step in range(1, n_z):
            block = metabuf.at[place.z_peer(step)]
            remote(block, block, sent.at[1], meta_r.at[place.z_peer(step)], partner).wait_recv()
        pieces = []
        for first in range(0, n_z, per):
            piece = metabuf[first]
            for i in range(1, per):
                piece = jnp.where(lane >= i * tok, metabuf[first + i], piece)
            pieces.append(piece)
        meta = jnp.concatenate(pieces, axis=1)
        slot_id = lax.broadcasted_iota(jnp.int32, (rows, part), 0).astype(jnp.float32)
        for e in range(n_sp):
            hit = meta[e : e + 1, :] == slot_id
            mixer[e] = jnp.where(
                hit, meta[named_rows + e : named_rows + e + 1, :], 0.0
            ).astype(jnp.bfloat16)
        for i in range(RES_PARTS):
            for src in range(n_z):
                away = z - src
                passed = ((away >= 2) & (z + 1 < n_z)) | ((away <= -2) & (z > 0))

                @pl.when((away != 0) & jnp.logical_not(passed))
                def _(src=src, i=i):
                    res_copy(src, i, z).wait_recv()

        for load in loads[4:]:
            load.wait()
        own.wait()
        for away in range(2, n_z - 1):
            for sign in (1, -1):
                src, to = z - sign * away, z + sign

                @pl.when((src >= 0) & (src < n_z) & (to >= 0) & (to < n_z))
                def _(src=src, to=to):
                    for which in range(2):
                        att_copy(2 * src + which, core, z, core).wait_recv()
                        att_copy(2 * src + which, core, to, core).start()

        for src in range(n_tp):
            away = z - src // 2
            passed = ((away >= 2) & (z + 1 < n_z)) | ((away <= -2) & (z > 0))

            @pl.when((tp != src) & jnp.logical_not(passed))
            def _(src=src):
                att_copy(src, core, z, core).wait_recv()

        square = None
        for t in range(n_tp):
            block = gath[t].astype(jnp.float32)
            square = block * block if square is None else square + block * block
        scale = lax.rsqrt(jnp.sum(square, axis=-1, keepdims=True) / att_width + epsilon)
        for t in range(n_tp):
            normed[:, t * lanes : (t + 1) * lanes] = (
                gath[t].astype(jnp.float32) * scale * outg[t]
            ).astype(jnp.bfloat16)
        ct = 512
        square = None
        for c in range(D // ct):
            cols = slice(c * ct, (c + 1) * ct)
            values = split_dot(normed[...], wbuf[:, cols], NN) + resbuf[:, :, cols].reshape(
                part, ct
            ).astype(jnp.float32)
            mid[:, cols] = values
            more = jnp.sum(values * values, axis=-1, keepdims=True)
            square = more if square is None else square + more
        scale = lax.rsqrt(square / D + epsilon)
        for c in range(D // ct):
            cols = slice(c * ct, (c + 1) * ct)
            ffn[:, cols] = (mid[:, cols] * scale * ffng[0:1, cols]).astype(jnp.bfloat16)
        mid_out[...] = mid[pl.ds(pl.multiple_of(z * tok, tok), tok), :]
        for e in range(n_sp):
            hit = jnp.where(meta[e : e + 1, :] == slot_id, 1.0, 0.0).astype(jnp.bfloat16)
            for c in range(D // ct):
                cols = slice(c * ct, (c + 1) * ct)
                out_rows[e, :, cols] = split_dot(hit, ffn[:, cols], NN).astype(jnp.bfloat16)

        def drain():
            for i in range(RES_PARTS):
                block = resbuf.at[0, :, parts[i]]
                one = remote(block, block, sent.at[0], res_r.at[0, 0], partner)
                for away in (2, -2, 1, -1):

                    @pl.when((z + away >= 0) & (z + away < n_z))
                    def _(one=one):
                        one.wait_send()

            for away, i in hops:
                block = resbuf.at[0, :, parts[i]]
                one = remote(block, block, sent.at[0], res_r.at[0, 0], partner)
                for sign in (1, -1):
                    src, to = z - sign * away, z + sign

                    @pl.when((src >= 0) & (src < n_z) & (to >= 0) & (to < n_z))
                    def _(one=one):
                        one.wait_send()

            block = metabuf.at[pl.ds(0, n_z - 1)]
            remote(block, block, sent.at[1], meta_r.at[0], partner).wait_send()
            one = att_copy(tp, core, z, core)
            one.wait_send()
            for away in (2, -2, 1, -1):

                @pl.when((z + away >= 0) & (z + away < n_z))
                def _():
                    one.wait_send()
                    one.wait_send()

            for away in range(2, n_z - 1):
                for sign in (1, -1):
                    src, to = z - sign * away, z + sign

                    @pl.when((src >= 0) & (src < n_z) & (to >= 0) & (to < n_z))
                    def _():
                        one.wait_send()
                        one.wait_send()

            for step in range(1, n_sp):
                dst = sp + n_sp - step

                @pl.when(dst < n_sp)
                def _(dst=dst):
                    remote(mine, mine, kv_s.at[dst], kv_r.at[sp], place.sp_id(dst)).wait_send()

        return drain

    dma = pltpu.SemaphoreType.DMA
    bf, f4 = jnp.bfloat16, jnp.float32
    hbm = pl.BlockSpec(memory_space=pl.ANY)
    return dict(
        body=body,
        ins=(
            queries, latent, rot_key, lat_gain, key_up, value_up, q_gain, k_gain, out_gain,
            out_weight, residual, ffn_gain, routes, weights,
        ),
        in_specs=[
            hbm, hbm, vmem(), vmem(), hbm, hbm, vmem(), vmem(), vmem(), hbm, hbm, vmem(),
            vmem(), vmem(),
        ],
        outs=[((n_sp, rows, D), bf), ((n_sp, rows, part), bf), ((tok, D), f4)],
        scratch=[
            pltpu.VMEM(queries.shape, bf),
            pltpu.VMEM(latent.shape, bf),
            pltpu.VMEM(key_up.shape, bf),
            pltpu.VMEM(value_up.shape, bf),
            pltpu.VMEM((2, length, lanes), f4),
            pltpu.VMEM((8, lanes), f4),
            pltpu.VMEM((8, lanes), f4),
            pltpu.VMEM((heads, 2, length, 2 * lanes), bf),
            pltpu.VMEM((n_sp, bundle, lanes), bf),
            pltpu.VMEM((heads, length, lanes), f4),
            pltpu.VMEM((heads, length, lanes), f4),
            pltpu.VMEM((length, lanes), f4),
            pltpu.VMEM((2, part, lanes), bf),
            pltpu.VMEM((n_tp, part, lanes), bf),
            pltpu.VMEM((part, n_tp * lanes), bf),
            pltpu.VMEM(out_weight.shape, bf),
            pltpu.VMEM((n_z, tok, D), bf),
            pltpu.VMEM((n_z, 2 * named_rows, lanes), f4),
            pltpu.VMEM((part, D), f4),
            pltpu.VMEM((part, D), bf),
            dma((7,)),
            dma((3,)),
            dma((n_sp,)),
            dma((n_sp,)),
            dma((n_z, RES_PARTS)),
            dma((n_z,)),
            dma((n_tp,)),
        ],
    )


def shards(
    queries, latent, rot_key, latent_gain, key_up, value_up, query_gain, key_gain, out_gain,
    out_weight, residual, ffn_gain, routes, route_weights, expert_gate, expert_up, expert_down,
):
    heads = key_up.shape[1] // NOPE
    n_sp = lax.axis_size("sp")
    n_tp = lax.axis_size("tp")
    n_z = n_tp // 2
    width = heads * VH
    out_gain = out_gain.reshape(n_tp, 1, width)
    if width < 128:
        spare = 128 - width
        key_up = jnp.pad(key_up, ((0, 0), (0, spare)))
        value_up = jnp.pad(value_up, ((0, 0), (0, spare)))
        out_gain = jnp.pad(out_gain, ((0, 0), (0, 0), (0, spare)))
        out_weight = jnp.pad(
            out_weight.reshape(n_tp, width, D), ((0, 0), (0, spare), (0, 0))
        ).reshape(n_tp * 128, D)
    first = front_plan(
        queries.T, latent, rot_key.T, latent_gain[None, :], key_up, value_up,
        query_gain[None, :], key_gain[None, :], out_gain, out_weight,
        residual, ffn_gain[None, :], routes.T, route_weights.T, n_sp, n_z, n_tp * width,
    )
    cap = max(2, 9 * residual.shape[0] * TOPK // (8 * n_sp))
    second = expert_plan(
        n_z * cap, residual.shape[0], expert_gate[0], expert_up[0], expert_down[0], n_sp, n_z
    )
    return run_plans(first, second, residual.shape[0], n_sp, n_z)


def solution(mesh):
    return jax.shard_map(
        shards,
        mesh=mesh,
        in_specs=(
            P("sp", "tp"),
            P("sp", None),
            P("sp", None),
            P(),
            P(None, "tp"),
            P(None, "tp"),
            P(),
            P(),
            P(),
            P(),
            P(("sp", "tp"), None),
            P(),
            P(("sp", "tp"), None),
            P(("sp", "tp"), None),
            P("sp", None, "tp"),
            P("sp", None, "tp"),
            P("sp", "tp", None),
        ),
        out_specs=P(("sp", "tp"), None),
        check_vma=False,
    )
```
